32 devices in a mesh: sp: 16 (over z, y, x), tp: 2 (over core).
Axes of the slice: x: 2, y: 2, z: 4, core: 2. Of those that a mesh axis runs over, the one named last changes fastest.
Arguments:
- residual: bfloat16 [2048, 2048], P(('sp', 'tp')), may hold values from -6 to 6
- query_wide: bfloat16 [2048, 1024], P('sp', 'tp'), may hold values from -6 to 6
- key_wide: bfloat16 [2048, 1024], P('sp', 'tp'), may hold values from -6 to 6
- value_wide: bfloat16 [2048, 2048], P('sp', 'tp'), may hold values from -6 to 6
- outgate_wide: bfloat16 [2048, 2048], P('sp', 'tp'), may hold values from -6 to 6
- gating_wide: float32 [3, 8, 2048], P(None, 'tp', 'sp'), may hold values from -4 to 240, as said below
- gain_wide: bfloat16 [2048], P('tp'), may hold values from 0.099609375 to 1.8984375
- readout_wide: bfloat16 [2048, 2048], P('tp'), may hold values from -0.109375 to 0.109375
- query_narrow: bfloat16 [2048, 512], P('sp', 'tp'), may hold values from -6 to 6
- key_narrow: bfloat16 [2048, 512], P('sp', 'tp'), may hold values from -6 to 6
- value_narrow: bfloat16 [2048, 1024], P('sp', 'tp'), may hold values from -6 to 6
- outgate_narrow: bfloat16 [2048, 1024], P('sp', 'tp'), may hold values from -6 to 6
- gating_narrow: float32 [3, 8, 2048], P(None, 'tp', 'sp'), may hold values from -4 to 240, as said below
- gain_narrow: bfloat16 [1024], P('tp'), may hold values from 0.099609375 to 1.8984375
- readout_narrow: bfloat16 [1024, 2048], P('tp'), may hold values from -0.109375 to 0.109375
- norm_gain: bfloat16 [2048], replicated, may hold values from 0.099609375 to 1.8984375
- gate_weight: bfloat16 [2048, 5632], P('sp', 'tp'), may hold values from -0.125 to 0.125
- up_weight: bfloat16 [2048, 5632], P('sp', 'tp'), may hold values from -0.125 to 0.125
- down_weight: bfloat16 [5632, 2048], P('tp', 'sp'), may hold values from -0.078125 to 0.078125
Outputs:
- mixed_out: bfloat16 [2048, 2048], P(('sp', 'tp'))
The draws below stay inside these ranges and needn't reach their ends.
Inputs may be any that keep to these rules, and one draw needn't show every extreme that they name: `gating_wide`: row 0 holds input gate pre-activations, row 1 forget gate pre-activations, row 2 an added log-decay that is zero or negative. `gating_narrow`: row 0 holds input gate pre-activations, row 1 forget gate pre-activations, row 2 an added log-decay that is zero or negative.
All inputs are finite; a program needn't handle non-finite values.
Results may differ from the reference program's by a relative error of at most 0.017.
Values may be sent and summed in bfloat16 or wider, within the bound.
A program may use at most 128 MiB of HBM per device.

```python
import math
import jax
import jax.numpy as jnp
from jax import lax

D = 2048
FF = 5632
HEADS_A = 8
DK_A = 128
DV_A = 256
HEADS_B = 8
DK_B = 64
DV_B = 128
BLOCK = 64
TOK_DEV = 128
CONTEXT_LENGTH = 2048
N_TP = 2


def draw_gating(key, attention_tally):
    keys = jax.random.split(key, 10)
    incoming_matrix = jnp.clip(jax.random.normal(keys[0], (attention_tally, CONTEXT_LENGTH), jnp.float32), -4.0, 4.0)
    entry_ordinal = jnp.broadcast_to(jnp.arange(attention_tally)[:, None], (attention_tally, 4))
    threshold = 50
    fast = jax.random.randint(keys[5], (attention_tally,), 0, 100) < threshold
    base = jnp.where(fast, 4.0, math.log(CONTEXT_LENGTH) + 1.0)
    levels = jnp.repeat(jax.random.uniform(keys[6], (CONTEXT_LENGTH // TOK_DEV,), jnp.float32, -0.7, 0.7), TOK_DEV)
    jitter = jax.random.uniform(keys[7], (attention_tally, CONTEXT_LENGTH), jnp.float32, -1.0, 1.0)
    retention_factor = base[:, None] + levels[None, :] + jitter
    word_locations = jax.random.randint(keys[8], (attention_tally, 3), 0, CONTEXT_LENGTH)
    objective_scores = jnp.log(jax.random.uniform(keys[9], (attention_tally, 3), jnp.float32, 0.5, 0.8))
    admission_exponent = jnp.zeros((attention_tally, CONTEXT_LENGTH), jnp.float32).at[entry_ordinal[:, :3], word_locations].add(objective_scores)
    admission_exponent = jnp.maximum(admission_exponent, -4.0)
    return jnp.stack([incoming_matrix, retention_factor, admission_exponent])


def draw_gating_wide(key, part):
    return draw_gating(jax.random.fold_in(key, 11), HEADS_A)


def draw_gating_narrow(key, part):
    return draw_gating(jax.random.fold_in(key, 12), HEADS_B)


def steps_of(own_key, extent, cuts, low, largest):
    level, own = 1.0, jax.random.fold_in(own_key, 6)
    for position, shards_of in cuts:
        draws = jnp.exp(jax.random.uniform(jax.random.fold_in(own, position), (shards_of,), jnp.float32, low / len(cuts), largest / len(cuts)))
        level = level * jnp.repeat(draws, extent[position] // shards_of).reshape([-1 if axis == position else 1 for axis in range(len(extent))])
    return level


def scatter_about(key, shape, width, bound, pieces=(), kind=jnp.bfloat16):
    array = jax.random.normal(key, shape, jnp.float32) * width
    if len(pieces) > 0:
        array = steps_of(key, shape, pieces, -0.22, 0.18) * array
    return jnp.clip(array, min=-bound, max=bound).astype(kind)


def setup_inputs(seed: int = 0) -> dict:
    splits = jax.random.split(jax.random.key(seed), 20)
    return {
        "residual": scatter_about(splits[0], (CONTEXT_LENGTH, D), 1.0, 6.0, ((0, 32),)),
        "query_wide": scatter_about(splits[1], (CONTEXT_LENGTH, HEADS_A * DK_A), 1.0, 6.0, ((0, 16), (1, 2))),
        "key_wide": scatter_about(splits[2], (CONTEXT_LENGTH, HEADS_A * DK_A), 1.0, 6.0, ((0, 16), (1, 2))),
        "value_wide": scatter_about(splits[3], (CONTEXT_LENGTH, HEADS_A * DV_A), 1.0, 6.0, ((0, 16), (1, 2))),
        "outgate_wide": scatter_about(splits[4], (CONTEXT_LENGTH, HEADS_A * DV_A), 1.0, 6.0, ((0, 16), (1, 2))),
        "gating_wide": draw_gating_wide(jax.random.fold_in(splits[19], 71), 0),
        "gain_wide": jnp.clip(1.0 + 0.18 * jax.random.normal(splits[6], (HEADS_A * DV_A,), jnp.float32), 0.099609375, 1.8984375).astype(jnp.bfloat16),
        "readout_wide": scatter_about(splits[7], (HEADS_A * DV_A, D), (HEADS_A * DV_A + HEADS_B * DV_B) ** -0.5, 0.109375, ((0, 2),)),
        "query_narrow": scatter_about(splits[8], (CONTEXT_LENGTH, HEADS_B * DK_B), 1.0, 6.0, ((0, 16), (1, 2))),
        "key_narrow": scatter_about(splits[9], (CONTEXT_LENGTH, HEADS_B * DK_B), 1.0, 6.0, ((0, 16), (1, 2))),
        "value_narrow": scatter_about(splits[10], (CONTEXT_LENGTH, HEADS_B * DV_B), 1.0, 6.0, ((0, 16), (1, 2))),
        "outgate_narrow": scatter_about(splits[11], (CONTEXT_LENGTH, HEADS_B * DV_B), 1.0, 6.0, ((0, 16), (1, 2))),
        "gating_narrow": draw_gating_narrow(jax.random.fold_in(splits[19], 71), 0),
        "gain_narrow": jnp.clip(1.0 + 0.18 * jax.random.normal(splits[13], (HEADS_B * DV_B,), jnp.float32), 0.099609375, 1.8984375).astype(jnp.bfloat16),
        "readout_narrow": scatter_about(splits[14], (HEADS_B * DV_B, D), (HEADS_A * DV_A + HEADS_B * DV_B) ** -0.5, 0.109375, ((0, 2),)),
        "norm_gain": jnp.clip(1.0 + 0.18 * jax.random.normal(splits[15], (D,), jnp.float32), 0.099609375, 1.8984375).astype(jnp.bfloat16),
        "gate_weight": scatter_about(splits[16], (D, FF), D ** -0.5, 0.125, ((0, 16), (1, 2))),
        "up_weight": scatter_about(splits[17], (D, FF), D ** -0.5, 0.125, ((0, 16), (1, 2))),
        "down_weight": scatter_about(splits[18], (FF, D), FF ** -0.5, 0.078125, ((0, 2), (1, 16))),
    }


def block_scan(query, key_rows, value, gating):
    tokens = query.shape[0]
    attention_tally = gating.shape[1]
    key_size = query.shape[1] // attention_tally
    value_size = value.shape[1] // attention_tally
    nblocks = tokens // BLOCK
    scale = key_size ** (-0.5)
    queries = query.astype(jnp.float32).reshape(nblocks, BLOCK, attention_tally, key_size)
    keys_all = key_rows.astype(jnp.float32).reshape(nblocks, BLOCK, attention_tally, key_size)
    values_all = value.astype(jnp.float32).reshape(nblocks, BLOCK, attention_tally, value_size)
    incoming_matrix = jnp.moveaxis(gating[0].reshape(attention_tally, nblocks, BLOCK), 1, 0)
    forget_log = jax.nn.log_sigmoid(gating[1]) + gating[2]
    forgets = jnp.moveaxis(forget_log.reshape(attention_tally, nblocks, BLOCK), 1, 0)
    causal = jnp.tril(jnp.ones((BLOCK, BLOCK), dtype=bool))

    def advance(carry, blocks):
        memory, level = carry
        q_block, k_block, v_block, in_block, f_block = blocks
        cumul = jnp.cumsum(f_block, axis=-1)
        logits = cumul[:, :, None] - cumul[:, None, :] + in_block[:, None, :]
        logits = jnp.where(causal, logits, -jnp.inf)
        carried = cumul + level[:, None]
        stab = jnp.maximum(carried, lax.optimization_barrier(jnp.max(logits, axis=-1)))
        weights = jnp.exp(logits - stab[:, :, None])
        scores = jnp.einsum('thd,shd->hts', q_block, k_block) * scale
        weighted = (scores * weights).astype(jnp.bfloat16).astype(jnp.float32)
        within = jnp.einsum('hts,shv->thv', weighted, v_block)
        earlier = jnp.einsum('thd,hdv->thv', q_block, memory, precision=lax.Precision.HIGHEST)
        earlier = earlier * jnp.exp(carried - stab).T[:, :, None]
        last = cumul[:, -1]
        tail = last[:, None] - cumul + in_block
        level_new = jnp.maximum(last + level, lax.optimization_barrier(jnp.max(tail, axis=-1)))
        tail_weights = jnp.exp(tail - level_new[:, None]) * scale
        scaled_keys = (k_block * tail_weights.T[:, :, None]).astype(jnp.bfloat16).astype(jnp.float32)
        memory_new = jnp.exp(last + level - level_new)[:, None, None] * memory
        memory_new = memory_new + jnp.einsum('shd,shv->hdv', scaled_keys, v_block)
        return ((memory_new, level_new), within + earlier)
    init = (jnp.zeros((attention_tally, key_size, value_size), jnp.float32), jnp.full((attention_tally,), -1e+30, jnp.float32))
    _, raw = lax.scan(advance, init, (queries, keys_all, values_all, incoming_matrix, forgets))
    return raw.reshape(tokens, attention_tally, value_size)

def finish(raw, gain, outgate):
    tokens, attention_tally, value_size = raw.shape
    normal_raw = raw * lax.rsqrt(lax.optimization_barrier(jnp.mean(raw * raw, axis=-1, keepdims=True)) + 1e-06)
    flat = normal_raw.reshape(tokens, attention_tally * value_size)
    flat = flat * gain.astype(jnp.float32) * jax.nn.sigmoid(outgate.astype(jnp.float32))
    return flat.astype(jnp.bfloat16)

def reference(residual, query_wide, key_wide, value_wide, outgate_wide, gating_wide, gain_wide, readout_wide, query_narrow, key_narrow, value_narrow, outgate_narrow, gating_narrow, gain_narrow, readout_narrow, norm_gain, gate_weight, up_weight, down_weight):
    gated_wide = finish(block_scan(query_wide, key_wide, value_wide, gating_wide), gain_wide, outgate_wide)
    gated_narrow = finish(block_scan(query_narrow, key_narrow, value_narrow, gating_narrow), gain_narrow, outgate_narrow)
    span_wide = gated_wide.shape[1] // N_TP
    span_narrow = gated_narrow.shape[1] // N_TP
    mixed = jnp.zeros(residual.shape, jnp.float32)
    for index in range(N_TP):
        part = jnp.dot(gated_wide[:, index * span_wide:(index + 1) * span_wide], readout_wide[index * span_wide:(index + 1) * span_wide], preferred_element_type=jnp.float32)
        part = part + jnp.dot(gated_narrow[:, index * span_narrow:(index + 1) * span_narrow], readout_narrow[index * span_narrow:(index + 1) * span_narrow], preferred_element_type=jnp.float32)
        mixed = mixed + part.astype(jnp.bfloat16).astype(jnp.float32)
    middle = (residual.astype(jnp.float32) + mixed).astype(jnp.bfloat16)
    middle_f = middle.astype(jnp.float32)
    normed = middle_f * lax.rsqrt(lax.optimization_barrier(jnp.mean(middle_f * middle_f, axis=-1, keepdims=True)) + 1e-06)
    normed = (normed * norm_gain.astype(jnp.float32)).astype(jnp.bfloat16)
    hidden_span = FF // N_TP
    back = jnp.zeros(residual.shape, jnp.float32)
    for index in range(N_TP):
        cols = slice(index * hidden_span, (index + 1) * hidden_span)
        gate = jnp.dot(normed, gate_weight[:, cols], preferred_element_type=jnp.float32)
        upper = jnp.dot(normed, up_weight[:, cols], preferred_element_type=jnp.float32)
        hidden = (jax.nn.silu(gate) * upper).astype(jnp.bfloat16)
        part = jnp.dot(hidden, down_weight[cols], preferred_element_type=jnp.float32)
        back = back + part.astype(jnp.bfloat16).astype(jnp.float32)
    return (middle_f + back).astype(jnp.bfloat16)
```

```python
import functools

import jax
import jax.numpy as jnp
from jax import lax
from jax.experimental import pallas as pl
from jax.experimental.pallas import tpu as pltpu
from jax.sharding import Mesh, PartitionSpec as P

DK_A = 128
DK_B = 64
LOW = -1e30
MESH = pl.DeviceIdType.MESH


def cell_kernel(
    n,
    q_w,
    k_w,
    v_w,
    og_w,
    gain_w,
    q_n,
    k_n,
    v_n,
    og_n,
    gain_n,
    gating,
    out_w,
    out_n,
    raw_w,
    raw_n,
    stabs,
    sent,
    got,
    back,
    carried,
    mem_w,
    mem_n,
    state,
    levels,
    send_sem,
    recv_sem,
    send_sem2,
    recv_sem2,
):
    na, nb = lax.axis_size("a"), lax.axis_size("b")
    tp = lax.axis_index("tp")
    me = lax.axis_index("a") * nb + lax.axis_index("b")

    def where_is(index):
        return (index // nb, lax.rem(index, nb), tp)

    barrier = pltpu.get_barrier_semaphore()

    def greet(r, _):
        peer = lax.rem(me + r, n)
        pl.semaphore_signal(barrier, inc=1, device_id=where_is(peer), device_id_type=MESH)
        return 0

    lax.fori_loop(1, n, greet, 0)

    rows = q_w.shape[0]
    heads_p = gating.shape[1]
    groups = (
        (q_w, k_w, v_w, og_w, gain_w, out_w, raw_w, mem_w, DK_A),
        (q_n, k_n, v_n, og_n, gain_n, out_n, raw_n, mem_n, DK_B),
    )
    heads = tuple(g[0].shape[1] // g[8] for g in groups)
    parts = tuple(h * g[8] // n for h, g in zip(heads, groups))
    starts = (0, parts[0])
    extra = parts[0] + parts[1]

    it = lax.broadcasted_iota(jnp.int32, (rows, rows), 0)
    js = lax.broadcasted_iota(jnp.int32, (rows, rows), 1)
    upper = (it <= js).astype(jnp.float32)
    eye = (it == js).astype(jnp.float32)
    last_dims = (((1,), (1,)), ((), ()))
    first_dims = (((0,), (0,)), ((), ()))
    gate_in = gating[0]
    x = gating[1]
    forget = jnp.minimum(x, 0.0) - jnp.log1p(jnp.exp(-jnp.abs(x))) + gating[2]
    cum = jnp.dot(
        forget, upper, precision=lax.Precision.HIGHEST, preferred_element_type=jnp.float32
    )
    cum_t = lax.dot_general(
        eye, cum, last_dims, precision=lax.Precision.HIGHEST, preferred_element_type=jnp.float32
    )
    diff = gate_in - cum
    diff_t = lax.dot_general(
        eye, diff, last_dims, precision=lax.Precision.HIGHEST, preferred_element_type=jnp.float32
    )
    total = cum[:, rows - 1 : rows]
    level = jnp.max(total + diff, axis=1, keepdims=True)
    total_t = cum_t[rows - 1 : rows, :]
    level_t = jnp.max(total_t + diff_t, axis=0, keepdims=True)
    tail_t = jnp.exp(total_t + diff_t - level_t)
    width = sent.shape[2]
    lane = lax.broadcasted_iota(jnp.int32, (heads_p, width), 1)
    marks = jnp.where(
        lane < width // 2,
        jnp.broadcast_to(level, (heads_p, width)),
        jnp.broadcast_to(total, (heads_p, width)),
    )

    index = 0
    for g, (q, k, v, _, _, _, raw, _, dk) in enumerate(groups):
        dv = v.shape[1] // heads[g]
        scale = dk ** (-0.5)
        for h in range(heads[g]):
            k_h = k[:, h * dk : (h + 1) * dk]
            v_h = v[:, h * dv : (h + 1) * dv]
            scaled = k_h.astype(jnp.float32) * (tail_t[:, index : index + 1] * scale)
            memory = lax.dot_general(
                scaled.astype(jnp.bfloat16), v_h, first_dims, preferred_element_type=jnp.float32
            )
            size = parts[g]
            per = dk // size
            for p in range(per):
                sent[h * per + p, starts[g] : starts[g] + size, :dv] = memory[
                    p * size : (p + 1) * size
                ]
            index += 1
    spare = v_n.shape[1] // heads[1]
    if spare < width:
        sent[:, starts[1] : extra, spare:] = jnp.zeros((n, parts[1], width - spare), jnp.float32)
    for p in range(n):
        sent[p, extra : extra + heads_p, :] = marks

    pl.semaphore_wait(barrier, n - 1)

    def out_copy(r):
        peer = lax.rem(me + r, n)
        return pltpu.make_async_remote_copy(
            src_ref=sent.at[peer],
            dst_ref=got.at[me],
            send_sem=send_sem.at[r],
            recv_sem=recv_sem.at[r],
            device_id=where_is(peer),
            device_id_type=MESH,
        )

    lax.fori_loop(1, n, lambda r, c: (out_copy(r).start(), c)[1], 0)
    got[me] = sent[me]

    index = 0
    for g, (q, k, v, _, _, _, raw, _, dk) in enumerate(groups):
        dv = v.shape[1] // heads[g]
        scale = dk ** (-0.5)
        for h in range(heads[g]):
            q_h = q[:, h * dk : (h + 1) * dk]
            k_h = k[:, h * dk : (h + 1) * dk]
            v_h = v[:, h * dv : (h + 1) * dv]
            scores = lax.dot_general(q_h, k_h, last_dims, preferred_element_type=jnp.float32)
            logits = cum_t[:, index : index + 1] + diff[index : index + 1, :]
            logits = jnp.where(js <= it, logits, LOW)
            stab = jnp.max(logits, axis=1, keepdims=True)
            weighted = scores * scale * jnp.exp(logits - stab)
            raw[:, h * dv : (h + 1) * dv] = jnp.dot(
                weighted.astype(jnp.bfloat16), v_h, preferred_element_type=jnp.float32
            )
            stabs[:, index : index + 1] = stab
            index += 1

    lax.fori_loop(1, n, lambda r, c: (out_copy(r).wait(), c)[1], 0)

    which = tuple(
        (me * parts[g]) // groups[g][8] + (heads[0] if g else 0) for g in range(2)
    )
    sub = lax.broadcasted_iota(jnp.int32, (heads_p, width), 0)
    picks = tuple(sub == w for w in which)

    def merge(t, _):
        level_c = levels[0]
        back[t] = state[...]
        levels[1] = jnp.where(t == me, level_c, levels[1])
        mark = got[t, extra : extra + heads_p, :]
        lev = jnp.broadcast_to(mark[:, :1], mark.shape)
        tot = jnp.broadcast_to(mark[:, width - 1 :], mark.shape)
        new = jnp.maximum(level_c + tot, lev)
        old_f = jnp.exp(level_c + tot - new)
        new_f = jnp.exp(lev - new)
        levels[0] = new
        for g in range(2):
            span = slice(starts[g], starts[g] + parts[g])

            def pick(f):
                return jnp.sum(jnp.where(picks[g], f, 0.0), axis=0, keepdims=True)

            state[span, :] = pick(old_f) * state[span, :] + pick(new_f) * got[t, span, :]
        return 0

    levels[...] = jnp.full(levels.shape, LOW, jnp.float32)
    state[...] = jnp.zeros(state.shape, jnp.float32)
    lax.fori_loop(0, n, merge, 0)
    entering = levels[1]

    def back_copy(r):
        peer = lax.rem(me + r, n)
        return pltpu.make_async_remote_copy(
            src_ref=back.at[peer],
            dst_ref=carried.at[me],
            send_sem=send_sem2.at[r],
            recv_sem=recv_sem2.at[r],
            device_id=where_is(peer),
            device_id_type=MESH,
        )

    lax.fori_loop(1, n, lambda r, c: (back_copy(r).start(), c)[1], 0)
    carried[me] = back[me]
    entering_t = lax.dot_general(
        jnp.where(
            lax.broadcasted_iota(jnp.int32, (rows, width), 1) == 0, 1.0, 0.0
        ),
        entering,
        last_dims,
        precision=lax.Precision.HIGHEST,
        preferred_element_type=jnp.float32,
    )
    shifted = cum_t + entering_t
    own = stabs[:, :heads_p]
    both = jnp.maximum(own, shifted)
    own_f = jnp.exp(own - both)
    in_f = jnp.exp(shifted - both)
    lax.fori_loop(1, n, lambda r, c: (back_copy(r).wait(), c)[1], 0)

    index = 0
    for g, (q, _, v, og, gain, out, raw, mem, dk) in enumerate(groups):
        dv = v.shape[1] // heads[g]
        size = parts[g]
        per = dk // size
        for h in range(heads[g]):
            for p in range(per):
                mem[p * size : (p + 1) * size, :] = carried[
                    h * per + p, starts[g] : starts[g] + size, :dv
                ]
            memory = mem[...]
            high = memory.astype(jnp.bfloat16)
            rest = (memory - high.astype(jnp.float32)).astype(jnp.bfloat16)
            q_h = q[:, h * dk : (h + 1) * dk]
            cols = slice(h * dv, (h + 1) * dv)
            incoming = jnp.dot(q_h, high, preferred_element_type=jnp.float32) + jnp.dot(
                q_h, rest, preferred_element_type=jnp.float32
            )
            value = (
                raw[:, cols] * own_f[:, index : index + 1]
                + incoming * in_f[:, index : index + 1]
            )
            value = value * lax.rsqrt(jnp.mean(value * value, axis=1, keepdims=True) + 1e-06)
            gate = 1.0 / (1.0 + jnp.exp(-og[:, cols].astype(jnp.float32)))
            value = value * gain[:, cols].astype(jnp.float32) * gate
            out[:, cols] = value.astype(jnp.bfloat16)
            index += 1


def cell(q_w, k_w, v_w, og_w, gat_w, gain_w, q_n, k_n, v_n, og_n, gat_n, gain_n):
    n = lax.axis_size("a") * lax.axis_size("b")
    rows = q_w.shape[0]
    heads = gat_w.shape[1] + gat_n.shape[1]
    heads_p = -(-heads // 8) * 8
    gating = jnp.concatenate([gat_w, gat_n], axis=1)
    gating = jnp.pad(gating, ((0, 0), (0, heads_p - heads), (0, 0)))
    parts = (q_w.shape[1] // n, q_n.shape[1] // n)
    width = v_w.shape[1] // gat_w.shape[1]
    width_n = v_n.shape[1] // gat_n.shape[1]
    vmem = pl.BlockSpec(memory_space=pltpu.VMEM)
    state = parts[0] + parts[1]
    return pl.pallas_call(
        functools.partial(cell_kernel, n),
        out_shape=(
            jax.ShapeDtypeStruct(v_w.shape, jnp.bfloat16),
            jax.ShapeDtypeStruct(v_n.shape, jnp.bfloat16),
        ),
        in_specs=[vmem] * 11,
        out_specs=(vmem, vmem),
        scratch_shapes=[
            pltpu.VMEM(v_w.shape, jnp.float32),
            pltpu.VMEM(v_n.shape, jnp.float32),
            pltpu.VMEM((rows, 128), jnp.float32),
            pltpu.VMEM((n, state + heads_p, width), jnp.float32),
            pltpu.VMEM((n, state + heads_p, width), jnp.float32),
            pltpu.VMEM((n, state, width), jnp.float32),
            pltpu.VMEM((n, state, width), jnp.float32),
            pltpu.VMEM((DK_A, width), jnp.float32),
            pltpu.VMEM((DK_B, width_n), jnp.float32),
            pltpu.VMEM((state, width), jnp.float32),
            pltpu.VMEM((2, heads_p, width), jnp.float32),
            pltpu.SemaphoreType.DMA((n,)),
            pltpu.SemaphoreType.DMA((n,)),
            pltpu.SemaphoreType.DMA((n,)),
            pltpu.SemaphoreType.DMA((n,)),
        ],
        compiler_params=pltpu.CompilerParams(
            collective_id=0, has_side_effects=True, vmem_limit_bytes=32 * 2**20
        ),
        cost_estimate=pl.CostEstimate(
            flops=2 * 10**9, bytes_accessed=120 * 10**6, transcendentals=0
        ),
    )(
        q_w,
        k_w,
        v_w,
        og_w,
        gain_w.reshape(1, -1),
        q_n,
        k_n,
        v_n,
        og_n,
        gain_n.reshape(1, -1),
        gating,
    )


def layer_kernel(na, nb, *refs):
    (
        residual,
        q_w,
        k_w,
        v_w,
        og_w,
        gat_w,
        gain_w,
        read_w,
        q_n,
        k_n,
        v_n,
        og_n,
        gat_n,
        gain_n,
        read_n,
        norm_gain,
        gate,
        up,
        down,
        out,
        res_v,
        qw_v,
        kw_v,
        vw_v,
        ogw_v,
        gatw_v,
        gainw_v,
        qn_v,
        kn_v,
        vn_v,
        ogn_v,
        gatn_v,
        gainn_v,
        read_v,
        ngain_v,
        edge_v,
        gu_own,
        d_own,
        gu_all,
        d_all,
        gat_v,
        raw_w,
        raw_n,
        stabs,
        sent,
        got,
        mark,
        mark_got,
        prefix,
        total_s,
        total_got,
        tmark,
        tmark_got,
        enter,
        enter_mark,
        back,
        carried,
        bmark,
        bmark_got,
        gated,
        part,
        part_got,
        middle,
        x_all,
        acc,
        hidden,
        terms,
        terms_got,
        sums,
        sums_got,
        in_sem,
        p1_s,
        p1_r,
        p2_s,
        p2_r,
        p3_s,
        p3_r,
        z_s,
        z_r,
        f_s,
        f_r,
        g_s,
        g_r,
        t_s,
        t_r,
        x_s,
        x_r,
        y_s,
        y_r,
        r_s,
        r_r,
    ) = refs
    n = na * nb
    a, b, t = lax.axis_index("a"), lax.axis_index("b"), lax.axis_index("tp")
    me = a * nb + b
    f32, bf16 = jnp.float32, jnp.bfloat16

    barrier = pltpu.get_barrier_semaphore()
    peers = [(a ^ k, b, t) for k in range(1, na)]
    peers += [(a, b ^ m, t) for m in range(1, nb)]
    peers += [(a, b, 1 - t)]
    for peer in peers:
        pl.semaphore_signal(barrier, inc=1, device_id=peer, device_id_type=MESH)

    depth = gate.shape[0]
    chunk = gate.shape[1] // na
    whole = chunk // 128 * 128
    half = chunk - whole
    cols = down.shape[1]
    model = residual.shape[1]
    own_rows = residual.shape[0]
    rows = q_w.shape[0]
    kspan = nb * depth
    span = nb * cols
    wide_heads, narrow_heads = gat_w.shape[1], gat_n.shape[1]
    heads = wide_heads + narrow_heads
    dv_w = v_w.shape[1] // wide_heads
    dv_n = v_n.shape[1] // narrow_heads

    def local(src, dst, i):
        copy = pltpu.make_async_copy(src, dst, in_sem.at[i])
        copy.start()
        return copy

    loads = {}
    loads["gat"] = [local(gat_w, gatw_v, 0), local(gat_n, gatn_v, 1)]
    loads["k"] = [
        local(k_w, kw_v, 2),
        local(k_n, kn_v, 3),
        local(v_w, vw_v, 4),
        local(v_n, vn_v, 5),
    ]

    def slab_parts(c):
        odd = c % 2
        return c * chunk + odd * half, c * chunk + (1 - odd) * whole

    def d_slab(r, lo=0, size=chunk):
        return d_all.at[
            r // 2, pl.ds(lo, size), pl.ds(pl.multiple_of(lax.rem(r, 2) * cols, cols), cols)
        ]

    first, second = slab_parts(a)
    own_down = (
        pltpu.make_async_copy(
            down.at[pl.ds(pl.multiple_of(first, half), whole)],
            d_slab(me, 0, whole),
            in_sem.at[6],
        ),
        pltpu.make_async_copy(
            down.at[pl.ds(pl.multiple_of(second, half), half)],
            d_slab(me, whole, half),
            in_sem.at[7],
        ),
    )
    for c in own_down:
        c.start()
    for c in range(na):
        lo, hi = slab_parts(c)
        pltpu.make_async_copy(
            down.at[lo : lo + whole], d_own.at[c, 0:whole], in_sem.at[8]
        ).start()
        pltpu.make_async_copy(
            down.at[hi : hi + half], d_own.at[c, whole:chunk], in_sem.at[8]
        ).start()
    for i, w in enumerate((gate, up)):
        for c in range(na):
            lo, _ = slab_parts(c)
            pltpu.make_async_copy(
                w.at[:, lo : lo + whole],
                gu_own.at[c, :, i * whole : (i + 1) * whole],
                in_sem.at[9],
            ).start()
        for c in range(na // 2):
            lo = 2 * c * chunk + whole
            pltpu.make_async_copy(
                w.at[:, lo : lo + 128], edge_v.at[i, c], in_sem.at[10]
            ).start()
    loads["q"] = [local(q_w, qw_v, 11), local(q_n, qn_v, 12)]
    loads["og"] = [
        local(og_w, ogw_v, 13),
        local(og_n, ogn_v, 14),
        local(gain_w, gainw_v, 15),
        local(gain_n, gainn_v, 16),
    ]
    loads["read"] = [
        local(read_w, read_v.at[: read_w.shape[0]], 17),
        local(read_n, read_v.at[read_w.shape[0] :], 18),
        local(residual, res_v, 19),
        local(norm_gain, ngain_v, 20),
    ]

    started = []

    def remote(src, dst, s_sem, r_sem, peer):
        return pltpu.make_async_remote_copy(
            src_ref=src,
            dst_ref=dst,
            send_sem=s_sem,
            recv_sem=r_sem,
            device_id=peer,
            device_id_type=MESH,
        )

    def go(copy):
        copy.start()
        started.append(copy)

    def slab(kind, r, lo, size):
        if kind == 0:
            return gu_all.at[r, pl.ds(lo, size)]
        return d_slab(r, lo, size)

    extent = (depth, chunk)

    def z_copy(kind, k, r):
        src = (gu_own, d_own)[kind].at[a ^ k]
        return remote(
            src, slab(kind, r, 0, extent[kind]), z_s.at[kind, k], z_r.at[kind, k], (a ^ k, b, t)
        )

    def z_start(kind, k):
        go(z_copy(kind, k, me))

    def z_wait(kind, k):
        z_copy(kind, k, (a ^ k) * nb + b).wait_recv()

    def full_copy(kind, s, d, h, who):
        size = extent[kind] // 2
        ref = slab(kind, (a ^ s) * nb + who, h * size, size)
        return remote(
            ref, ref, f_s.at[kind, s, d, h], f_r.at[kind, s, d, h], (a, b ^ (1 << d), t)
        )

    def full_start(kind, s, h):
        for d in range(2):
            go(full_copy(kind, s, d, h, b))

    def full_wait(kind, s, d, h):
        full_copy(kind, s, d, h, b ^ (1 << d)).wait_recv()

    def diag_copy(kind, s, h, who):
        size = extent[kind] // 2
        ref = slab(kind, (a ^ s) * nb + who, h * size, size)
        return remote(ref, ref, g_s.at[kind, s, h], g_r.at[kind, s, h], (a, b ^ (2 >> h), t))

    def relay(kind, s):
        for h in range(2):
            full_wait(kind, s, h, h)
            go(diag_copy(kind, s, h, b ^ (1 << h)))

    def arrived(kind, s):
        for h in range(2):
            full_wait(kind, s, 1 - h, h)
            diag_copy(kind, s, h, b ^ 3).wait_recv()

    for c in loads["gat"]:
        c.wait()
    gat_v[:, :wide_heads, :] = gatw_v[...]
    gat_v[:, wide_heads:, :] = gatn_v[...]
    it = lax.broadcasted_iota(jnp.int32, (rows, rows), 0)
    js = lax.broadcasted_iota(jnp.int32, (rows, rows), 1)
    upper = (it <= js).astype(f32)
    eye = (it == js).astype(f32)
    last_dims = (((1,), (1,)), ((), ()))
    first_dims = (((0,), (0,)), ((), ()))
    exact = dict(precision=lax.Precision.HIGHEST, preferred_element_type=f32)
    gate_in = gat_v[0]
    x = gat_v[1]
    forget = jnp.minimum(x, 0.0) - jnp.log1p(jnp.exp(-jnp.abs(x))) + gat_v[2]
    cum = jnp.dot(forget, upper, **exact)
    cum_t = lax.dot_general(eye, cum, last_dims, **exact)
    diff = gate_in - cum
    diff_t = lax.dot_general(eye, diff, last_dims, **exact)
    total = cum[:, rows - 1 : rows]
    level = jnp.max(total + diff, axis=1, keepdims=True)
    total_t = cum_t[rows - 1 : rows, :]
    level_t = jnp.max(total_t + diff_t, axis=0, keepdims=True)
    tail_t = jnp.exp(total_t + diff_t - level_t)
    lane = lax.broadcasted_iota(jnp.int32, (heads, 128), 1)
    mark[...] = jnp.where(
        lane < 64, jnp.broadcast_to(level, (heads, 128)), jnp.broadcast_to(total, (heads, 128))
    )

    groups = (
        (qw_v, kw_v, vw_v, ogw_v, gainw_v, raw_w, DK_A, dv_w, wide_heads, 0),
        (qn_v, kn_v, vn_v, ogn_v, gainn_v, raw_n, DK_B, dv_n, narrow_heads, wide_heads),
    )
    fold = DK_B // 2
    deep = DK_A + fold

    for c in own_down:
        c.wait()
    pltpu.make_async_copy(d_own, d_own, in_sem.at[8]).wait()
    pl.semaphore_wait(barrier, len(peers))
    full_start(1, 0, 0)
    full_start(1, 0, 1)
    z_start(1, 1)

    for c in loads["k"]:
        c.wait()
    for _, k, v, _, _, _, dk, dv, count, base in groups:
        scale = dk ** (-0.5)
        for h in range(count):
            i = base + h
            scaled = k[:, h * dk : (h + 1) * dk].astype(f32) * (tail_t[:, i : i + 1] * scale)
            memory = lax.dot_general(
                scaled.astype(bf16),
                v[:, h * dv : (h + 1) * dv],
                first_dims,
                preferred_element_type=f32,
            ).astype(bf16)
            if base == 0:
                sent[h, :dk, :] = memory
            else:
                sent[h, DK_A:deep, :dv] = memory[:fold]
                sent[h, DK_A:deep, dv:] = memory[fold:]

    def p1(m, r):
        peer = (a, b ^ m, t)
        return (
            remote(mark, mark_got.at[r], p1_s.at[0, m], p1_r.at[0, m], peer),
            remote(sent.at[b ^ m], got.at[r], p1_s.at[1, m], p1_r.at[1, m], peer),
        )

    for m in range(1, nb):
        for c in p1(m, b):
            go(c)
    got[b] = sent[b]
    mark_got[b] = mark[...]

    pltpu.make_async_copy(
        gu_own.at[:, :, : 2 * whole], gu_own.at[:, :, : 2 * whole], in_sem.at[9]
    ).wait()
    pltpu.make_async_copy(edge_v, edge_v, in_sem.at[10]).wait()
    for c in range(na // 2):
        ge, ue = edge_v[0, c], edge_v[1, c]
        gu_own[2 * c, :, 2 * whole :] = jnp.concatenate([ge[:, :half], ue[:, :half]], axis=1)
        gu_own[2 * c + 1, :, 2 * whole :] = jnp.concatenate([ge[:, half:], ue[:, half:]], axis=1)
    gu_all[me] = gu_own[a]
    full_start(0, 0, 0)
    full_start(0, 0, 1)
    z_start(0, 1)

    for c in loads["q"]:
        c.wait()
    for q, k, v, _, _, raw, dk, dv, count, base in groups:
        scale = dk ** (-0.5)
        for h in range(count):
            i = base + h
            q_h = q[:, h * dk : (h + 1) * dk]
            k_h = k[:, h * dk : (h + 1) * dk]
            v_h = v[:, h * dv : (h + 1) * dv]
            scores = lax.dot_general(q_h, k_h, last_dims, preferred_element_type=f32)
            logits = cum_t[:, i : i + 1] + diff[i : i + 1, :]
            logits = jnp.where(js <= it, logits, LOW)
            stab = jnp.max(logits, axis=1, keepdims=True)
            weighted = scores * scale * jnp.exp(logits - stab)
            raw[:, h * dv : (h + 1) * dv] = jnp.dot(
                weighted.astype(bf16), v_h, preferred_element_type=f32
            )
            stabs[:, i : i + 1] = stab

    for m in range(1, nb):
        for c in p1(m, b ^ m):
            c.wait_recv()
    spans = ((0, DK_A), (DK_A, deep))

    def read_mark(ref, where, row):
        line = ref[where, pl.ds(row, 1), :]
        return line[:, :1], line[:, 127:128]

    run = []
    for g, (lo, hi) in enumerate(spans):
        lev, tot = read_mark(mark_got, 0, b + g * wide_heads)
        state = got[0, lo:hi, :].astype(f32)
        run.append([(lev, tot)])
        for j in range(1, nb):
            prefix[j - 1, lo:hi, :] = state
            lev2, tot2 = read_mark(mark_got, j, b + g * wide_heads)
            new = jnp.maximum(lev + tot2, lev2)
            state = (
                jnp.exp(lev + tot2 - new) * state
                + jnp.exp(lev2 - new) * got[j, lo:hi, :].astype(f32)
            )
            lev, tot = new, tot + tot2
            run[g].append((lev, tot))
        total_s[lo:hi, :] = state.astype(bf16)
    lane1 = lax.broadcasted_iota(jnp.int32, (1, 128), 1)
    for g in range(2):
        lev, tot = run[g][nb - 1]
        tmark[g : g + 1, :] = jnp.where(
            lane1 < 64, jnp.broadcast_to(lev, (1, 128)), jnp.broadcast_to(tot, (1, 128))
        )

    def p2(k, r):
        peer = (a ^ k, b, t)
        return (
            remote(tmark, tmark_got.at[r], p2_s.at[0, k], p2_r.at[0, k], peer),
            remote(total_s, total_got.at[r], p2_s.at[1, k], p2_r.at[1, k], peer),
        )

    for k in range(1, na):

        @pl.when((a ^ k) > a)
        def _():
            for c in p2(k, a):
                c.start()

    z_start(0, 2)
    z_start(0, 3)
    relay(1, 0)
    z_wait(0, 1)
    full_start(0, 1, 0)
    relay(0, 0)

    enter[...] = jnp.zeros(enter.shape, f32)
    enter_mark[...] = jnp.full(enter_mark.shape, LOW, f32)
    for k in range(1, na):

        @pl.when((a ^ k) < a)
        def _():
            for c in p2(k, a ^ k):
                c.wait_recv()

    for z in range(na - 1):

        @pl.when(z < a)
        def _():
            for g, (lo, hi) in enumerate(spans):
                lev = enter_mark[g : g + 1, :1]
                lev2, tot2 = read_mark(tmark_got, z, g)
                new = jnp.maximum(lev + tot2, lev2)
                enter[lo:hi, :] = (
                    jnp.exp(lev + tot2 - new) * enter[lo:hi, :]
                    + jnp.exp(lev2 - new) * total_got[z, lo:hi, :].astype(f32)
                )
                enter_mark[g : g + 1, :] = jnp.broadcast_to(new, (1, 128))

    for g, (lo, hi) in enumerate(spans):
        lev = enter_mark[g : g + 1, :1]
        back[0, lo:hi, :] = enter[lo:hi, :].astype(bf16)
        bmark[0, g : g + 1, :] = jnp.broadcast_to(lev, (1, 128))
        for j in range(1, nb):
            lev2, tot2 = run[g][j - 1]
            new = jnp.maximum(lev + tot2, lev2)
            back[j, lo:hi, :] = (
                jnp.exp(lev + tot2 - new) * enter[lo:hi, :]
                + jnp.exp(lev2 - new) * prefix[j - 1, lo:hi, :]
            ).astype(bf16)
            bmark[j, g : g + 1, :] = jnp.broadcast_to(new, (1, 128))

    def p3(m, r):
        peer = (a, b ^ m, t)
        return (
            remote(bmark.at[b ^ m], bmark_got.at[r], p3_s.at[0, m], p3_r.at[0, m], peer),
            remote(back.at[b ^ m], carried.at[r], p3_s.at[1, m], p3_r.at[1, m], peer),
        )

    for m in range(1, nb):
        for c in p3(m, b):
            go(c)
    carried[b] = back[b]
    bmark_got[b] = bmark[b]
    full_start(0, 1, 1)

    for c in loads["og"]:
        c.wait()
    for m in range(1, nb):
        for c in p3(m, b ^ m):
            c.wait_recv()

    for g, (q, _, _, og, gain, raw, dk, dv, count, base) in enumerate(groups):
        for h in range(count):
            i = base + h
            if g == 0:
                memory = carried[h, :dk, :]
            else:
                memory = jnp.concatenate(
                    [carried[h, DK_A:deep, :dv], carried[h, DK_A:deep, dv:]], axis=0
                )
            own = stabs[:, i : i + 1]
            shifted = cum_t[:, i : i + 1] + bmark_got[h, g : g + 1, :1]
            both = jnp.maximum(own, shifted)
            span_h = slice(h * dv, (h + 1) * dv)
            incoming = jnp.dot(
                q[:, h * dk : (h + 1) * dk], memory, preferred_element_type=f32
            )
            value = raw[:, span_h] * jnp.exp(own - both) + incoming * jnp.exp(shifted - both)
            value = value * lax.rsqrt(jnp.mean(value * value, axis=1, keepdims=True) + 1e-06)
            gate_h = 1.0 / (1.0 + jnp.exp(-og[:, span_h].astype(f32)))
            value = value * gain[:, span_h].astype(f32) * gate_h
            lo = g * raw_w.shape[1] + h * dv
            gated[:, lo : lo + dv] = value.astype(bf16)

    relay(0, 1)
    z_wait(0, 2)
    full_start(0, 2, 0)
    full_start(0, 2, 1)

    for c in loads["read"]:
        c.wait()
    tile = model // 4
    for j in range(model // tile):
        sl = slice(j * tile, (j + 1) * tile)
        p = jnp.dot(gated[...], read_v[:, sl], preferred_element_type=f32).astype(bf16)
        part[:, :, sl] = p.reshape(2, own_rows, tile)
    partner = (a, b, 1 - t)
    swap = remote(part.at[1 - t], part_got, t_s.at[0], t_r.at[0], partner)
    go(swap)
    swap.wait_recv()
    mixed = part[t].astype(f32) + part_got[...].astype(f32)
    mid = (res_v[...].astype(f32) + mixed).astype(bf16)
    middle[...] = mid
    mid = mid.astype(f32)
    normed = mid * lax.rsqrt(jnp.mean(mid * mid, axis=-1, keepdims=True) + 1e-06)
    block = 2 * own_rows

    def row_block(z, core):
        return x_all.at[pl.ds(pl.multiple_of((z * 2 + core) * own_rows, own_rows), own_rows)]

    x_all[pl.ds(pl.multiple_of((a * 2 + t) * own_rows, own_rows), own_rows), :] = (
        normed * ngain_v[...].astype(f32)
    ).astype(bf16)

    def x_copy(k, z):
        return remote(row_block(z, t), row_block(z, t), x_s.at[k], x_r.at[k], (a ^ k, b, t))

    def y_copy(k, core):
        ref = row_block(a ^ k, core)
        return remote(ref, ref, y_s.at[k], y_r.at[k], partner)

    for k in range(1, na):
        go(x_copy(k, a))
    go(y_copy(0, t))
    z_start(1, 2)
    z_start(1, 3)

    width = gu_all.shape[2]
    tiles = [(lo, min(lo + 512, width)) for lo in range(0, width, 512)]

    def unit(lo, m, s, fresh):
        z = a ^ s
        xs = x_all[pl.ds(lo, m), pl.ds(pl.multiple_of(z * kspan, kspan), kspan)]
        for c0, c1 in tiles:
            w = gu_all[pl.ds(z * nb, nb), :, c0:c1].reshape(kspan, c1 - c0)
            p = jnp.dot(xs, w, preferred_element_type=f32)
            if fresh:
                acc[pl.ds(lo, m), c0:c1] = p
            else:
                acc[pl.ds(lo, m), c0:c1] += p

    def row_unit(k, s, fresh):
        unit(pl.multiple_of((a ^ k) * block, block), block, s, fresh)

    arrived(0, 0)
    y_copy(0, 1 - t).wait_recv()
    row_unit(0, 0, True)
    arrived(0, 1)
    row_unit(0, 1, False)
    for k in range(1, na):
        if k == 1:
            z_wait(0, 3)
            full_start(0, 3, 0)
            full_start(0, 3, 1)
            relay(0, 2)
        if k == 2:
            z_wait(1, 1)
            full_start(1, 1, 0)
            full_start(1, 1, 1)
        x_copy(k, a ^ k).wait_recv()
        go(y_copy(k, t))
        if k == 3:
            relay(0, 3)
        y_copy(k, 1 - t).wait_recv()
        row_unit(k, 0, True)
        row_unit(k, 1, False)
    z_wait(1, 2)
    full_start(1, 2, 0)
    full_start(1, 2, 1)
    relay(1, 1)
    arrived(0, 2)
    total_rows = na * block
    unit(0, total_rows, 2, False)
    z_wait(1, 3)
    full_start(1, 3, 0)
    full_start(1, 3, 1)
    relay(1, 2)
    arrived(0, 3)
    unit(0, total_rows, 3, False)

    for j in range(2):
        sl = slice(j * total_rows // 2, (j + 1) * total_rows // 2)
        gt = acc[sl, :whole]
        hidden[sl, :whole] = (
            gt * (1.0 / (1.0 + jnp.exp(-gt))) * acc[sl, whole : 2 * whole]
        ).astype(bf16)
        mx = acc[sl, 2 * whole :]
        hx = mx * (1.0 / (1.0 + jnp.exp(-mx))) * pltpu.roll(mx, half, 1)
        hidden[sl, whole:] = hx[:, :half].astype(bf16)
    relay(1, 3)

    def t_copy(s):
        return remote(
            terms.at[s, :, 1 - t], terms_got.at[s], t_s.at[1 + s], t_r.at[1 + s], partner
        )

    def down_group(s):
        arrived(1, s)
        for p in range(nb // 2):
            w = d_all[(a ^ s) * (nb // 2) + p]
            v = jnp.dot(hidden[...], w, preferred_element_type=f32).astype(bf16)
            terms[s, :, :, :, p * 2 * cols : (p + 1) * 2 * cols] = v.reshape(
                na, 2, own_rows, 2 * cols
            )
        go(t_copy(s))

    def r_copy(k, s, z):
        c0 = pl.multiple_of((z ^ s) * span, span)
        return remote(
            sums.at[s, a ^ k],
            sums_got.at[k, :, pl.ds(c0, span)],
            r_s.at[k, s],
            r_r.at[k, s],
            (a ^ k, b, t),
        )

    def sum_group(s):
        t_copy(s).wait_recv()
        sums[s] = (terms[s, :, t].astype(f32) + terms_got[s].astype(f32)).astype(bf16)
        for k in range(1, na):
            go(r_copy(k, s, a))

    for s in range(na):
        down_group(s)
        if s > 0:
            sum_group(s - 1)
    sum_group(na - 1)
    for s in range(na):
        for k in range(1, na):
            r_copy(k, s, a ^ k).wait_recv()
    for s in range(na):
        c0 = pl.ds(pl.multiple_of((a ^ s) * span, span), span)
        v = sums[s, a].astype(f32)
        for k in range(1, na):
            v = v + sums_got[k, :, c0].astype(f32)
        out[:, c0] = (middle[:, c0].astype(f32) + v).astype(bf16)

    for c in started:
        c.wait_send()
    for k in range(1, na):

        @pl.when((a ^ k) > a)
        def _():
            for c in p2(k, a):
                c.wait_send()


def layer(na, nb, *args):
    (res, q_w, k_w, v_w, og_w, gat_w, gain_w, read_w) = args[:8]
    (q_n, k_n, v_n, og_n, gat_n, gain_n, read_n, norm_gain, gate, up, down) = args[8:]
    bf16, f32 = jnp.bfloat16, jnp.float32
    n = na * nb
    depth = gate.shape[0]
    chunk = gate.shape[1] // na
    whole = chunk // 128 * 128
    width = 2 * whole + 128
    cols = down.shape[1]
    own_rows, model = res.shape
    rows = q_w.shape[0]
    heads = gat_w.shape[1] + gat_n.shape[1]
    deep = DK_A + DK_B // 2
    dv = v_w.shape[1] // gat_w.shape[1]
    total_rows = na * 2 * own_rows
    span = nb * cols

    def vm(shape, dtype=bf16):
        return pltpu.VMEM(shape, dtype)

    def like(x):
        return pltpu.VMEM(x.shape, x.dtype)

    dma = pltpu.SemaphoreType.DMA
    gain_w, gain_n, norm_gain = (g.reshape(1, -1) for g in (gain_w, gain_n, norm_gain))
    scratch = [
        like(res),
        like(q_w),
        like(k_w),
        like(v_w),
        like(og_w),
        like(gat_w),
        like(gain_w),
        like(q_n),
        like(k_n),
        like(v_n),
        like(og_n),
        like(gat_n),
        like(gain_n),
        vm((read_w.shape[0] + read_n.shape[0], model)),
        like(norm_gain),
        vm((2, na // 2, depth, 128)),
        vm((na, depth, width)),
        vm((na, chunk, cols)),
        vm((n, depth, width)),
        vm((n // 2, chunk, 2 * cols)),
        vm((3, heads, rows), f32),
        vm(v_w.shape, f32),
        vm(v_n.shape, f32),
        vm((rows, 128), f32),
        vm((nb, deep, dv)),
        vm((nb, deep, dv)),
        vm((heads, 128), f32),
        vm((nb, heads, 128), f32),
        vm((nb - 1, deep, dv), f32),
        vm((deep, dv)),
        vm((na, deep, dv)),
        vm((8, 128), f32),
        vm((na, 8, 128), f32),
        vm((deep, dv), f32),
        vm((8, 128), f32),
        vm((nb, deep, dv)),
        vm((nb, deep, dv)),
        vm((nb, 8, 128), f32),
        vm((nb, 8, 128), f32),
        vm((rows, v_w.shape[1] + v_n.shape[1])),
        vm((2, own_rows, model)),
        vm((own_rows, model)),
        vm((own_rows, model)),
        vm((total_rows, model)),
        vm((total_rows, width), f32),
        vm((total_rows, chunk)),
        vm((na, na, 2, own_rows, span)),
        vm((na, na, own_rows, span)),
        vm((na, na, own_rows, span)),
        vm((na, own_rows, model)),
        dma((21,)),
        dma((2, nb)),
        dma((2, nb)),
        dma((2, na)),
        dma((2, na)),
        dma((2, nb)),
        dma((2, nb)),
        dma((2, na)),
        dma((2, na)),
        dma((2, na, 2, 2)),
        dma((2, na, 2, 2)),
        dma((2, na, 2)),
        dma((2, na, 2)),
        dma((1 + na,)),
        dma((1 + na,)),
        dma((na,)),
        dma((na,)),
        dma((na,)),
        dma((na,)),
        dma((na, na)),
        dma((na, na)),
    ]
    hbm = pl.BlockSpec(memory_space=pl.ANY)
    return pl.pallas_call(
        functools.partial(layer_kernel, na, nb),
        out_shape=jax.ShapeDtypeStruct(res.shape, bf16),
        in_specs=[hbm] * 19,
        out_specs=pl.BlockSpec(memory_space=pltpu.VMEM),
        scratch_shapes=scratch,
        compiler_params=pltpu.CompilerParams(
            collective_id=0, has_side_effects=True, vmem_limit_bytes=60 * 2**20
        ),
    )(
        res,
        q_w,
        k_w,
        v_w,
        og_w,
        gat_w,
        gain_w,
        read_w,
        q_n,
        k_n,
        v_n,
        og_n,
        gat_n,
        gain_n,
        read_n,
        norm_gain,
        gate,
        up,
        down,
    )


def fits(mesh_shape, args):
    na, nb, ntp = mesh_shape
    gate, gat_w, gat_n = args[16], args[5], args[12]
    q_w, v_w, v_n = args[1], args[3], args[10]
    heads_w, heads_n = gat_w.shape[1], gat_n.shape[1]
    return (
        na == nb == 4
        and ntp == 2
        and gate.shape[1] % na == 0
        and gate.shape[1] // na % 128 == 64
        and heads_w == heads_n == nb
        and q_w.shape[0] == 128
        and v_w.shape[1] // heads_w == 2 * (v_n.shape[1] // heads_n)
    )


def passed(block, axis, step):
    size = lax.axis_size(axis)
    if step % size == 0:
        return block
    return lax.ppermute(block, axis, [(i, (i + step) % size) for i in range(size)])


def gathered(block, axis):
    return jnp.concatenate([passed(block, axis, r) for r in range(lax.axis_size(axis))], axis=0)


def returned(blocks, axis):
    size = lax.axis_size(axis)
    rows = blocks.shape[0] // size
    pieces = [passed(blocks[r * rows : (r + 1) * rows], axis, -r) for r in range(size)]
    return sum(p.astype(jnp.float32) for p in pieces)


def plain_body(
    residual,
    query_wide,
    key_wide,
    value_wide,
    outgate_wide,
    gating_wide,
    gain_wide,
    readout_wide,
    query_narrow,
    key_narrow,
    value_narrow,
    outgate_narrow,
    gating_narrow,
    gain_narrow,
    readout_narrow,
    norm_gain,
    gate_weight,
    up_weight,
    down_weight,
):
    na, nb = lax.axis_size("a"), lax.axis_size("b")
    depth, hidden_tp = gate_weight.shape
    chunk = hidden_tp // na
    out_cols = down_weight.shape[1]
    model = residual.shape[1]

    def spread(pieces):
        return lax.all_to_all(pieces, "a", split_axis=0, concat_axis=0, tiled=True)

    mine = (
        spread(jnp.moveaxis(gate_weight.reshape(depth, na, chunk), 1, 0)),
        spread(jnp.moveaxis(up_weight.reshape(depth, na, chunk), 1, 0)),
        spread(down_weight.reshape(na, chunk, out_cols)),
    )
    gate_all, up_all, down_all = (
        lax.all_gather(m, "b", axis=0, tiled=True) for m in mine
    )
    *_, gating_wide, gating_narrow = lax.optimization_barrier(
        (*mine, gating_wide, gating_narrow)
    )

    gated_w, gated_n = cell(
        query_wide,
        key_wide,
        value_wide,
        outgate_wide,
        gating_wide,
        gain_wide,
        query_narrow,
        key_narrow,
        value_narrow,
        outgate_narrow,
        gating_narrow,
        gain_narrow,
    )
    partial = (
        jnp.dot(gated_w, readout_wide, preferred_element_type=jnp.float32)
        + jnp.dot(gated_n, readout_narrow, preferred_element_type=jnp.float32)
    ).astype(jnp.bfloat16)
    own_rows = residual.shape[0]
    ntp, core = lax.axis_size("tp"), lax.axis_index("tp")
    mixed = 0.0
    for r in range(ntp):
        block = lax.dynamic_slice_in_dim(partial, lax.rem(core + r, ntp) * own_rows, own_rows)
        mixed = mixed + passed(block, "tp", r).astype(jnp.float32)
    middle_f = (residual.astype(jnp.float32) + mixed).astype(jnp.bfloat16).astype(jnp.float32)
    normed = middle_f * lax.rsqrt(jnp.mean(middle_f * middle_f, axis=-1, keepdims=True) + 1e-06)
    normed = (normed * norm_gain.astype(jnp.float32)).astype(jnp.bfloat16)
    own_rows = normed.shape[0]
    normed = normed.reshape(own_rows, na, nb, depth).swapaxes(1, 2).reshape(own_rows, model)
    all_rows = gathered(gathered(normed, "a"), "tp")
    gate = jnp.dot(all_rows, gate_all.reshape(model, chunk), preferred_element_type=jnp.float32)
    upper = jnp.dot(all_rows, up_all.reshape(model, chunk), preferred_element_type=jnp.float32)
    hidden = (jax.nn.silu(gate) * upper).astype(jnp.bfloat16)
    down = jnp.transpose(down_all, (1, 0, 2)).reshape(chunk, model)
    terms = jnp.dot(hidden, down, preferred_element_type=jnp.float32)
    back = returned(returned(terms.astype(jnp.bfloat16), "tp").astype(jnp.bfloat16), "a")
    back = back.reshape(own_rows, nb, na, out_cols).swapaxes(1, 2).reshape(own_rows, model)
    return (middle_f + back).astype(jnp.bfloat16)


def body(*args):
    sizes = tuple(lax.axis_size(x) for x in ("a", "b", "tp"))
    if fits(sizes, args):
        return layer(sizes[0], sizes[1], *args)
    return plain_body(*args)


def solution(mesh):
    sp, tp = mesh.shape["sp"], mesh.shape["tp"]
    a = 4 if sp % 4 == 0 else 1
    split = Mesh(mesh.devices.reshape(a, sp // a, tp), ("a", "b", "tp"))
    s = ("a", "b")
    in_specs = (
        P(("a", "b", "tp"), None),
        P(s, "tp"),
        P(s, "tp"),
        P(s, "tp"),
        P(s, "tp"),
        P(None, "tp", s),
        P("tp"),
        P("tp", None),
        P(s, "tp"),
        P(s, "tp"),
        P(s, "tp"),
        P(s, "tp"),
        P(None, "tp", s),
        P("tp"),
        P("tp", None),
        P(),
        P(s, "tp"),
        P(s, "tp"),
        P("tp", s),
    )
    out_specs = P(("a", "b", "tp"), None)
    return jax.shard_map(body, mesh=split, in_specs=in_specs, out_specs=out_specs, check_vma=False)
```

```python
import functools

import jax
import jax.numpy as jnp
from jax import lax
from jax.experimental import pallas as pl
from jax.experimental.pallas import tpu as pltpu
from jax.sharding import Mesh, PartitionSpec as P

DK_A = 128
DK_B = 64
LOW = -1e30
MESH = pl.DeviceIdType.MESH


def cell_kernel(
    n,
    q_w,
    k_w,
    v_w,
    og_w,
    gain_w,
    q_n,
    k_n,
    v_n,
    og_n,
    gain_n,
    gating,
    out_w,
    out_n,
    raw_w,
    raw_n,
    stabs,
    sent,
    got,
    back,
    carried,
    mem_w,
    mem_n,
    state,
    levels,
    send_sem,
    recv_sem,
    send_sem2,
    recv_sem2,
):
    na, nb = lax.axis_size("a"), lax.axis_size("b")
    tp = lax.axis_index("tp")
    me = lax.axis_index("a") * nb + lax.axis_index("b")

    def where_is(index):
        return (index // nb, lax.rem(index, nb), tp)

    barrier = pltpu.get_barrier_semaphore()

    def greet(r, _):
        peer = lax.rem(me + r, n)
        pl.semaphore_signal(barrier, inc=1, device_id=where_is(peer), device_id_type=MESH)
        return 0

    lax.fori_loop(1, n, greet, 0)

    rows = q_w.shape[0]
    heads_p = gating.shape[1]
    groups = (
        (q_w, k_w, v_w, og_w, gain_w, out_w, raw_w, mem_w, DK_A),
        (q_n, k_n, v_n, og_n, gain_n, out_n, raw_n, mem_n, DK_B),
    )
    heads = tuple(g[0].shape[1] // g[8] for g in groups)
    parts = tuple(h * g[8] // n for h, g in zip(heads, groups))
    starts = (0, parts[0])
    extra = parts[0] + parts[1]

    it = lax.broadcasted_iota(jnp.int32, (rows, rows), 0)
    js = lax.broadcasted_iota(jnp.int32, (rows, rows), 1)
    upper = (it <= js).astype(jnp.float32)
    eye = (it == js).astype(jnp.float32)
    last_dims = (((1,), (1,)), ((), ()))
    first_dims = (((0,), (0,)), ((), ()))
    gate_in = gating[0]
    x = gating[1]
    forget = jnp.minimum(x, 0.0) - jnp.log1p(jnp.exp(-jnp.abs(x))) + gating[2]
    cum = jnp.dot(
        forget, upper, precision=lax.Precision.HIGHEST, preferred_element_type=jnp.float32
    )
    cum_t = lax.dot_general(
        eye, cum, last_dims, precision=lax.Precision.HIGHEST, preferred_element_type=jnp.float32
    )
    diff = gate_in - cum
    diff_t = lax.dot_general(
        eye, diff, last_dims, precision=lax.Precision.HIGHEST, preferred_element_type=jnp.float32
    )
    total = cum[:, rows - 1 : rows]
    level = jnp.max(total + diff, axis=1, keepdims=True)
    total_t = cum_t[rows - 1 : rows, :]
    level_t = jnp.max(total_t + diff_t, axis=0, keepdims=True)
    tail_t = jnp.exp(total_t + diff_t - level_t)
    width = sent.shape[2]
    lane = lax.broadcasted_iota(jnp.int32, (heads_p, width), 1)
    marks = jnp.where(
        lane < width // 2,
        jnp.broadcast_to(level, (heads_p, width)),
        jnp.broadcast_to(total, (heads_p, width)),
    )

    index = 0
    for g, (q, k, v, _, _, _, raw, _, dk) in enumerate(groups):
        dv = v.shape[1] // heads[g]
        scale = dk ** (-0.5)
        for h in range(heads[g]):
            k_h = k[:, h * dk : (h + 1) * dk]
            v_h = v[:, h * dv : (h + 1) * dv]
            scaled = k_h.astype(jnp.float32) * (tail_t[:, index : index + 1] * scale)
            memory = lax.dot_general(
                scaled.astype(jnp.bfloat16), v_h, first_dims, preferred_element_type=jnp.float32
            )
            size = parts[g]
            per = dk // size
            for p in range(per):
                sent[h * per + p, starts[g] : starts[g] + size, :dv] = memory[
                    p * size : (p + 1) * size
                ]
            index += 1
    spare = v_n.shape[1] // heads[1]
    if spare < width:
        sent[:, starts[1] : extra, spare:] = jnp.zeros((n, parts[1], width - spare), jnp.float32)
    for p in range(n):
        sent[p, extra : extra + heads_p, :] = marks

    pl.semaphore_wait(barrier, n - 1)

    def out_copy(r):
        peer = lax.rem(me + r, n)
        return pltpu.make_async_remote_copy(
            src_ref=sent.at[peer],
            dst_ref=got.at[me],
            send_sem=send_sem.at[r],
            recv_sem=recv_sem.at[r],
            device_id=where_is(peer),
            device_id_type=MESH,
        )

    lax.fori_loop(1, n, lambda r, c: (out_copy(r).start(), c)[1], 0)
    got[me] = sent[me]

    index = 0
    for g, (q, k, v, _, _, _, raw, _, dk) in enumerate(groups):
        dv = v.shape[1] // heads[g]
        scale = dk ** (-0.5)
        for h in range(heads[g]):
            q_h = q[:, h * dk : (h + 1) * dk]
            k_h = k[:, h * dk : (h + 1) * dk]
            v_h = v[:, h * dv : (h + 1) * dv]
            scores = lax.dot_general(q_h, k_h, last_dims, preferred_element_type=jnp.float32)
            logits = cum_t[:, index : index + 1] + diff[index : index + 1, :]
            logits = jnp.where(js <= it, logits, LOW)
            stab = jnp.max(logits, axis=1, keepdims=True)
            weighted = scores * scale * jnp.exp(logits - stab)
            raw[:, h * dv : (h + 1) * dv] = jnp.dot(
                weighted.astype(jnp.bfloat16), v_h, preferred_element_type=jnp.float32
            )
            stabs[:, index : index + 1] = stab
            index += 1

    lax.fori_loop(1, n, lambda r, c: (out_copy(r).wait(), c)[1], 0)

    which = tuple(
        (me * parts[g]) // groups[g][8] + (heads[0] if g else 0) for g in range(2)
    )
    sub = lax.broadcasted_iota(jnp.int32, (heads_p, width), 0)
    picks = tuple(sub == w for w in which)

    def merge(t, _):
        level_c = levels[0]
        back[t] = state[...]
        levels[1] = jnp.where(t == me, level_c, levels[1])
        mark = got[t, extra : extra + heads_p, :]
        lev = jnp.broadcast_to(mark[:, :1], mark.shape)
        tot = jnp.broadcast_to(mark[:, width - 1 :], mark.shape)
        new = jnp.maximum(level_c + tot, lev)
        old_f = jnp.exp(level_c + tot - new)
        new_f = jnp.exp(lev - new)
        levels[0] = new
        for g in range(2):
            span = slice(starts[g], starts[g] + parts[g])

            def pick(f):
                return jnp.sum(jnp.where(picks[g], f, 0.0), axis=0, keepdims=True)

            state[span, :] = pick(old_f) * state[span, :] + pick(new_f) * got[t, span, :]
        return 0

    levels[...] = jnp.full(levels.shape, LOW, jnp.float32)
    state[...] = jnp.zeros(state.shape, jnp.float32)
    lax.fori_loop(0, n, merge, 0)
    entering = levels[1]

    def back_copy(r):
        peer = lax.rem(me + r, n)
        return pltpu.make_async_remote_copy(
            src_ref=back.at[peer],
            dst_ref=carried.at[me],
            send_sem=send_sem2.at[r],
            recv_sem=recv_sem2.at[r],
            device_id=where_is(peer),
            device_id_type=MESH,
        )

    lax.fori_loop(1, n, lambda r, c: (back_copy(r).start(), c)[1], 0)
    carried[me] = back[me]
    entering_t = lax.dot_general(
        jnp.where(
            lax.broadcasted_iota(jnp.int32, (rows, width), 1) == 0, 1.0, 0.0
        ),
        entering,
        last_dims,
        precision=lax.Precision.HIGHEST,
        preferred_element_type=jnp.float32,
    )
    shifted = cum_t + entering_t
    own = stabs[:, :heads_p]
    both = jnp.maximum(own, shifted)
    own_f = jnp.exp(own - both)
    in_f = jnp.exp(shifted - both)
    lax.fori_loop(1, n, lambda r, c: (back_copy(r).wait(), c)[1], 0)

    index = 0
    for g, (q, _, v, og, gain, out, raw, mem, dk) in enumerate(groups):
        dv = v.shape[1] // heads[g]
        size = parts[g]
        per = dk // size
        for h in range(heads[g]):
            for p in range(per):
                mem[p * size : (p + 1) * size, :] = carried[
                    h * per + p, starts[g] : starts[g] + size, :dv
                ]
            memory = mem[...]
            high = memory.astype(jnp.bfloat16)
            rest = (memory - high.astype(jnp.float32)).astype(jnp.bfloat16)
            q_h = q[:, h * dk : (h + 1) * dk]
            cols = slice(h * dv, (h + 1) * dv)
            incoming = jnp.dot(q_h, high, preferred_element_type=jnp.float32) + jnp.dot(
                q_h, rest, preferred_element_type=jnp.float32
            )
            value = (
                raw[:, cols] * own_f[:, index : index + 1]
                + incoming * in_f[:, index : index + 1]
            )
            value = value * lax.rsqrt(jnp.mean(value * value, axis=1, keepdims=True) + 1e-06)
            gate = 1.0 / (1.0 + jnp.exp(-og[:, cols].astype(jnp.float32)))
            value = value * gain[:, cols].astype(jnp.float32) * gate
            out[:, cols] = value.astype(jnp.bfloat16)
            index += 1


def cell(q_w, k_w, v_w, og_w, gat_w, gain_w, q_n, k_n, v_n, og_n, gat_n, gain_n):
    n = lax.axis_size("a") * lax.axis_size("b")
    rows = q_w.shape[0]
    heads = gat_w.shape[1] + gat_n.shape[1]
    heads_p = -(-heads // 8) * 8
    gating = jnp.concatenate([gat_w, gat_n], axis=1)
    gating = jnp.pad(gating, ((0, 0), (0, heads_p - heads), (0, 0)))
    parts = (q_w.shape[1] // n, q_n.shape[1] // n)
    width = v_w.shape[1] // gat_w.shape[1]
    width_n = v_n.shape[1] // gat_n.shape[1]
    vmem = pl.BlockSpec(memory_space=pltpu.VMEM)
    state = parts[0] + parts[1]
    return pl.pallas_call(
        functools.partial(cell_kernel, n),
        out_shape=(
            jax.ShapeDtypeStruct(v_w.shape, jnp.bfloat16),
            jax.ShapeDtypeStruct(v_n.shape, jnp.bfloat16),
        ),
        in_specs=[vmem] * 11,
        out_specs=(vmem, vmem),
        scratch_shapes=[
            pltpu.VMEM(v_w.shape, jnp.float32),
            pltpu.VMEM(v_n.shape, jnp.float32),
            pltpu.VMEM((rows, 128), jnp.float32),
            pltpu.VMEM((n, state + heads_p, width), jnp.float32),
            pltpu.VMEM((n, state + heads_p, width), jnp.float32),
            pltpu.VMEM((n, state, width), jnp.float32),
            pltpu.VMEM((n, state, width), jnp.float32),
            pltpu.VMEM((DK_A, width), jnp.float32),
            pltpu.VMEM((DK_B, width_n), jnp.float32),
            pltpu.VMEM((state, width), jnp.float32),
            pltpu.VMEM((2, heads_p, width), jnp.float32),
            pltpu.SemaphoreType.DMA((n,)),
            pltpu.SemaphoreType.DMA((n,)),
            pltpu.SemaphoreType.DMA((n,)),
            pltpu.SemaphoreType.DMA((n,)),
        ],
        compiler_params=pltpu.CompilerParams(
            collective_id=0, has_side_effects=True, vmem_limit_bytes=32 * 2**20
        ),
        cost_estimate=pl.CostEstimate(
            flops=2 * 10**9, bytes_accessed=120 * 10**6, transcendentals=0
        ),
    )(
        q_w,
        k_w,
        v_w,
        og_w,
        gain_w.reshape(1, -1),
        q_n,
        k_n,
        v_n,
        og_n,
        gain_n.reshape(1, -1),
        gating,
    )


def layer_kernel(na, nb, *refs):
    (
        residual,
        q_w,
        k_w,
        v_w,
        og_w,
        gat_w,
        gain_w,
        read_w,
        q_n,
        k_n,
        v_n,
        og_n,
        gat_n,
        gain_n,
        read_n,
        norm_gain,
        gate,
        up,
        down,
        out,
        res_v,
        qw_v,
        kw_v,
        vw_v,
        ogw_v,
        gatw_v,
        gainw_v,
        qn_v,
        kn_v,
        vn_v,
        ogn_v,
        gatn_v,
        gainn_v,
        read_v,
        ngain_v,
        edge_v,
        gu_own,
        d_own,
        gu_all,
        d_all,
        gat_v,
        raw_w,
        raw_n,
        stabs,
        sent,
        got,
        mark,
        mark_got,
        prefix,
        total_s,
        total_got,
        tmark,
        tmark_got,
        enter,
        enter_mark,
        back,
        carried,
        bmark,
        bmark_got,
        gated,
        part,
        part_got,
        middle,
        x_all,
        acc,
        hidden,
        terms,
        terms_got,
        sums,
        a_got,
        joined,
        b_got,
        r_got,
        in_sem,
        p1_s,
        p1_r,
        p2_s,
        p2_r,
        p3_s,
        p3_r,
        z_s,
        z_r,
        f_s,
        f_r,
        g_s,
        g_r,
        t_s,
        t_r,
        x_s,
        x_r,
        y_s,
        y_r,
        a_s,
        a_r,
        b_s,
        b_r,
        r_s,
        r_r,
    ) = refs
    n = na * nb
    a, b, t = lax.axis_index("a"), lax.axis_index("b"), lax.axis_index("tp")
    me = a * nb + b
    f32, bf16 = jnp.float32, jnp.bfloat16

    barrier = pltpu.get_barrier_semaphore()
    peers = [(a ^ k, b, t) for k in range(1, na)]
    peers += [(a, b ^ m, t) for m in range(1, nb)]
    peers += [(a, b, 1 - t)]
    for peer in peers:
        pl.semaphore_signal(barrier, inc=1, device_id=peer, device_id_type=MESH)

    depth = gate.shape[0]
    chunk = gate.shape[1] // na
    whole = chunk // 128 * 128
    half = chunk - whole
    cols = down.shape[1]
    model = residual.shape[1]
    own_rows = residual.shape[0]
    rows = q_w.shape[0]
    kspan = nb * depth
    span = nb * cols
    wide_heads, narrow_heads = gat_w.shape[1], gat_n.shape[1]
    heads = wide_heads + narrow_heads
    dv_w = v_w.shape[1] // wide_heads
    dv_n = v_n.shape[1] // narrow_heads

    def local(src, dst, i):
        copy = pltpu.make_async_copy(src, dst, in_sem.at[i])
        copy.start()
        return copy

    loads = {}
    loads["gat"] = [local(gat_w, gatw_v, 0), local(gat_n, gatn_v, 1)]
    loads["k"] = [
        local(k_w, kw_v, 2),
        local(k_n, kn_v, 3),
        local(v_w, vw_v, 4),
        local(v_n, vn_v, 5),
    ]

    def slab_parts(c):
        odd = c % 2
        return c * chunk + odd * half, c * chunk + (1 - odd) * whole

    def d_slab(r, lo=0, size=chunk):
        return d_all.at[
            r // 2, pl.ds(lo, size), pl.ds(pl.multiple_of(lax.rem(r, 2) * cols, cols), cols)
        ]

    first, second = slab_parts(a)
    own_down = (
        pltpu.make_async_copy(
            down.at[pl.ds(pl.multiple_of(first, half), whole)],
            d_slab(me, 0, whole),
            in_sem.at[6],
        ),
        pltpu.make_async_copy(
            down.at[pl.ds(pl.multiple_of(second, half), half)],
            d_slab(me, whole, half),
            in_sem.at[7],
        ),
    )
    for c in own_down:
        c.start()
    for c in range(na):
        lo, hi = slab_parts(c)
        pltpu.make_async_copy(
            down.at[lo : lo + whole], d_own.at[c, 0:whole], in_sem.at[8]
        ).start()
        pltpu.make_async_copy(
            down.at[hi : hi + half], d_own.at[c, whole:chunk], in_sem.at[8]
        ).start()
    for i, w in enumerate((gate, up)):
        for c in range(na):
            lo, _ = slab_parts(c)
            pltpu.make_async_copy(
                w.at[:, lo : lo + whole],
                gu_own.at[c, :, i * whole : (i + 1) * whole],
                in_sem.at[9],
            ).start()
        for c in range(na // 2):
            lo = 2 * c * chunk + whole
            pltpu.make_async_copy(
                w.at[:, lo : lo + 128], edge_v.at[i, c], in_sem.at[10]
            ).start()
    loads["q"] = [local(q_w, qw_v, 11), local(q_n, qn_v, 12)]
    loads["og"] = [
        local(og_w, ogw_v, 13),
        local(og_n, ogn_v, 14),
        local(gain_w, gainw_v, 15),
        local(gain_n, gainn_v, 16),
    ]
    loads["read"] = [
        local(read_w, read_v.at[: read_w.shape[0]], 17),
        local(read_n, read_v.at[read_w.shape[0] :], 18),
        local(residual, res_v, 19),
        local(norm_gain, ngain_v, 20),
    ]

    started = []

    def remote(src, dst, s_sem, r_sem, peer):
        return pltpu.make_async_remote_copy(
            src_ref=src,
            dst_ref=dst,
            send_sem=s_sem,
            recv_sem=r_sem,
            device_id=peer,
            device_id_type=MESH,
        )

    def go(copy):
        copy.start()
        started.append(copy)

    def slab(kind, r, lo, size):
        if kind == 0:
            return gu_all.at[r, pl.ds(lo, size)]
        return d_slab(r, lo, size)

    extent = (depth, chunk)

    def z_copy(kind, k, r):
        src = (gu_own, d_own)[kind].at[a ^ k]
        return remote(
            src, slab(kind, r, 0, extent[kind]), z_s.at[kind, k], z_r.at[kind, k], (a ^ k, b, t)
        )

    def z_start(kind, k):
        go(z_copy(kind, k, me))

    def z_wait(kind, k):
        z_copy(kind, k, (a ^ k) * nb + b).wait_recv()

    def full_copy(kind, s, d, h, who):
        size = extent[kind] // 2
        ref = slab(kind, (a ^ s) * nb + who, h * size, size)
        return remote(
            ref, ref, f_s.at[kind, s, d, h], f_r.at[kind, s, d, h], (a, b ^ (1 << d), t)
        )

    def full_start(kind, s):
        for d, h in ((0, 0), (1, 1), (0, 1), (1, 0)):
            go(full_copy(kind, s, d, h, b))

    def full_wait(kind, s, d, h):
        full_copy(kind, s, d, h, b ^ (1 << d)).wait_recv()

    def diag_copy(kind, s, h, who):
        size = extent[kind] // 2
        ref = slab(kind, (a ^ s) * nb + who, h * size, size)
        return remote(ref, ref, g_s.at[kind, s, h], g_r.at[kind, s, h], (a, b ^ (2 >> h), t))

    def relay(kind, s):
        for h in range(2):
            full_wait(kind, s, h, h)
            go(diag_copy(kind, s, h, b ^ (1 << h)))

    def arrived(kind, s):
        for h in range(2):
            full_wait(kind, s, 1 - h, h)
            diag_copy(kind, s, h, b ^ 3).wait_recv()

    for c in loads["gat"]:
        c.wait()
    gat_v[:, :wide_heads, :] = gatw_v[...]
    gat_v[:, wide_heads:, :] = gatn_v[...]
    it = lax.broadcasted_iota(jnp.int32, (rows, rows), 0)
    js = lax.broadcasted_iota(jnp.int32, (rows, rows), 1)
    upper = (it <= js).astype(f32)
    eye = (it == js).astype(f32)
    last_dims = (((1,), (1,)), ((), ()))
    first_dims = (((0,), (0,)), ((), ()))
    exact = dict(precision=lax.Precision.HIGHEST, preferred_element_type=f32)
    gate_in = gat_v[0]
    x = gat_v[1]
    forget = jnp.minimum(x, 0.0) - jnp.log1p(jnp.exp(-jnp.abs(x))) + gat_v[2]
    cum = jnp.dot(forget, upper, **exact)
    cum_t = lax.dot_general(eye, cum, last_dims, **exact)
    diff = gate_in - cum
    diff_t = lax.dot_general(eye, diff, last_dims, **exact)
    total = cum[:, rows - 1 : rows]
    level = jnp.max(total + diff, axis=1, keepdims=True)
    total_t = cum_t[rows - 1 : rows, :]
    level_t = jnp.max(total_t + diff_t, axis=0, keepdims=True)
    tail_t = jnp.exp(total_t + diff_t - level_t)
    lane = lax.broadcasted_iota(jnp.int32, (heads, 128), 1)
    mark[...] = jnp.where(
        lane < 64, jnp.broadcast_to(level, (heads, 128)), jnp.broadcast_to(total, (heads, 128))
    )

    groups = (
        (qw_v, kw_v, vw_v, ogw_v, gainw_v, raw_w, DK_A, dv_w, wide_heads, 0),
        (qn_v, kn_v, vn_v, ogn_v, gainn_v, raw_n, DK_B, dv_n, narrow_heads, wide_heads),
    )
    fold = DK_B // 2
    deep = DK_A + fold

    for c in own_down:
        c.wait()
    pltpu.make_async_copy(d_own, d_own, in_sem.at[8]).wait()
    pl.semaphore_wait(barrier, len(peers))
    z_start(1, 1)
    is_inner = (a + 1) // 2 % 2
    inner = is_inner == 1
    order = (0, 1 + 2 * is_inner, 3 - 2 * is_inner, 2)


    for c in loads["k"]:
        c.wait()
    for _, k, v, _, _, _, dk, dv, count, base in groups:
        scale = dk ** (-0.5)
        for h in range(count):
            i = base + h
            scaled = k[:, h * dk : (h + 1) * dk].astype(f32) * (tail_t[:, i : i + 1] * scale)
            memory = lax.dot_general(
                scaled.astype(bf16),
                v[:, h * dv : (h + 1) * dv],
                first_dims,
                preferred_element_type=f32,
            ).astype(bf16)
            if base == 0:
                sent[h, :dk, :] = memory
            else:
                sent[h, DK_A:deep, :dv] = memory[:fold]
                sent[h, DK_A:deep, dv:] = memory[fold:]

    def p1(m, r):
        peer = (a, b ^ m, t)
        return (
            remote(mark, mark_got.at[r], p1_s.at[0, m], p1_r.at[0, m], peer),
            remote(sent.at[b ^ m], got.at[r], p1_s.at[1, m], p1_r.at[1, m], peer),
        )

    for m in range(1, nb):
        for c in p1(m, b):
            go(c)
    got[b] = sent[b]
    mark_got[b] = mark[...]

    pltpu.make_async_copy(
        gu_own.at[:, :, : 2 * whole], gu_own.at[:, :, : 2 * whole], in_sem.at[9]
    ).wait()
    pltpu.make_async_copy(edge_v, edge_v, in_sem.at[10]).wait()
    for c in range(na // 2):
        ge, ue = edge_v[0, c], edge_v[1, c]
        gu_own[2 * c, :, 2 * whole :] = jnp.concatenate([ge[:, :half], ue[:, :half]], axis=1)
        gu_own[2 * c + 1, :, 2 * whole :] = jnp.concatenate([ge[:, half:], ue[:, half:]], axis=1)
    gu_all[me] = gu_own[a]

    @pl.when(inner)
    def _():
        z_copy(0, 3, me).start()

    full_start(0, 0)
    full_start(1, 0)

    for c in loads["q"]:
        c.wait()
    for q, k, v, _, _, raw, dk, dv, count, base in groups:
        scale = dk ** (-0.5)
        for h in range(count):
            i = base + h
            q_h = q[:, h * dk : (h + 1) * dk]
            k_h = k[:, h * dk : (h + 1) * dk]
            v_h = v[:, h * dv : (h + 1) * dv]
            scores = lax.dot_general(q_h, k_h, last_dims, preferred_element_type=f32)
            logits = cum_t[:, i : i + 1] + diff[i : i + 1, :]
            logits = jnp.where(js <= it, logits, LOW)
            stab = jnp.max(logits, axis=1, keepdims=True)
            weighted = scores * scale * jnp.exp(logits - stab)
            raw[:, h * dv : (h + 1) * dv] = jnp.dot(
                weighted.astype(bf16), v_h, preferred_element_type=f32
            )
            stabs[:, i : i + 1] = stab

    for m in range(1, nb):
        for c in p1(m, b ^ m):
            c.wait_recv()
    spans = ((0, DK_A), (DK_A, deep))

    def read_mark(ref, where, row):
        line = ref[where, pl.ds(row, 1), :]
        return line[:, :1], line[:, 127:128]

    run = []
    for g, (lo, hi) in enumerate(spans):
        lev, tot = read_mark(mark_got, 0, b + g * wide_heads)
        state = got[0, lo:hi, :].astype(f32)
        run.append([(lev, tot)])
        for j in range(1, nb):
            prefix[j - 1, lo:hi, :] = state
            lev2, tot2 = read_mark(mark_got, j, b + g * wide_heads)
            new = jnp.maximum(lev + tot2, lev2)
            state = (
                jnp.exp(lev + tot2 - new) * state
                + jnp.exp(lev2 - new) * got[j, lo:hi, :].astype(f32)
            )
            lev, tot = new, tot + tot2
            run[g].append((lev, tot))
        total_s[lo:hi, :] = state.astype(bf16)
    lane1 = lax.broadcasted_iota(jnp.int32, (1, 128), 1)
    for g in range(2):
        lev, tot = run[g][nb - 1]
        tmark[g : g + 1, :] = jnp.where(
            lane1 < 64, jnp.broadcast_to(lev, (1, 128)), jnp.broadcast_to(tot, (1, 128))
        )

    def p2(k, r):
        peer = (a ^ k, b, t)
        return (
            remote(tmark, tmark_got.at[r], p2_s.at[0, k], p2_r.at[0, k], peer),
            remote(total_s, total_got.at[r], p2_s.at[1, k], p2_r.at[1, k], peer),
        )

    for k in range(1, na):

        @pl.when((a ^ k) > a)
        def _():
            for c in p2(k, a):
                c.start()

    @pl.when(inner)
    def _():
        z_copy(0, 2, me).start()
        z_copy(0, 1, me).start()

    @pl.when(jnp.logical_not(inner))
    def _():
        for k in range(1, na):
            z_copy(0, k, me).start()

    started.extend(z_copy(0, k, me) for k in range(1, na))

    enter[...] = jnp.zeros(enter.shape, f32)
    enter_mark[...] = jnp.full(enter_mark.shape, LOW, f32)
    for k in range(1, na):

        @pl.when((a ^ k) < a)
        def _():
            for c in p2(k, a ^ k):
                c.wait_recv()

    for z in range(na - 1):

        @pl.when(z < a)
        def _():
            for g, (lo, hi) in enumerate(spans):
                lev = enter_mark[g : g + 1, :1]
                lev2, tot2 = read_mark(tmark_got, z, g)
                new = jnp.maximum(lev + tot2, lev2)
                enter[lo:hi, :] = (
                    jnp.exp(lev + tot2 - new) * enter[lo:hi, :]
                    + jnp.exp(lev2 - new) * total_got[z, lo:hi, :].astype(f32)
                )
                enter_mark[g : g + 1, :] = jnp.broadcast_to(new, (1, 128))

    for g, (lo, hi) in enumerate(spans):
        lev = enter_mark[g : g + 1, :1]
        back[0, lo:hi, :] = enter[lo:hi, :].astype(bf16)
        bmark[0, g : g + 1, :] = jnp.broadcast_to(lev, (1, 128))
        for j in range(1, nb):
            lev2, tot2 = run[g][j - 1]
            new = jnp.maximum(lev + tot2, lev2)
            back[j, lo:hi, :] = (
                jnp.exp(lev + tot2 - new) * enter[lo:hi, :]
                + jnp.exp(lev2 - new) * prefix[j - 1, lo:hi, :]
            ).astype(bf16)
            bmark[j, g : g + 1, :] = jnp.broadcast_to(new, (1, 128))

    def p3(m, r):
        peer = (a, b ^ m, t)
        return (
            remote(bmark.at[b ^ m], bmark_got.at[r], p3_s.at[0, m], p3_r.at[0, m], peer),
            remote(back.at[b ^ m], carried.at[r], p3_s.at[1, m], p3_r.at[1, m], peer),
        )

    for m in range(1, nb):
        for c in p3(m, b):
            go(c)
    carried[b] = back[b]
    bmark_got[b] = bmark[b]
    relay(0, 0)
    relay(1, 0)

    for c in loads["og"]:
        c.wait()
    for m in range(1, nb):
        for c in p3(m, b ^ m):
            c.wait_recv()

    for g, (q, _, _, og, gain, raw, dk, dv, count, base) in enumerate(groups):
        for h in range(count):
            i = base + h
            if g == 0:
                memory = carried[h, :dk, :]
            else:
                memory = jnp.concatenate(
                    [carried[h, DK_A:deep, :dv], carried[h, DK_A:deep, dv:]], axis=0
                )
            own = stabs[:, i : i + 1]
            shifted = cum_t[:, i : i + 1] + bmark_got[h, g : g + 1, :1]
            both = jnp.maximum(own, shifted)
            span_h = slice(h * dv, (h + 1) * dv)
            incoming = jnp.dot(
                q[:, h * dk : (h + 1) * dk], memory, preferred_element_type=f32
            )
            value = raw[:, span_h] * jnp.exp(own - both) + incoming * jnp.exp(shifted - both)
            value = value * lax.rsqrt(jnp.mean(value * value, axis=1, keepdims=True) + 1e-06)
            gate_h = 1.0 / (1.0 + jnp.exp(-og[:, span_h].astype(f32)))
            value = value * gain[:, span_h].astype(f32) * gate_h
            lo = g * raw_w.shape[1] + h * dv
            gated[:, lo : lo + dv] = value.astype(bf16)

    z_wait(0, order[1])
    full_start(0, order[1])

    for c in loads["read"]:
        c.wait()
    tile = model // 4
    for j in range(model // tile):
        sl = slice(j * tile, (j + 1) * tile)
        p = jnp.dot(gated[...], read_v[:, sl], preferred_element_type=f32).astype(bf16)
        part[:, :, sl] = p.reshape(2, own_rows, tile)
    partner = (a, b, 1 - t)
    swap = remote(part.at[1 - t], part_got, t_s.at[0], t_r.at[0], partner)
    go(swap)
    swap.wait_recv()
    mixed = part[t].astype(f32) + part_got[...].astype(f32)
    mid = (res_v[...].astype(f32) + mixed).astype(bf16)
    middle[...] = mid
    mid = mid.astype(f32)
    normed = mid * lax.rsqrt(jnp.mean(mid * mid, axis=-1, keepdims=True) + 1e-06)
    block = 2 * own_rows

    piece = own_rows // 2

    def row_block(z, core, c, size=piece):
        lo = (z * 2 + core) * own_rows + c * piece
        return x_all.at[pl.ds(pl.multiple_of(lo, piece), size)]

    x_all[pl.ds(pl.multiple_of((a * 2 + t) * own_rows, own_rows), own_rows), :] = (
        normed * ngain_v[...].astype(f32)
    ).astype(bf16)

    def x_copy(i, k, z, c):
        ref = row_block(z, t, c)
        return remote(ref, ref, x_s.at[i, c], x_r.at[i, c], (a ^ k, b, t))

    def y_copy(z, k, core, c):
        ref = row_block(z, core, c)
        return remote(ref, ref, y_s.at[k, c], y_r.at[k, c], partner)

    for c in range(2):
        go(x_copy(0, 2, a, c))
    for c in range(2):
        go(x_copy(1, 1, a, c))
    for c in range(2):
        go(y_copy(a, 0, t, c))

    width = gu_all.shape[2]
    tiles = [(lo, min(lo + 512, width)) for lo in range(0, width, 512)]

    def unit(lo, m, s, fresh):
        z = a ^ s
        xs = x_all[pl.ds(lo, m), pl.ds(pl.multiple_of(z * kspan, kspan), kspan)]
        for c0, c1 in tiles:
            w = gu_all[pl.ds(z * nb, nb), :, c0:c1].reshape(kspan, c1 - c0)
            p = jnp.dot(xs, w, preferred_element_type=f32)
            if fresh:
                acc[pl.ds(lo, m), c0:c1] = p
            else:
                acc[pl.ds(lo, m), c0:c1] += p

    def passed_on(i, k):
        z = a ^ k
        for c in range(2):
            x_copy(i, 1 if i else 2, z, c).wait_recv()
            if i == 0:
                go(x_copy(2, 1, z, c))
            go(y_copy(z, k, t, c))

    z_wait(0, order[2])
    full_start(0, order[2])
    relay(0, order[1])
    z_wait(0, order[3])
    full_start(0, order[3])
    relay(0, order[2])
    passed_on(0, 2)
    z_start(1, 2)
    z_start(1, 3)
    passed_on(1, 1)
    z_wait(1, 1)
    full_start(1, 1)
    relay(0, order[3])
    passed_on(2, 3)
    for k in range(na):
        for c in range(2):
            y_copy(a ^ k, k, 1 - t, c).wait_recv()
    total_rows = na * block
    for s in range(na):
        if s == 3:
            z_wait(1, 2)
            full_start(1, 2)
            relay(1, 1)
        arrived(0, order[s])
        unit(0, total_rows, order[s], s == 0)

    for j in range(2):
        sl = slice(j * total_rows // 2, (j + 1) * total_rows // 2)
        gt = acc[sl, :whole]
        hidden[sl, :whole] = (
            gt * (1.0 / (1.0 + jnp.exp(-gt))) * acc[sl, whole : 2 * whole]
        ).astype(bf16)
        mx = acc[sl, 2 * whole :]
        hx = mx * (1.0 / (1.0 + jnp.exp(-mx))) * pltpu.roll(mx, half, 1)
        hidden[sl, whole:] = hx[:, :half].astype(bf16)
    def t_copy(s):
        return remote(
            terms.at[s, :, 1 - t], terms_got.at[s], t_s.at[1 + s], t_r.at[1 + s], partner
        )

    def down_group(s):
        arrived(1, s)
        for p in range(nb // 2):
            w = d_all[(a ^ s) * (nb // 2) + p]
            v = jnp.dot(hidden[...], w, preferred_element_type=f32).astype(bf16)
            terms[s, :, :, :, p * 2 * cols : (p + 1) * 2 * cols] = v.reshape(
                na, 2, own_rows, 2 * cols
            )
        go(t_copy(s))

    high = a // 2

    def a_copy(s, z):
        return remote(
            sums.at[s, :, 1 - a % 2], a_got.at[z ^ s], a_s.at[s], a_r.at[z ^ s], (a ^ 1, b, t)
        )

    def b_copy(s, z):
        return remote(
            joined.at[s % 2], b_got.at[z ^ s], b_s.at[s], b_r.at[z ^ s], (a ^ 2, b, t)
        )

    def r_copy(k, s, z):
        return remote(
            sums.at[s, (a ^ k) // 2, (a ^ k) % 2],
            r_got.at[k, z ^ s],
            r_s.at[k, s],
            r_r.at[k, z ^ s],
            (a ^ k, b, t),
        )

    def sum_group(s):
        t_copy(s).wait_recv()
        sums[s] = (
            (terms[s, :, t].astype(f32) + terms_got[s].astype(f32))
            .astype(bf16)
            .reshape(sums.shape[1:])
        )
        if s < 2:
            go(a_copy(s, a))
        else:
            for k in (3, 2, 1):
                go(r_copy(k, s, a))

    def join_group(s):
        a_copy(s, a).wait_recv()
        joined[s] = (
            sums[s, 1 - high, a % 2].astype(f32) + a_got[a ^ s, 1 - high].astype(f32)
        ).astype(bf16)
        go(b_copy(s, a))

    down_group(0)
    sum_group(0)
    z_wait(1, 3)
    full_start(1, 3)
    down_group(1)
    sum_group(1)
    relay(1, 2)
    join_group(0)
    join_group(1)
    down_group(2)
    relay(1, 3)
    sum_group(2)
    down_group(3)
    sum_group(3)

    def finish_group(s, v):
        col = a ^ s
        v = v + sums[s, high, a % 2].astype(f32)
        c0 = pl.ds(pl.multiple_of(col * span, span), span)
        out[:, c0] = (middle[:, c0].astype(f32) + v).astype(bf16)

    for s in (2, 3):
        b_copy(s, a).wait_recv()
        r_copy(1, s, a).wait_recv()
        finish_group(s, b_got[a ^ s].astype(f32) + r_got[1, a ^ s].astype(f32))
    for s in (0, 1):
        r_copy(2, s, a).wait_recv()
        r_copy(3, s, a).wait_recv()
        v = r_got[2, a ^ s].astype(f32) + r_got[3, a ^ s].astype(f32)
        finish_group(s, v + a_got[a ^ s, high].astype(f32))

    for c in started:
        c.wait_send()
    for k in range(1, na):

        @pl.when((a ^ k) > a)
        def _():
            for c in p2(k, a):
                c.wait_send()


def layer(na, nb, *args):
    (res, q_w, k_w, v_w, og_w, gat_w, gain_w, read_w) = args[:8]
    (q_n, k_n, v_n, og_n, gat_n, gain_n, read_n, norm_gain, gate, up, down) = args[8:]
    bf16, f32 = jnp.bfloat16, jnp.float32
    n = na * nb
    depth = gate.shape[0]
    chunk = gate.shape[1] // na
    whole = chunk // 128 * 128
    width = 2 * whole + 128
    cols = down.shape[1]
    own_rows, model = res.shape
    rows = q_w.shape[0]
    heads = gat_w.shape[1] + gat_n.shape[1]
    deep = DK_A + DK_B // 2
    dv = v_w.shape[1] // gat_w.shape[1]
    total_rows = na * 2 * own_rows
    span = nb * cols

    def vm(shape, dtype=bf16):
        return pltpu.VMEM(shape, dtype)

    def like(x):
        return pltpu.VMEM(x.shape, x.dtype)

    dma = pltpu.SemaphoreType.DMA
    gain_w, gain_n, norm_gain = (g.reshape(1, -1) for g in (gain_w, gain_n, norm_gain))
    scratch = [
        like(res),
        like(q_w),
        like(k_w),
        like(v_w),
        like(og_w),
        like(gat_w),
        like(gain_w),
        like(q_n),
        like(k_n),
        like(v_n),
        like(og_n),
        like(gat_n),
        like(gain_n),
        vm((read_w.shape[0] + read_n.shape[0], model)),
        like(norm_gain),
        vm((2, na // 2, depth, 128)),
        vm((na, depth, width)),
        vm((na, chunk, cols)),
        vm((n, depth, width)),
        vm((n // 2, chunk, 2 * cols)),
        vm((3, heads, rows), f32),
        vm(v_w.shape, f32),
        vm(v_n.shape, f32),
        vm((rows, 128), f32),
        vm((nb, deep, dv)),
        vm((nb, deep, dv)),
        vm((heads, 128), f32),
        vm((nb, heads, 128), f32),
        vm((nb - 1, deep, dv), f32),
        vm((deep, dv)),
        vm((na, deep, dv)),
        vm((8, 128), f32),
        vm((na, 8, 128), f32),
        vm((deep, dv), f32),
        vm((8, 128), f32),
        vm((nb, deep, dv)),
        vm((nb, deep, dv)),
        vm((nb, 8, 128), f32),
        vm((nb, 8, 128), f32),
        vm((rows, v_w.shape[1] + v_n.shape[1])),
        vm((2, own_rows, model)),
        vm((own_rows, model)),
        vm((own_rows, model)),
        vm((total_rows, model)),
        vm((total_rows, width), f32),
        vm((total_rows, chunk)),
        vm((na, na, 2, own_rows, span)),
        vm((na, na, own_rows, span)),
        vm((na, na // 2, 2, own_rows, span)),
        vm((na, na // 2, own_rows, span)),
        vm((2, own_rows, span)),
        vm((na, own_rows, span)),
        vm((na, na, own_rows, span)),
        dma((21,)),
        dma((2, nb)),
        dma((2, nb)),
        dma((2, na)),
        dma((2, na)),
        dma((2, nb)),
        dma((2, nb)),
        dma((2, na)),
        dma((2, na)),
        dma((2, na, 2, 2)),
        dma((2, na, 2, 2)),
        dma((2, na, 2)),
        dma((2, na, 2)),
        dma((1 + na,)),
        dma((1 + na,)),
        dma((3, 2)),
        dma((3, 2)),
        dma((na, 2)),
        dma((na, 2)),
        dma((na,)),
        dma((na,)),
        dma((na,)),
        dma((na,)),
        dma((na, na)),
        dma((na, na)),
    ]
    hbm = pl.BlockSpec(memory_space=pl.ANY)
    return pl.pallas_call(
        functools.partial(layer_kernel, na, nb),
        out_shape=jax.ShapeDtypeStruct(res.shape, bf16),
        in_specs=[hbm] * 19,
        out_specs=pl.BlockSpec(memory_space=pltpu.VMEM),
        scratch_shapes=scratch,
        compiler_params=pltpu.CompilerParams(
            collective_id=0, has_side_effects=True, vmem_limit_bytes=60 * 2**20
        ),
    )(
        res,
        q_w,
        k_w,
        v_w,
        og_w,
        gat_w,
        gain_w,
        read_w,
        q_n,
        k_n,
        v_n,
        og_n,
        gat_n,
        gain_n,
        read_n,
        norm_gain,
        gate,
        up,
        down,
    )


def fits(mesh_shape, args):
    na, nb, ntp = mesh_shape
    gate, gat_w, gat_n = args[16], args[5], args[12]
    q_w, v_w, v_n = args[1], args[3], args[10]
    heads_w, heads_n = gat_w.shape[1], gat_n.shape[1]
    return (
        na == nb == 4
        and ntp == 2
        and gate.shape[1] % na == 0
        and gate.shape[1] // na % 128 == 64
        and heads_w == heads_n == nb
        and q_w.shape[0] == 128
        and v_w.shape[1] // heads_w == 2 * (v_n.shape[1] // heads_n)
    )


def passed(block, axis, step):
    size = lax.axis_size(axis)
    if step % size == 0:
        return block
    return lax.ppermute(block, axis, [(i, (i + step) % size) for i in range(size)])


def gathered(block, axis):
    return jnp.concatenate([passed(block, axis, r) for r in range(lax.axis_size(axis))], axis=0)


def returned(blocks, axis):
    size = lax.axis_size(axis)
    rows = blocks.shape[0] // size
    pieces = [passed(blocks[r * rows : (r + 1) * rows], axis, -r) for r in range(size)]
    return sum(p.astype(jnp.float32) for p in pieces)


def plain_body(
    residual,
    query_wide,
    key_wide,
    value_wide,
    outgate_wide,
    gating_wide,
    gain_wide,
    readout_wide,
    query_narrow,
    key_narrow,
    value_narrow,
    outgate_narrow,
    gating_narrow,
    gain_narrow,
    readout_narrow,
    norm_gain,
    gate_weight,
    up_weight,
    down_weight,
):
    na, nb = lax.axis_size("a"), lax.axis_size("b")
    depth, hidden_tp = gate_weight.shape
    chunk = hidden_tp // na
    out_cols = down_weight.shape[1]
    model = residual.shape[1]

    def spread(pieces):
        return lax.all_to_all(pieces, "a", split_axis=0, concat_axis=0, tiled=True)

    mine = (
        spread(jnp.moveaxis(gate_weight.reshape(depth, na, chunk), 1, 0)),
        spread(jnp.moveaxis(up_weight.reshape(depth, na, chunk), 1, 0)),
        spread(down_weight.reshape(na, chunk, out_cols)),
    )
    gate_all, up_all, down_all = (
        lax.all_gather(m, "b", axis=0, tiled=True) for m in mine
    )
    *_, gating_wide, gating_narrow = lax.optimization_barrier(
        (*mine, gating_wide, gating_narrow)
    )

    gated_w, gated_n = cell(
        query_wide,
        key_wide,
        value_wide,
        outgate_wide,
        gating_wide,
        gain_wide,
        query_narrow,
        key_narrow,
        value_narrow,
        outgate_narrow,
        gating_narrow,
        gain_narrow,
    )
    partial = (
        jnp.dot(gated_w, readout_wide, preferred_element_type=jnp.float32)
        + jnp.dot(gated_n, readout_narrow, preferred_element_type=jnp.float32)
    ).astype(jnp.bfloat16)
    own_rows = residual.shape[0]
    ntp, core = lax.axis_size("tp"), lax.axis_index("tp")
    mixed = 0.0
    for r in range(ntp):
        block = lax.dynamic_slice_in_dim(partial, lax.rem(core + r, ntp) * own_rows, own_rows)
        mixed = mixed + passed(block, "tp", r).astype(jnp.float32)
    middle_f = (residual.astype(jnp.float32) + mixed).astype(jnp.bfloat16).astype(jnp.float32)
    normed = middle_f * lax.rsqrt(jnp.mean(middle_f * middle_f, axis=-1, keepdims=True) + 1e-06)
    normed = (normed * norm_gain.astype(jnp.float32)).astype(jnp.bfloat16)
    own_rows = normed.shape[0]
    normed = normed.reshape(own_rows, na, nb, depth).swapaxes(1, 2).reshape(own_rows, model)
    all_rows = gathered(gathered(normed, "a"), "tp")
    gate = jnp.dot(all_rows, gate_all.reshape(model, chunk), preferred_element_type=jnp.float32)
    upper = jnp.dot(all_rows, up_all.reshape(model, chunk), preferred_element_type=jnp.float32)
    hidden = (jax.nn.silu(gate) * upper).astype(jnp.bfloat16)
    down = jnp.transpose(down_all, (1, 0, 2)).reshape(chunk, model)
    terms = jnp.dot(hidden, down, preferred_element_type=jnp.float32)
    back = returned(returned(terms.astype(jnp.bfloat16), "tp").astype(jnp.bfloat16), "a")
    back = back.reshape(own_rows, nb, na, out_cols).swapaxes(1, 2).reshape(own_rows, model)
    return (middle_f + back).astype(jnp.bfloat16)


def body(*args):
    sizes = tuple(lax.axis_size(x) for x in ("a", "b", "tp"))
    if fits(sizes, args):
        return layer(sizes[0], sizes[1], *args)
    return plain_body(*args)


def solution(mesh):
    sp, tp = mesh.shape["sp"], mesh.shape["tp"]
    a = 4 if sp % 4 == 0 else 1
    split = Mesh(mesh.devices.reshape(a, sp // a, tp), ("a", "b", "tp"))
    s = ("a", "b")
    in_specs = (
        P(("a", "b", "tp"), None),
        P(s, "tp"),
        P(s, "tp"),
        P(s, "tp"),
        P(s, "tp"),
        P(None, "tp", s),
        P("tp"),
        P("tp", None),
        P(s, "tp"),
        P(s, "tp"),
        P(s, "tp"),
        P(s, "tp"),
        P(None, "tp", s),
        P("tp"),
        P("tp", None),
        P(),
        P(s, "tp"),
        P(s, "tp"),
        P("tp", s),
    )
    out_specs = P(("a", "b", "tp"), None)
    return jax.shard_map(body, mesh=split, in_specs=in_specs, out_specs=out_specs, check_vma=False)
```

```python
import functools

import jax
import jax.numpy as jnp
from jax import lax
from jax.experimental import pallas as pl
from jax.experimental.pallas import tpu as pltpu
from jax.sharding import Mesh, PartitionSpec as P

DK_A = 128
DK_B = 64
LOW = -1e30
MESH = pl.DeviceIdType.MESH


def cell_kernel(
    n,
    q_w,
    k_w,
    v_w,
    og_w,
    gain_w,
    q_n,
    k_n,
    v_n,
    og_n,
    gain_n,
    gating,
    out_w,
    out_n,
    raw_w,
    raw_n,
    stabs,
    sent,
    got,
    back,
    carried,
    mem_w,
    mem_n,
    state,
    levels,
    send_sem,
    recv_sem,
    send_sem2,
    recv_sem2,
):
    na, nb = lax.axis_size("a"), lax.axis_size("b")
    tp = lax.axis_index("tp")
    me = lax.axis_index("a") * nb + lax.axis_index("b")

    def where_is(index):
        return (index // nb, lax.rem(index, nb), tp)

    barrier = pltpu.get_barrier_semaphore()

    def greet(r, _):
        peer = lax.rem(me + r, n)
        pl.semaphore_signal(barrier, inc=1, device_id=where_is(peer), device_id_type=MESH)
        return 0

    lax.fori_loop(1, n, greet, 0)

    rows = q_w.shape[0]
    heads_p = gating.shape[1]
    groups = (
        (q_w, k_w, v_w, og_w, gain_w, out_w, raw_w, mem_w, DK_A),
        (q_n, k_n, v_n, og_n, gain_n, out_n, raw_n, mem_n, DK_B),
    )
    heads = tuple(g[0].shape[1] // g[8] for g in groups)
    parts = tuple(h * g[8] // n for h, g in zip(heads, groups))
    starts = (0, parts[0])
    extra = parts[0] + parts[1]

    it = lax.broadcasted_iota(jnp.int32, (rows, rows), 0)
    js = lax.broadcasted_iota(jnp.int32, (rows, rows), 1)
    upper = (it <= js).astype(jnp.float32)
    eye = (it == js).astype(jnp.float32)
    last_dims = (((1,), (1,)), ((), ()))
    first_dims = (((0,), (0,)), ((), ()))
    gate_in = gating[0]
    x = gating[1]
    forget = jnp.minimum(x, 0.0) - jnp.log1p(jnp.exp(-jnp.abs(x))) + gating[2]
    cum = jnp.dot(
        forget, upper, precision=lax.Precision.HIGHEST, preferred_element_type=jnp.float32
    )
    cum_t = lax.dot_general(
        eye, cum, last_dims, precision=lax.Precision.HIGHEST, preferred_element_type=jnp.float32
    )
    diff = gate_in - cum
    diff_t = lax.dot_general(
        eye, diff, last_dims, precision=lax.Precision.HIGHEST, preferred_element_type=jnp.float32
    )
    total = cum[:, rows - 1 : rows]
    level = jnp.max(total + diff, axis=1, keepdims=True)
    total_t = cum_t[rows - 1 : rows, :]
    level_t = jnp.max(total_t + diff_t, axis=0, keepdims=True)
    tail_t = jnp.exp(total_t + diff_t - level_t)
    width = sent.shape[2]
    lane = lax.broadcasted_iota(jnp.int32, (heads_p, width), 1)
    marks = jnp.where(
        lane < width // 2,
        jnp.broadcast_to(level, (heads_p, width)),
        jnp.broadcast_to(total, (heads_p, width)),
    )

    index = 0
    for g, (q, k, v, _, _, _, raw, _, dk) in enumerate(groups):
        dv = v.shape[1] // heads[g]
        scale = dk ** (-0.5)
        for h in range(heads[g]):
            k_h = k[:, h * dk : (h + 1) * dk]
            v_h = v[:, h * dv : (h + 1) * dv]
            scaled = k_h.astype(jnp.float32) * (tail_t[:, index : index + 1] * scale)
            memory = lax.dot_general(
                scaled.astype(jnp.bfloat16), v_h, first_dims, preferred_element_type=jnp.float32
            )
            size = parts[g]
            per = dk // size
            for p in range(per):
                sent[h * per + p, starts[g] : starts[g] + size, :dv] = memory[
                    p * size : (p + 1) * size
                ]
            index += 1
    spare = v_n.shape[1] // heads[1]
    if spare < width:
        sent[:, starts[1] : extra, spare:] = jnp.zeros((n, parts[1], width - spare), jnp.float32)
    for p in range(n):
        sent[p, extra : extra + heads_p, :] = marks

    pl.semaphore_wait(barrier, n - 1)

    def out_copy(r):
        peer = lax.rem(me + r, n)
        return pltpu.make_async_remote_copy(
            src_ref=sent.at[peer],
            dst_ref=got.at[me],
            send_sem=send_sem.at[r],
            recv_sem=recv_sem.at[r],
            device_id=where_is(peer),
            device_id_type=MESH,
        )

    lax.fori_loop(1, n, lambda r, c: (out_copy(r).start(), c)[1], 0)
    got[me] = sent[me]

    index = 0
    for g, (q, k, v, _, _, _, raw, _, dk) in enumerate(groups):
        dv = v.shape[1] // heads[g]
        scale = dk ** (-0.5)
        for h in range(heads[g]):
            q_h = q[:, h * dk : (h + 1) * dk]
            k_h = k[:, h * dk : (h + 1) * dk]
            v_h = v[:, h * dv : (h + 1) * dv]
            scores = lax.dot_general(q_h, k_h, last_dims, preferred_element_type=jnp.float32)
            logits = cum_t[:, index : index + 1] + diff[index : index + 1, :]
            logits = jnp.where(js <= it, logits, LOW)
            stab = jnp.max(logits, axis=1, keepdims=True)
            weighted = scores * scale * jnp.exp(logits - stab)
            raw[:, h * dv : (h + 1) * dv] = jnp.dot(
                weighted.astype(jnp.bfloat16), v_h, preferred_element_type=jnp.float32
            )
            stabs[:, index : index + 1] = stab
            index += 1

    lax.fori_loop(1, n, lambda r, c: (out_copy(r).wait(), c)[1], 0)

    which = tuple(
        (me * parts[g]) // groups[g][8] + (heads[0] if g else 0) for g in range(2)
    )
    sub = lax.broadcasted_iota(jnp.int32, (heads_p, width), 0)
    picks = tuple(sub == w for w in which)

    def merge(t, _):
        level_c = levels[0]
        back[t] = state[...]
        levels[1] = jnp.where(t == me, level_c, levels[1])
        mark = got[t, extra : extra + heads_p, :]
        lev = jnp.broadcast_to(mark[:, :1], mark.shape)
        tot = jnp.broadcast_to(mark[:, width - 1 :], mark.shape)
        new = jnp.maximum(level_c + tot, lev)
        old_f = jnp.exp(level_c + tot - new)
        new_f = jnp.exp(lev - new)
        levels[0] = new
        for g in range(2):
            span = slice(starts[g], starts[g] + parts[g])

            def pick(f):
                return jnp.sum(jnp.where(picks[g], f, 0.0), axis=0, keepdims=True)

            state[span, :] = pick(old_f) * state[span, :] + pick(new_f) * got[t, span, :]
        return 0

    levels[...] = jnp.full(levels.shape, LOW, jnp.float32)
    state[...] = jnp.zeros(state.shape, jnp.float32)
    lax.fori_loop(0, n, merge, 0)
    entering = levels[1]

    def back_copy(r):
        peer = lax.rem(me + r, n)
        return pltpu.make_async_remote_copy(
            src_ref=back.at[peer],
            dst_ref=carried.at[me],
            send_sem=send_sem2.at[r],
            recv_sem=recv_sem2.at[r],
            device_id=where_is(peer),
            device_id_type=MESH,
        )

    lax.fori_loop(1, n, lambda r, c: (back_copy(r).start(), c)[1], 0)
    carried[me] = back[me]
    entering_t = lax.dot_general(
        jnp.where(
            lax.broadcasted_iota(jnp.int32, (rows, width), 1) == 0, 1.0, 0.0
        ),
        entering,
        last_dims,
        precision=lax.Precision.HIGHEST,
        preferred_element_type=jnp.float32,
    )
    shifted = cum_t + entering_t
    own = stabs[:, :heads_p]
    both = jnp.maximum(own, shifted)
    own_f = jnp.exp(own - both)
    in_f = jnp.exp(shifted - both)
    lax.fori_loop(1, n, lambda r, c: (back_copy(r).wait(), c)[1], 0)

    index = 0
    for g, (q, _, v, og, gain, out, raw, mem, dk) in enumerate(groups):
        dv = v.shape[1] // heads[g]
        size = parts[g]
        per = dk // size
        for h in range(heads[g]):
            for p in range(per):
                mem[p * size : (p + 1) * size, :] = carried[
                    h * per + p, starts[g] : starts[g] + size, :dv
                ]
            memory = mem[...]
            high = memory.astype(jnp.bfloat16)
            rest = (memory - high.astype(jnp.float32)).astype(jnp.bfloat16)
            q_h = q[:, h * dk : (h + 1) * dk]
            cols = slice(h * dv, (h + 1) * dv)
            incoming = jnp.dot(q_h, high, preferred_element_type=jnp.float32) + jnp.dot(
                q_h, rest, preferred_element_type=jnp.float32
            )
            value = (
                raw[:, cols] * own_f[:, index : index + 1]
                + incoming * in_f[:, index : index + 1]
            )
            value = value * lax.rsqrt(jnp.mean(value * value, axis=1, keepdims=True) + 1e-06)
            gate = 1.0 / (1.0 + jnp.exp(-og[:, cols].astype(jnp.float32)))
            value = value * gain[:, cols].astype(jnp.float32) * gate
            out[:, cols] = value.astype(jnp.bfloat16)
            index += 1


def cell(q_w, k_w, v_w, og_w, gat_w, gain_w, q_n, k_n, v_n, og_n, gat_n, gain_n):
    n = lax.axis_size("a") * lax.axis_size("b")
    rows = q_w.shape[0]
    heads = gat_w.shape[1] + gat_n.shape[1]
    heads_p = -(-heads // 8) * 8
    gating = jnp.concatenate([gat_w, gat_n], axis=1)
    gating = jnp.pad(gating, ((0, 0), (0, heads_p - heads), (0, 0)))
    parts = (q_w.shape[1] // n, q_n.shape[1] // n)
    width = v_w.shape[1] // gat_w.shape[1]
    width_n = v_n.shape[1] // gat_n.shape[1]
    vmem = pl.BlockSpec(memory_space=pltpu.VMEM)
    state = parts[0] + parts[1]
    return pl.pallas_call(
        functools.partial(cell_kernel, n),
        out_shape=(
            jax.ShapeDtypeStruct(v_w.shape, jnp.bfloat16),
            jax.ShapeDtypeStruct(v_n.shape, jnp.bfloat16),
        ),
        in_specs=[vmem] * 11,
        out_specs=(vmem, vmem),
        scratch_shapes=[
            pltpu.VMEM(v_w.shape, jnp.float32),
            pltpu.VMEM(v_n.shape, jnp.float32),
            pltpu.VMEM((rows, 128), jnp.float32),
            pltpu.VMEM((n, state + heads_p, width), jnp.float32),
            pltpu.VMEM((n, state + heads_p, width), jnp.float32),
            pltpu.VMEM((n, state, width), jnp.float32),
            pltpu.VMEM((n, state, width), jnp.float32),
            pltpu.VMEM((DK_A, width), jnp.float32),
            pltpu.VMEM((DK_B, width_n), jnp.float32),
            pltpu.VMEM((state, width), jnp.float32),
            pltpu.VMEM((2, heads_p, width), jnp.float32),
            pltpu.SemaphoreType.DMA((n,)),
            pltpu.SemaphoreType.DMA((n,)),
            pltpu.SemaphoreType.DMA((n,)),
            pltpu.SemaphoreType.DMA((n,)),
        ],
        compiler_params=pltpu.CompilerParams(
            collective_id=0, has_side_effects=True, vmem_limit_bytes=32 * 2**20
        ),
        cost_estimate=pl.CostEstimate(
            flops=2 * 10**9, bytes_accessed=120 * 10**6, transcendentals=0
        ),
    )(
        q_w,
        k_w,
        v_w,
        og_w,
        gain_w.reshape(1, -1),
        q_n,
        k_n,
        v_n,
        og_n,
        gain_n.reshape(1, -1),
        gating,
    )


def layer_kernel(na, nb, *refs):
    (
        residual,
        q_w,
        k_w,
        v_w,
        og_w,
        gat_w,
        gain_w,
        read_w,
        q_n,
        k_n,
        v_n,
        og_n,
        gat_n,
        gain_n,
        read_n,
        norm_gain,
        gate,
        up,
        down,
        out,
        res_v,
        qw_v,
        kw_v,
        vw_v,
        ogw_v,
        gatw_v,
        gainw_v,
        qn_v,
        kn_v,
        vn_v,
        ogn_v,
        gatn_v,
        gainn_v,
        read_v,
        ngain_v,
        edge_v,
        gu_own,
        d_own,
        gu_all,
        d_all,
        gat_v,
        raw_w,
        raw_n,
        stabs,
        sent,
        got,
        mark,
        mark_got,
        prefix,
        total_s,
        total_got,
        tmark,
        tmark_got,
        enter,
        enter_mark,
        back,
        carried,
        bmark,
        bmark_got,
        gated,
        part,
        part_got,
        middle,
        x_all,
        acc,
        hidden,
        terms,
        terms_got,
        sums,
        a_got,
        joined,
        b_got,
        out_v,
        in_sem,
        s_sem,
        p1_r,
        p2_s,
        p2_r,
        p3_r,
        z_r,
        f_r,
        t_r,
        x_r,
        y_r,
        a_r,
        b_r,
    ) = refs
    n = na * nb
    a, b, t = lax.axis_index("a"), lax.axis_index("b"), lax.axis_index("tp")
    me = a * nb + b
    f32, bf16 = jnp.float32, jnp.bfloat16

    barrier = pltpu.get_barrier_semaphore()
    peers = [(a ^ k, b, t) for k in range(1, na)]
    peers += [(a, b ^ m, t) for m in range(1, nb)]
    peers += [(a, b, 1 - t)]
    for peer in peers:
        pl.semaphore_signal(barrier, inc=1, device_id=peer, device_id_type=MESH)

    depth = gate.shape[0]
    chunk = gate.shape[1] // na
    whole = chunk // 128 * 128
    half = chunk - whole
    cols = down.shape[1]
    model = residual.shape[1]
    own_rows = residual.shape[0]
    rows = q_w.shape[0]
    kspan = nb * depth
    wide_heads, narrow_heads = gat_w.shape[1], gat_n.shape[1]
    heads = wide_heads + narrow_heads
    dv_w = v_w.shape[1] // wide_heads
    dv_n = v_n.shape[1] // narrow_heads

    def local(src, dst, i):
        pltpu.make_async_copy(src, dst, in_sem.at[i]).start()

    def landed(sem, ref):
        pltpu.make_async_copy(ref, ref, sem).wait()

    local(gat_w, gatw_v, 0)
    local(gat_n, gatn_v, 1)
    for src, dst in ((k_w, kw_v), (v_w, vw_v)):
        local(src, dst, 2)
    for src, dst in ((k_n, kn_v), (v_n, vn_v)):
        local(src, dst, 3)

    def slab_parts(c):
        odd = c % 2
        return c * chunk + odd * half, c * chunk + (1 - odd) * whole

    def d_slab(r, lo=0, size=chunk):
        return d_all.at[
            r // 2, pl.ds(lo, size), pl.ds(pl.multiple_of(lax.rem(r, 2) * cols, cols), cols)
        ]

    first, second = slab_parts(a)
    own_down = (
        pltpu.make_async_copy(
            down.at[pl.ds(pl.multiple_of(first, half), whole)],
            d_slab(me, 0, whole),
            in_sem.at[4],
        ),
        pltpu.make_async_copy(
            down.at[pl.ds(pl.multiple_of(second, half), half)],
            d_slab(me, whole, half),
            in_sem.at[5],
        ),
    )
    for c in own_down:
        c.start()
    for c in range(na):
        lo, hi = slab_parts(c)
        pltpu.make_async_copy(
            down.at[lo : lo + whole], d_own.at[c, 0:whole], in_sem.at[6]
        ).start()
        pltpu.make_async_copy(
            down.at[hi : hi + half], d_own.at[c, whole:chunk], in_sem.at[6]
        ).start()
    for i, w in enumerate((gate, up)):
        for c in range(na):
            lo, _ = slab_parts(c)
            pltpu.make_async_copy(
                w.at[:, lo : lo + whole],
                gu_own.at[c, :, i * whole : (i + 1) * whole],
                in_sem.at[7],
            ).start()
        for c in range(na // 2):
            lo = 2 * c * chunk + whole
            pltpu.make_async_copy(
                w.at[:, lo : lo + 128], edge_v.at[i, c], in_sem.at[8]
            ).start()
    local(q_w, qw_v, 9)
    local(q_n, qn_v, 10)
    local(og_w, ogw_v, 11)
    local(og_n, ogn_v, 12)
    local(gain_w, gainw_v, 13)
    local(gain_n, gainn_v, 14)
    local(read_w, read_v.at[: read_w.shape[0]], 15)
    local(read_n, read_v.at[read_w.shape[0] :], 15)
    local(residual, res_v, 16)
    local(norm_gain, ngain_v, 17)

    def remote(src, dst, s_sem, r_sem, peer):
        return pltpu.make_async_remote_copy(
            src_ref=src,
            dst_ref=dst,
            send_sem=s_sem,
            recv_sem=r_sem,
            device_id=peer,
            device_id_type=MESH,
        )

    def go(copy):
        copy.start()

    def slab(kind, r, lo, size):
        if kind == 0:
            return gu_all.at[r, pl.ds(lo, size)]
        return d_slab(r, lo, size)

    extent = (depth, chunk)

    def z_copy(kind, k, r):
        src = (gu_own, d_own)[kind].at[a ^ k]
        return remote(
            src, slab(kind, r, 0, extent[kind]), s_sem.at[2 * kind], z_r.at[kind, k], (a ^ k, b, t)
        )

    def z_start(kind, k):
        go(z_copy(kind, k, me))

    def z_wait(kind, k):
        z_copy(kind, k, (a ^ k) * nb + b).wait_recv()

    def full_copy(kind, s, d, h, who):
        size = extent[kind] // 2
        ref = slab(kind, (a ^ s) * nb + who, h * size, size)
        i = h if d == h else 2 + kind * d
        return remote(ref, ref, s_sem.at[kind], f_r.at[kind, s, i], (a, b ^ (1 << d), t))

    def full_start(kind, s):
        for d, h in ((0, 0), (1, 1), (0, 1), (1, 0)):
            go(full_copy(kind, s, d, h, b))

    def full_wait(kind, s, d, h):
        full_copy(kind, s, d, h, b ^ (1 << d)).wait_recv()

    def diag_copy(kind, s, h, who):
        size = extent[kind] // 2
        ref = slab(kind, (a ^ s) * nb + who, h * size, size)
        return remote(ref, ref, s_sem.at[kind], f_r.at[kind, s, 2 + kind], (a, b ^ (2 >> h), t))

    def relay(kind, s):
        for h in range(2):
            full_wait(kind, s, h, h)
            go(diag_copy(kind, s, h, b ^ (1 << h)))

    def arrived(s):
        landed(f_r.at[0, s, 2], gu_all.at[:2])

    landed(in_sem.at[0], gatw_v)
    landed(in_sem.at[1], gatn_v)
    gat_v[:, :wide_heads, :] = gatw_v[...]
    gat_v[:, wide_heads:, :] = gatn_v[...]
    it = lax.broadcasted_iota(jnp.int32, (rows, rows), 0)
    js = lax.broadcasted_iota(jnp.int32, (rows, rows), 1)
    upper = (it <= js).astype(f32)
    eye = (it == js).astype(f32)
    last_dims = (((1,), (1,)), ((), ()))
    first_dims = (((0,), (0,)), ((), ()))
    exact = dict(precision=lax.Precision.HIGHEST, preferred_element_type=f32)
    gate_in = gat_v[0]
    x = gat_v[1]
    forget = jnp.minimum(x, 0.0) - jnp.log1p(jnp.exp(-jnp.abs(x))) + gat_v[2]
    cum = jnp.dot(forget, upper, **exact)
    cum_t = lax.dot_general(eye, cum, last_dims, **exact)
    diff = gate_in - cum
    diff_t = lax.dot_general(eye, diff, last_dims, **exact)
    total = cum[:, rows - 1 : rows]
    level = jnp.max(total + diff, axis=1, keepdims=True)
    total_t = cum_t[rows - 1 : rows, :]
    level_t = jnp.max(total_t + diff_t, axis=0, keepdims=True)
    tail_t = jnp.exp(total_t + diff_t - level_t)
    lane = lax.broadcasted_iota(jnp.int32, (heads, 128), 1)
    mark[...] = jnp.where(
        lane < 64, jnp.broadcast_to(level, (heads, 128)), jnp.broadcast_to(total, (heads, 128))
    )

    groups = (
        (qw_v, kw_v, vw_v, ogw_v, gainw_v, raw_w, DK_A, dv_w, wide_heads, 0),
        (qn_v, kn_v, vn_v, ogn_v, gainn_v, raw_n, DK_B, dv_n, narrow_heads, wide_heads),
    )
    fold = DK_B // 2
    deep = DK_A + fold

    for c in own_down:
        c.wait()
    pltpu.make_async_copy(d_own, d_own, in_sem.at[6]).wait()
    pl.semaphore_wait(barrier, len(peers))
    z_start(1, 1)
    is_inner = (a + 1) // 2 % 2
    inner = is_inner == 1
    order = (0, 1 + 2 * is_inner, 3 - 2 * is_inner, 2)
    odd = a % 2
    group = (is_inner, 1 - is_inner, 2 + is_inner, 3 - is_inner)
    late = group[2:]


    joint = kw_v.shape[1] + vw_v.shape[1]
    landed(in_sem.at[2], read_v.at[: rows * joint // model])
    joint = kn_v.shape[1] + vn_v.shape[1]
    landed(in_sem.at[3], read_v.at[: rows * joint // model])
    for _, k, v, _, _, _, dk, dv, count, base in groups:
        scale = dk ** (-0.5)
        for h in range(count):
            i = base + h
            scaled = k[:, h * dk : (h + 1) * dk].astype(f32) * (tail_t[:, i : i + 1] * scale)
            memory = lax.dot_general(
                scaled.astype(bf16),
                v[:, h * dv : (h + 1) * dv],
                first_dims,
                preferred_element_type=f32,
            ).astype(bf16)
            if base == 0:
                sent[h, :dk, :] = memory
            else:
                sent[h, DK_A:deep, :dv] = memory[:fold]
                sent[h, DK_A:deep, dv:] = memory[fold:]

    def p1(m, r):
        peer = (a, b ^ m, t)
        return (
            remote(mark, mark_got.at[r], s_sem.at[3], p1_r.at[0, m], peer),
            remote(sent.at[b ^ m], got.at[r], s_sem.at[4], p1_r.at[1, m], peer),
        )

    for m in range(1, nb):
        for c in p1(m, b):
            go(c)
    got[b] = sent[b]
    mark_got[b] = mark[...]

    pltpu.make_async_copy(
        gu_own.at[:, :, : 2 * whole], gu_own.at[:, :, : 2 * whole], in_sem.at[7]
    ).wait()
    pltpu.make_async_copy(edge_v, edge_v, in_sem.at[8]).wait()
    for c in range(na // 2):
        ge, ue = edge_v[0, c], edge_v[1, c]
        gu_own[2 * c, :, 2 * whole :] = jnp.concatenate([ge[:, :half], ue[:, :half]], axis=1)
        gu_own[2 * c + 1, :, 2 * whole :] = jnp.concatenate([ge[:, half:], ue[:, half:]], axis=1)
    gu_all[me] = gu_own[a]

    @pl.when(inner)
    def _():
        z_copy(0, 3, me).start()

    full_start(0, 0)
    full_start(1, 0)

    landed(in_sem.at[9], qw_v)
    landed(in_sem.at[10], qn_v)
    for q, k, v, _, _, raw, dk, dv, count, base in groups:
        scale = dk ** (-0.5)
        for h in range(count):
            i = base + h
            q_h = q[:, h * dk : (h + 1) * dk]
            k_h = k[:, h * dk : (h + 1) * dk]
            v_h = v[:, h * dv : (h + 1) * dv]
            scores = lax.dot_general(q_h, k_h, last_dims, preferred_element_type=f32)
            logits = cum_t[:, i : i + 1] + diff[i : i + 1, :]
            logits = jnp.where(js <= it, logits, LOW)
            stab = jnp.max(logits, axis=1, keepdims=True)
            weighted = scores * scale * jnp.exp(logits - stab)
            raw[:, h * dv : (h + 1) * dv] = jnp.dot(
                weighted.astype(bf16), v_h, preferred_element_type=f32
            )
            stabs[:, i : i + 1] = stab

    for m in range(1, nb):
        for c in p1(m, b ^ m):
            c.wait_recv()
    spans = ((0, DK_A), (DK_A, deep))

    def read_mark(ref, where, row):
        line = ref[where, pl.ds(row, 1), :]
        return line[:, :1], line[:, 127:128]

    run = []
    for g, (lo, hi) in enumerate(spans):
        lev, tot = read_mark(mark_got, 0, b + g * wide_heads)
        state = got[0, lo:hi, :].astype(f32)
        run.append([(lev, tot)])
        for j in range(1, nb):
            prefix[j - 1, lo:hi, :] = state
            lev2, tot2 = read_mark(mark_got, j, b + g * wide_heads)
            new = jnp.maximum(lev + tot2, lev2)
            state = (
                jnp.exp(lev + tot2 - new) * state
                + jnp.exp(lev2 - new) * got[j, lo:hi, :].astype(f32)
            )
            lev, tot = new, tot + tot2
            run[g].append((lev, tot))
        total_s[lo:hi, :] = state.astype(bf16)
    lane1 = lax.broadcasted_iota(jnp.int32, (1, 128), 1)
    for g in range(2):
        lev, tot = run[g][nb - 1]
        tmark[g : g + 1, :] = jnp.where(
            lane1 < 64, jnp.broadcast_to(lev, (1, 128)), jnp.broadcast_to(tot, (1, 128))
        )

    def p2(k, r):
        peer = (a ^ k, b, t)
        return (
            remote(tmark, tmark_got.at[r], p2_s.at[0, k], p2_r.at[0, k], peer),
            remote(total_s, total_got.at[r], p2_s.at[1, k], p2_r.at[1, k], peer),
        )

    for k in range(1, na):

        @pl.when((a ^ k) > a)
        def _():
            for c in p2(k, a):
                c.start()

    @pl.when(inner)
    def _():
        z_copy(0, 2, me).start()
        z_copy(0, 1, me).start()

    @pl.when(jnp.logical_not(inner))
    def _():
        for k in range(1, na):
            z_copy(0, k, me).start()


    enter[...] = jnp.zeros(enter.shape, f32)
    enter_mark[...] = jnp.full(enter_mark.shape, LOW, f32)
    for k in range(1, na):

        @pl.when((a ^ k) < a)
        def _():
            for c in p2(k, a ^ k):
                c.wait_recv()

    for z in range(na - 1):

        @pl.when(z < a)
        def _():
            for g, (lo, hi) in enumerate(spans):
                lev = enter_mark[g : g + 1, :1]
                lev2, tot2 = read_mark(tmark_got, z, g)
                new = jnp.maximum(lev + tot2, lev2)
                enter[lo:hi, :] = (
                    jnp.exp(lev + tot2 - new) * enter[lo:hi, :]
                    + jnp.exp(lev2 - new) * total_got[z, lo:hi, :].astype(f32)
                )
                enter_mark[g : g + 1, :] = jnp.broadcast_to(new, (1, 128))

    for g, (lo, hi) in enumerate(spans):
        lev = enter_mark[g : g + 1, :1]
        back[0, lo:hi, :] = enter[lo:hi, :].astype(bf16)
        bmark[0, g : g + 1, :] = jnp.broadcast_to(lev, (1, 128))
        for j in range(1, nb):
            lev2, tot2 = run[g][j - 1]
            new = jnp.maximum(lev + tot2, lev2)
            back[j, lo:hi, :] = (
                jnp.exp(lev + tot2 - new) * enter[lo:hi, :]
                + jnp.exp(lev2 - new) * prefix[j - 1, lo:hi, :]
            ).astype(bf16)
            bmark[j, g : g + 1, :] = jnp.broadcast_to(new, (1, 128))

    def p3(m, r):
        peer = (a, b ^ m, t)
        return (
            remote(bmark.at[b ^ m], bmark_got.at[r], s_sem.at[5], p3_r.at[0, m], peer),
            remote(back.at[b ^ m], carried.at[r], s_sem.at[6], p3_r.at[1, m], peer),
        )

    for m in range(1, nb):
        for c in p3(m, b):
            go(c)
    carried[b] = back[b]
    bmark_got[b] = bmark[b]
    relay(0, 0)
    relay(1, 0)

    for i, ref in enumerate((ogw_v, ogn_v, gainw_v, gainn_v)):
        landed(in_sem.at[11 + i], ref)
    for m in range(1, nb):
        for c in p3(m, b ^ m):
            c.wait_recv()

    for g, (q, _, _, og, gain, raw, dk, dv, count, base) in enumerate(groups):
        for h in range(count):
            i = base + h
            if g == 0:
                memory = carried[h, :dk, :]
            else:
                memory = jnp.concatenate(
                    [carried[h, DK_A:deep, :dv], carried[h, DK_A:deep, dv:]], axis=0
                )
            own = stabs[:, i : i + 1]
            shifted = cum_t[:, i : i + 1] + bmark_got[h, g : g + 1, :1]
            both = jnp.maximum(own, shifted)
            span_h = slice(h * dv, (h + 1) * dv)
            incoming = jnp.dot(
                q[:, h * dk : (h + 1) * dk], memory, preferred_element_type=f32
            )
            value = raw[:, span_h] * jnp.exp(own - both) + incoming * jnp.exp(shifted - both)
            value = value * lax.rsqrt(jnp.mean(value * value, axis=1, keepdims=True) + 1e-06)
            gate_h = 1.0 / (1.0 + jnp.exp(-og[:, span_h].astype(f32)))
            value = value * gain[span_h].astype(f32).reshape(1, dv) * gate_h
            lo = g * raw_w.shape[1] + h * dv
            gated[:, lo : lo + dv] = value.astype(bf16)

    z_wait(0, order[1])
    full_start(0, order[1])

    for i, ref in enumerate((read_v, res_v, ngain_v)):
        landed(in_sem.at[15 + i], ref)
    tile = model // 4
    for j in range(model // tile):
        sl = slice(j * tile, (j + 1) * tile)
        p = jnp.dot(gated[...], read_v[:, sl], preferred_element_type=f32).astype(bf16)
        part[:, :, sl] = p.reshape(2, own_rows, tile)
    partner = (a, b, 1 - t)
    swap = remote(part.at[1 - t], part_got, s_sem.at[7], t_r.at[0], partner)
    go(swap)
    swap.wait_recv()
    mixed = part[t].astype(f32) + part_got[...].astype(f32)
    mid = (res_v[...].astype(f32) + mixed).astype(bf16)
    middle[...] = mid
    mid = mid.astype(f32)
    normed = mid * lax.rsqrt(jnp.mean(mid * mid, axis=-1, keepdims=True) + 1e-06)
    block = 2 * own_rows

    piece = own_rows // 2

    def row_block(z, core, c, size=piece):
        lo = (z * 2 + core) * own_rows + c * piece
        return x_all.at[pl.ds(pl.multiple_of(lo, piece), size)]

    x_all[pl.ds(pl.multiple_of((a * 2 + t) * own_rows, own_rows), own_rows), :] = (
        normed * ngain_v[...].astype(f32).reshape(1, model)
    ).astype(bf16)

    def x_copy(i, k, z, c):
        ref = row_block(z, t, c)
        return remote(ref, ref, s_sem.at[9], x_r.at[i, c], (a ^ k, b, t))

    def y_copy(z, core, c):
        ref = row_block(z, core, c)
        return remote(ref, ref, s_sem.at[10], y_r.at[0], partner)

    for c in range(2):
        go(x_copy(0, 2, a, c))
    for c in range(2):
        go(x_copy(1, 1, a, c))
    for c in range(2):
        go(y_copy(a, t, c))

    @pl.when(inner)
    def _():
        z_copy(1, 3, me).start()
        z_copy(1, 2, me).start()

    width = gu_all.shape[2]
    tiles = [(lo, min(lo + 512, width)) for lo in range(0, width, 512)]

    def unit(lo, m, s, fresh):
        z = a ^ s
        xs = x_all[pl.ds(lo, m), pl.ds(pl.multiple_of(z * kspan, kspan), kspan)]
        for c0, c1 in tiles:
            w = gu_all[pl.ds(z * nb, nb), :, c0:c1].reshape(kspan, c1 - c0)
            p = jnp.dot(xs, w, preferred_element_type=f32)
            if fresh:
                acc[pl.ds(lo, m), c0:c1] = p
            else:
                acc[pl.ds(lo, m), c0:c1] += p

    def passed_on(i, k):
        z = a ^ k
        for c in range(2):
            x_copy(i, 1 if i else 2, z, c).wait_recv()
            if i == 0:
                go(x_copy(2, 1, z, c))
            go(y_copy(z, t, c))

    z_wait(0, order[2])
    full_start(0, order[2])
    relay(0, order[1])
    z_wait(0, order[3])
    full_start(0, order[3])
    relay(0, order[2])
    passed_on(0, 2)

    @pl.when(jnp.logical_not(inner))
    def _():
        z_copy(1, 2, me).start()
        z_copy(1, 3, me).start()


    passed_on(1, 1)
    z_wait(1, 1)
    full_start(1, 1)
    relay(0, order[3])
    passed_on(2, 3)
    total_rows = na * block
    landed(y_r.at[0], x_all.at[: total_rows // 2])
    for s in range(na):
        if s == 3:
            relay(1, 1)
            z_wait(1, late[0])
            full_start(1, late[0])
        arrived(order[s])
        unit(0, total_rows, order[s], s == 0)

    for j in range(2):
        sl = slice(j * total_rows // 2, (j + 1) * total_rows // 2)
        gt = acc[sl, :whole]
        hidden[sl, :whole] = (
            gt * (1.0 / (1.0 + jnp.exp(-gt))) * acc[sl, whole : 2 * whole]
        ).astype(bf16)
        mx = acc[sl, 2 * whole :]
        hx = mx * (1.0 / (1.0 + jnp.exp(-mx))) * pltpu.roll(mx, half, 1)
        hidden[sl, whole:] = hx[:, :half].astype(bf16)
    z_wait(1, late[1])
    full_start(1, late[1])

    side = b // 2
    high = a // 2
    unit_cols = 2 * cols

    def t_copy(u):
        return remote(
            terms.at[u, :, 1 - t], terms_got.at[u], s_sem.at[8], t_r.at[1 + u], partner
        )

    def other(u):
        return 2 * (na - 1 - u // 2) + u % 2

    def place(u):
        return (a ^ group[u // 2]) * 2 + (side + u) % 2

    def down_unit(u):
        g = group[u // 2]
        if u % 2 == 0:
            full_wait(1, g, 0, 1)
        else:
            landed(f_r.at[1, g, 3], d_all.at[0, : 3 * chunk // 4])
        v = jnp.dot(hidden[...], d_all[place(u)], preferred_element_type=f32)
        terms[u] = v.astype(bf16).reshape(terms.shape[1:])
        go(t_copy(u))

    def a_copy(u):
        return remote(sums.at[u, :, 1 - odd], a_got.at[u], s_sem.at[11], a_r.at[u], (a ^ 1, b, t))

    def b_copy(u, w):
        return remote(joined.at[u], b_got.at[w], s_sem.at[12], b_r.at[w], (a ^ 2, b, t))

    def sum_unit(u):
        t_copy(u).wait_recv()
        sums[u] = (
            (terms[u, :, t].astype(f32) + terms_got[u].astype(f32))
            .astype(bf16)
            .reshape(sums.shape[1:])
        )
        go(a_copy(u))

    def join_unit(u):
        a_copy(u).wait_recv()
        joined[u] = (
            sums[u, 1 - high, odd].astype(f32) + a_got[u, 1 - high].astype(f32)
        ).astype(bf16)
        go(b_copy(u, other(u)))

    def finish_unit(u):
        b_copy(u, u).wait_recv()
        v = sums[u, high, odd].astype(f32) + a_got[u, high].astype(f32)
        v = v + b_got[u].astype(f32)
        c0 = pl.ds(pl.multiple_of(place(u) * unit_cols, unit_cols), unit_cols)
        out_v[:, c0] = (middle[:, c0].astype(f32) + v).astype(bf16)
        local(out_v.at[:, c0], out.at[:, c0], 0)

    down_unit(0)
    down_unit(1)
    sum_unit(0)
    sum_unit(1)
    down_unit(2)
    down_unit(3)
    relay(1, late[0])
    sum_unit(2)
    sum_unit(3)
    join_unit(0)
    join_unit(1)
    down_unit(4)
    join_unit(2)
    relay(1, late[1])
    join_unit(3)
    sum_unit(4)
    down_unit(5)
    sum_unit(5)
    down_unit(6)
    sum_unit(6)
    down_unit(7)
    join_unit(4)
    sum_unit(7)
    join_unit(5)
    join_unit(6)
    join_unit(7)
    for u in (4, 5, 2, 3, 6, 7, 0, 1):
        finish_unit(u)

    sends = (
        gu_all.at[: n - 1],
        d_all.at[: 3 * n // 8],
        d_own.at[: na - 1],
        mark_got.at[: nb - 1],
        got.at[: nb - 1],
        bmark_got.at[: nb - 1],
        carried.at[: nb - 1],
        part_got,
        terms_got,
        x_all.at[: 3 * own_rows],
        x_all.at[: total_rows // 2],
        a_got,
        b_got,
    )
    for i, ref in enumerate(sends):
        landed(s_sem.at[i], ref)
    for k in range(1, na):

        @pl.when((a ^ k) > a)
        def _():
            for c in p2(k, a):
                c.wait_send()

    landed(in_sem.at[0], out_v)


def layer(na, nb, *args):
    (res, q_w, k_w, v_w, og_w, gat_w, gain_w, read_w) = args[:8]
    (q_n, k_n, v_n, og_n, gat_n, gain_n, read_n, norm_gain, gate, up, down) = args[8:]
    bf16, f32 = jnp.bfloat16, jnp.float32
    n = na * nb
    depth = gate.shape[0]
    chunk = gate.shape[1] // na
    whole = chunk // 128 * 128
    width = 2 * whole + 128
    cols = down.shape[1]
    own_rows, model = res.shape
    rows = q_w.shape[0]
    heads = gat_w.shape[1] + gat_n.shape[1]
    deep = DK_A + DK_B // 2
    dv = v_w.shape[1] // gat_w.shape[1]
    total_rows = na * 2 * own_rows
    units = n // 2

    def vm(shape, dtype=bf16):
        return pltpu.VMEM(shape, dtype)

    def like(x):
        return pltpu.VMEM(x.shape, x.dtype)

    dma = pltpu.SemaphoreType.DMA
    scratch = [
        like(res),
        like(q_w),
        like(k_w),
        like(v_w),
        like(og_w),
        like(gat_w),
        like(gain_w),
        like(q_n),
        like(k_n),
        like(v_n),
        like(og_n),
        like(gat_n),
        like(gain_n),
        vm((read_w.shape[0] + read_n.shape[0], model)),
        like(norm_gain),
        vm((2, na // 2, depth, 128)),
        vm((na, depth, width)),
        vm((na, chunk, cols)),
        vm((n, depth, width)),
        vm((n // 2, chunk, 2 * cols)),
        vm((3, heads, rows), f32),
        vm(v_w.shape, f32),
        vm(v_n.shape, f32),
        vm((rows, 128), f32),
        vm((nb, deep, dv)),
        vm((nb, deep, dv)),
        vm((heads, 128), f32),
        vm((nb, heads, 128), f32),
        vm((nb - 1, deep, dv), f32),
        vm((deep, dv)),
        vm((na, deep, dv)),
        vm((8, 128), f32),
        vm((na, 8, 128), f32),
        vm((deep, dv), f32),
        vm((8, 128), f32),
        vm((nb, deep, dv)),
        vm((nb, deep, dv)),
        vm((nb, 8, 128), f32),
        vm((nb, 8, 128), f32),
        vm((rows, v_w.shape[1] + v_n.shape[1])),
        vm((2, own_rows, model)),
        vm((own_rows, model)),
        vm((own_rows, model)),
        vm((total_rows, model)),
        vm((total_rows, width), f32),
        vm((total_rows, chunk)),
        vm((units, na, 2, own_rows, 2 * cols)),
        vm((units, na, own_rows, 2 * cols)),
        vm((units, na // 2, 2, own_rows, 2 * cols)),
        vm((units, na // 2, own_rows, 2 * cols)),
        vm((units, own_rows, 2 * cols)),
        vm((units, own_rows, 2 * cols)),
        vm(res.shape),
        dma((18,)),
        dma((13,)),
        dma((2, nb)),
        dma((2, na)),
        dma((2, na)),
        dma((2, nb)),
        dma((2, na)),
        dma((2, na, 4)),
        dma((1 + units,)),
        dma((3, 2)),
        dma((1,)),
        dma((units,)),
        dma((units,)),
    ]
    hbm = pl.BlockSpec(memory_space=pl.ANY)
    return pl.pallas_call(
        functools.partial(layer_kernel, na, nb),
        out_shape=jax.ShapeDtypeStruct(res.shape, bf16),
        in_specs=[hbm] * 19,
        out_specs=hbm,
        scratch_shapes=scratch,
        compiler_params=pltpu.CompilerParams(
            collective_id=0, has_side_effects=True, vmem_limit_bytes=60 * 2**20
        ),
    )(
        res,
        q_w,
        k_w,
        v_w,
        og_w,
        gat_w,
        gain_w,
        read_w,
        q_n,
        k_n,
        v_n,
        og_n,
        gat_n,
        gain_n,
        read_n,
        norm_gain,
        gate,
        up,
        down,
    )


def fits(mesh_shape, args):
    na, nb, ntp = mesh_shape
    gate, gat_w, gat_n = args[16], args[5], args[12]
    q_w, v_w, v_n = args[1], args[3], args[10]
    heads_w, heads_n = gat_w.shape[1], gat_n.shape[1]
    return (
        na == nb == 4
        and ntp == 2
        and gate.shape[1] % na == 0
        and gate.shape[1] // na % 128 == 64
        and heads_w == heads_n == nb
        and q_w.shape[0] == 128
        and v_w.shape[1] // heads_w == 2 * (v_n.shape[1] // heads_n)
    )


def passed(block, axis, step):
    size = lax.axis_size(axis)
    if step % size == 0:
        return block
    return lax.ppermute(block, axis, [(i, (i + step) % size) for i in range(size)])


def gathered(block, axis):
    return jnp.concatenate([passed(block, axis, r) for r in range(lax.axis_size(axis))], axis=0)


def returned(blocks, axis):
    size = lax.axis_size(axis)
    rows = blocks.shape[0] // size
    pieces = [passed(blocks[r * rows : (r + 1) * rows], axis, -r) for r in range(size)]
    return sum(p.astype(jnp.float32) for p in pieces)


def plain_body(
    residual,
    query_wide,
    key_wide,
    value_wide,
    outgate_wide,
    gating_wide,
    gain_wide,
    readout_wide,
    query_narrow,
    key_narrow,
    value_narrow,
    outgate_narrow,
    gating_narrow,
    gain_narrow,
    readout_narrow,
    norm_gain,
    gate_weight,
    up_weight,
    down_weight,
):
    na, nb = lax.axis_size("a"), lax.axis_size("b")
    depth, hidden_tp = gate_weight.shape
    chunk = hidden_tp // na
    out_cols = down_weight.shape[1]
    model = residual.shape[1]

    def spread(pieces):
        return lax.all_to_all(pieces, "a", split_axis=0, concat_axis=0, tiled=True)

    mine = (
        spread(jnp.moveaxis(gate_weight.reshape(depth, na, chunk), 1, 0)),
        spread(jnp.moveaxis(up_weight.reshape(depth, na, chunk), 1, 0)),
        spread(down_weight.reshape(na, chunk, out_cols)),
    )
    gate_all, up_all, down_all = (
        lax.all_gather(m, "b", axis=0, tiled=True) for m in mine
    )
    *_, gating_wide, gating_narrow = lax.optimization_barrier(
        (*mine, gating_wide, gating_narrow)
    )

    gated_w, gated_n = cell(
        query_wide,
        key_wide,
        value_wide,
        outgate_wide,
        gating_wide,
        gain_wide,
        query_narrow,
        key_narrow,
        value_narrow,
        outgate_narrow,
        gating_narrow,
        gain_narrow,
    )
    partial = (
        jnp.dot(gated_w, readout_wide, preferred_element_type=jnp.float32)
        + jnp.dot(gated_n, readout_narrow, preferred_element_type=jnp.float32)
    ).astype(jnp.bfloat16)
    own_rows = residual.shape[0]
    ntp, core = lax.axis_size("tp"), lax.axis_index("tp")
    mixed = 0.0
    for r in range(ntp):
        block = lax.dynamic_slice_in_dim(partial, lax.rem(core + r, ntp) * own_rows, own_rows)
        mixed = mixed + passed(block, "tp", r).astype(jnp.float32)
    middle_f = (residual.astype(jnp.float32) + mixed).astype(jnp.bfloat16).astype(jnp.float32)
    normed = middle_f * lax.rsqrt(jnp.mean(middle_f * middle_f, axis=-1, keepdims=True) + 1e-06)
    normed = (normed * norm_gain.astype(jnp.float32)).astype(jnp.bfloat16)
    own_rows = normed.shape[0]
    normed = normed.reshape(own_rows, na, nb, depth).swapaxes(1, 2).reshape(own_rows, model)
    all_rows = gathered(gathered(normed, "a"), "tp")
    gate = jnp.dot(all_rows, gate_all.reshape(model, chunk), preferred_element_type=jnp.float32)
    upper = jnp.dot(all_rows, up_all.reshape(model, chunk), preferred_element_type=jnp.float32)
    hidden = (jax.nn.silu(gate) * upper).astype(jnp.bfloat16)
    down = jnp.transpose(down_all, (1, 0, 2)).reshape(chunk, model)
    terms = jnp.dot(hidden, down, preferred_element_type=jnp.float32)
    back = returned(returned(terms.astype(jnp.bfloat16), "tp").astype(jnp.bfloat16), "a")
    back = back.reshape(own_rows, nb, na, out_cols).swapaxes(1, 2).reshape(own_rows, model)
    return (middle_f + back).astype(jnp.bfloat16)


def body(*args):
    sizes = tuple(lax.axis_size(x) for x in ("a", "b", "tp"))
    if fits(sizes, args):
        return layer(sizes[0], sizes[1], *args)
    return plain_body(*args)


def solution(mesh):
    sp, tp = mesh.shape["sp"], mesh.shape["tp"]
    a = 4 if sp % 4 == 0 else 1
    split = Mesh(mesh.devices.reshape(a, sp // a, tp), ("a", "b", "tp"))
    s = ("a", "b")
    in_specs = (
        P(("a", "b", "tp"), None),
        P(s, "tp"),
        P(s, "tp"),
        P(s, "tp"),
        P(s, "tp"),
        P(None, "tp", s),
        P("tp"),
        P("tp", None),
        P(s, "tp"),
        P(s, "tp"),
        P(s, "tp"),
        P(s, "tp"),
        P(None, "tp", s),
        P("tp"),
        P("tp", None),
        P(),
        P(s, "tp"),
        P(s, "tp"),
        P("tp", s),
    )
    out_specs = P(("a", "b", "tp"), None)
    return jax.shard_map(body, mesh=split, in_specs=in_specs, out_specs=out_specs, check_vma=False)
```

```python
import functools

import jax
import jax.numpy as jnp
from jax import lax
from jax.experimental import pallas as pl
from jax.experimental.pallas import tpu as pltpu
from jax.sharding import Mesh, PartitionSpec as P

DK_A = 128
DK_B = 64
LOW = -1e30
MESH = pl.DeviceIdType.MESH


def cell_kernel(
    n,
    q_w,
    k_w,
    v_w,
    og_w,
    gain_w,
    q_n,
    k_n,
    v_n,
    og_n,
    gain_n,
    gating,
    out_w,
    out_n,
    raw_w,
    raw_n,
    stabs,
    sent,
    got,
    back,
    carried,
    mem_w,
    mem_n,
    state,
    levels,
    send_sem,
    recv_sem,
    send_sem2,
    recv_sem2,
):
    na, nb = lax.axis_size("a"), lax.axis_size("b")
    tp = lax.axis_index("tp")
    me = lax.axis_index("a") * nb + lax.axis_index("b")

    def where_is(index):
        return (index // nb, lax.rem(index, nb), tp)

    barrier = pltpu.get_barrier_semaphore()

    def greet(r, _):
        peer = lax.rem(me + r, n)
        pl.semaphore_signal(barrier, inc=1, device_id=where_is(peer), device_id_type=MESH)
        return 0

    lax.fori_loop(1, n, greet, 0)

    rows = q_w.shape[0]
    heads_p = gating.shape[1]
    groups = (
        (q_w, k_w, v_w, og_w, gain_w, out_w, raw_w, mem_w, DK_A),
        (q_n, k_n, v_n, og_n, gain_n, out_n, raw_n, mem_n, DK_B),
    )
    heads = tuple(g[0].shape[1] // g[8] for g in groups)
    parts = tuple(h * g[8] // n for h, g in zip(heads, groups))
    starts = (0, parts[0])
    extra = parts[0] + parts[1]

    it = lax.broadcasted_iota(jnp.int32, (rows, rows), 0)
    js = lax.broadcasted_iota(jnp.int32, (rows, rows), 1)
    upper = (it <= js).astype(jnp.float32)
    eye = (it == js).astype(jnp.float32)
    last_dims = (((1,), (1,)), ((), ()))
    first_dims = (((0,), (0,)), ((), ()))
    gate_in = gating[0]
    x = gating[1]
    forget = jnp.minimum(x, 0.0) - jnp.log1p(jnp.exp(-jnp.abs(x))) + gating[2]
    cum = jnp.dot(
        forget, upper, precision=lax.Precision.HIGHEST, preferred_element_type=jnp.float32
    )
    cum_t = lax.dot_general(
        eye, cum, last_dims, precision=lax.Precision.HIGHEST, preferred_element_type=jnp.float32
    )
    diff = gate_in - cum
    diff_t = lax.dot_general(
        eye, diff, last_dims, precision=lax.Precision.HIGHEST, preferred_element_type=jnp.float32
    )
    total = cum[:, rows - 1 : rows]
    level = jnp.max(total + diff, axis=1, keepdims=True)
    total_t = cum_t[rows - 1 : rows, :]
    level_t = jnp.max(total_t + diff_t, axis=0, keepdims=True)
    tail_t = jnp.exp(total_t + diff_t - level_t)
    width = sent.shape[2]
    lane = lax.broadcasted_iota(jnp.int32, (heads_p, width), 1)
    marks = jnp.where(
        lane < width // 2,
        jnp.broadcast_to(level, (heads_p, width)),
        jnp.broadcast_to(total, (heads_p, width)),
    )

    index = 0
    for g, (q, k, v, _, _, _, raw, _, dk) in enumerate(groups):
        dv = v.shape[1] // heads[g]
        scale = dk ** (-0.5)
        for h in range(heads[g]):
            k_h = k[:, h * dk : (h + 1) * dk]
            v_h = v[:, h * dv : (h + 1) * dv]
            scaled = k_h.astype(jnp.float32) * (tail_t[:, index : index + 1] * scale)
            memory = lax.dot_general(
                scaled.astype(jnp.bfloat16), v_h, first_dims, preferred_element_type=jnp.float32
            )
            size = parts[g]
            per = dk // size
            for p in range(per):
                sent[h * per + p, starts[g] : starts[g] + size, :dv] = memory[
                    p * size : (p + 1) * size
                ]
            index += 1
    spare = v_n.shape[1] // heads[1]
    if spare < width:
        sent[:, starts[1] : extra, spare:] = jnp.zeros((n, parts[1], width - spare), jnp.float32)
    for p in range(n):
        sent[p, extra : extra + heads_p, :] = marks

    pl.semaphore_wait(barrier, n - 1)

    def out_copy(r):
        peer = lax.rem(me + r, n)
        return pltpu.make_async_remote_copy(
            src_ref=sent.at[peer],
            dst_ref=got.at[me],
            send_sem=send_sem.at[r],
            recv_sem=recv_sem.at[r],
            device_id=where_is(peer),
            device_id_type=MESH,
        )

    lax.fori_loop(1, n, lambda r, c: (out_copy(r).start(), c)[1], 0)
    got[me] = sent[me]

    index = 0
    for g, (q, k, v, _, _, _, raw, _, dk) in enumerate(groups):
        dv = v.shape[1] // heads[g]
        scale = dk ** (-0.5)
        for h in range(heads[g]):
            q_h = q[:, h * dk : (h + 1) * dk]
            k_h = k[:, h * dk : (h + 1) * dk]
            v_h = v[:, h * dv : (h + 1) * dv]
            scores = lax.dot_general(q_h, k_h, last_dims, preferred_element_type=jnp.float32)
            logits = cum_t[:, index : index + 1] + diff[index : index + 1, :]
            logits = jnp.where(js <= it, logits, LOW)
            stab = jnp.max(logits, axis=1, keepdims=True)
            weighted = scores * scale * jnp.exp(logits - stab)
            raw[:, h * dv : (h + 1) * dv] = jnp.dot(
                weighted.astype(jnp.bfloat16), v_h, preferred_element_type=jnp.float32
            )
            stabs[:, index : index + 1] = stab
            index += 1

    lax.fori_loop(1, n, lambda r, c: (out_copy(r).wait(), c)[1], 0)

    which = tuple(
        (me * parts[g]) // groups[g][8] + (heads[0] if g else 0) for g in range(2)
    )
    sub = lax.broadcasted_iota(jnp.int32, (heads_p, width), 0)
    picks = tuple(sub == w for w in which)

    def merge(t, _):
        level_c = levels[0]
        back[t] = state[...]
        levels[1] = jnp.where(t == me, level_c, levels[1])
        mark = got[t, extra : extra + heads_p, :]
        lev = jnp.broadcast_to(mark[:, :1], mark.shape)
        tot = jnp.broadcast_to(mark[:, width - 1 :], mark.shape)
        new = jnp.maximum(level_c + tot, lev)
        old_f = jnp.exp(level_c + tot - new)
        new_f = jnp.exp(lev - new)
        levels[0] = new
        for g in range(2):
            span = slice(starts[g], starts[g] + parts[g])

            def pick(f):
                return jnp.sum(jnp.where(picks[g], f, 0.0), axis=0, keepdims=True)

            state[span, :] = pick(old_f) * state[span, :] + pick(new_f) * got[t, span, :]
        return 0

    levels[...] = jnp.full(levels.shape, LOW, jnp.float32)
    state[...] = jnp.zeros(state.shape, jnp.float32)
    lax.fori_loop(0, n, merge, 0)
    entering = levels[1]

    def back_copy(r):
        peer = lax.rem(me + r, n)
        return pltpu.make_async_remote_copy(
            src_ref=back.at[peer],
            dst_ref=carried.at[me],
            send_sem=send_sem2.at[r],
            recv_sem=recv_sem2.at[r],
            device_id=where_is(peer),
            device_id_type=MESH,
        )

    lax.fori_loop(1, n, lambda r, c: (back_copy(r).start(), c)[1], 0)
    carried[me] = back[me]
    entering_t = lax.dot_general(
        jnp.where(
            lax.broadcasted_iota(jnp.int32, (rows, width), 1) == 0, 1.0, 0.0
        ),
        entering,
        last_dims,
        precision=lax.Precision.HIGHEST,
        preferred_element_type=jnp.float32,
    )
    shifted = cum_t + entering_t
    own = stabs[:, :heads_p]
    both = jnp.maximum(own, shifted)
    own_f = jnp.exp(own - both)
    in_f = jnp.exp(shifted - both)
    lax.fori_loop(1, n, lambda r, c: (back_copy(r).wait(), c)[1], 0)

    index = 0
    for g, (q, _, v, og, gain, out, raw, mem, dk) in enumerate(groups):
        dv = v.shape[1] // heads[g]
        size = parts[g]
        per = dk // size
        for h in range(heads[g]):
            for p in range(per):
                mem[p * size : (p + 1) * size, :] = carried[
                    h * per + p, starts[g] : starts[g] + size, :dv
                ]
            memory = mem[...]
            high = memory.astype(jnp.bfloat16)
            rest = (memory - high.astype(jnp.float32)).astype(jnp.bfloat16)
            q_h = q[:, h * dk : (h + 1) * dk]
            cols = slice(h * dv, (h + 1) * dv)
            incoming = jnp.dot(q_h, high, preferred_element_type=jnp.float32) + jnp.dot(
                q_h, rest, preferred_element_type=jnp.float32
            )
            value = (
                raw[:, cols] * own_f[:, index : index + 1]
                + incoming * in_f[:, index : index + 1]
            )
            value = value * lax.rsqrt(jnp.mean(value * value, axis=1, keepdims=True) + 1e-06)
            gate = 1.0 / (1.0 + jnp.exp(-og[:, cols].astype(jnp.float32)))
            value = value * gain[:, cols].astype(jnp.float32) * gate
            out[:, cols] = value.astype(jnp.bfloat16)
            index += 1


def cell(q_w, k_w, v_w, og_w, gat_w, gain_w, q_n, k_n, v_n, og_n, gat_n, gain_n):
    n = lax.axis_size("a") * lax.axis_size("b")
    rows = q_w.shape[0]
    heads = gat_w.shape[1] + gat_n.shape[1]
    heads_p = -(-heads // 8) * 8
    gating = jnp.concatenate([gat_w, gat_n], axis=1)
    gating = jnp.pad(gating, ((0, 0), (0, heads_p - heads), (0, 0)))
    parts = (q_w.shape[1] // n, q_n.shape[1] // n)
    width = v_w.shape[1] // gat_w.shape[1]
    width_n = v_n.shape[1] // gat_n.shape[1]
    vmem = pl.BlockSpec(memory_space=pltpu.VMEM)
    state = parts[0] + parts[1]
    return pl.pallas_call(
        functools.partial(cell_kernel, n),
        out_shape=(
            jax.ShapeDtypeStruct(v_w.shape, jnp.bfloat16),
            jax.ShapeDtypeStruct(v_n.shape, jnp.bfloat16),
        ),
        in_specs=[vmem] * 11,
        out_specs=(vmem, vmem),
        scratch_shapes=[
            pltpu.VMEM(v_w.shape, jnp.float32),
            pltpu.VMEM(v_n.shape, jnp.float32),
            pltpu.VMEM((rows, 128), jnp.float32),
            pltpu.VMEM((n, state + heads_p, width), jnp.float32),
            pltpu.VMEM((n, state + heads_p, width), jnp.float32),
            pltpu.VMEM((n, state, width), jnp.float32),
            pltpu.VMEM((n, state, width), jnp.float32),
            pltpu.VMEM((DK_A, width), jnp.float32),
            pltpu.VMEM((DK_B, width_n), jnp.float32),
            pltpu.VMEM((state, width), jnp.float32),
            pltpu.VMEM((2, heads_p, width), jnp.float32),
            pltpu.SemaphoreType.DMA((n,)),
            pltpu.SemaphoreType.DMA((n,)),
            pltpu.SemaphoreType.DMA((n,)),
            pltpu.SemaphoreType.DMA((n,)),
        ],
        compiler_params=pltpu.CompilerParams(
            collective_id=0, has_side_effects=True, vmem_limit_bytes=32 * 2**20
        ),
        cost_estimate=pl.CostEstimate(
            flops=2 * 10**9, bytes_accessed=120 * 10**6, transcendentals=0
        ),
    )(
        q_w,
        k_w,
        v_w,
        og_w,
        gain_w.reshape(1, -1),
        q_n,
        k_n,
        v_n,
        og_n,
        gain_n.reshape(1, -1),
        gating,
    )


def layer_kernel(na, nb, *refs):
    (
        residual,
        q_w,
        k_w,
        v_w,
        og_w,
        gat_w,
        gain_w,
        read_w,
        q_n,
        k_n,
        v_n,
        og_n,
        gat_n,
        gain_n,
        read_n,
        norm_gain,
        gate,
        up,
        down,
        out,
        res_v,
        qw_v,
        kw_v,
        vw_v,
        ogw_v,
        gatw_v,
        gainw_v,
        qn_v,
        kn_v,
        vn_v,
        ogn_v,
        gatn_v,
        gainn_v,
        read_v,
        ngain_v,
        edge_v,
        gu_own,
        d_own,
        gu_all,
        d_all,
        gat_v,
        raw_w,
        raw_n,
        stabs,
        sent,
        got,
        mark,
        mark_got,
        prefix,
        total_s,
        total_got,
        tmark,
        tmark_got,
        enter,
        enter_mark,
        back,
        carried,
        bmark,
        bmark_got,
        gated,
        part,
        part_got,
        middle,
        x_all,
        acc,
        hidden,
        terms,
        terms_got,
        sums,
        a_got,
        joined,
        b_got,
        out_v,
        in_sem,
        s_sem,
        p1_r,
        p2_s,
        p2_r,
        p3_r,
        z_r,
        f_r,
        t_r,
        x_r,
        y_r,
        a_r,
        b_r,
    ) = refs
    n = na * nb
    a, b, t = lax.axis_index("a"), lax.axis_index("b"), lax.axis_index("tp")
    me = a * nb + b
    f32, bf16 = jnp.float32, jnp.bfloat16

    barrier = pltpu.get_barrier_semaphore()
    peers = [(a ^ k, b, t) for k in range(1, na)]
    peers += [(a, b ^ m, t) for m in range(1, nb)]
    peers += [(a, b, 1 - t)]
    for peer in peers:
        pl.semaphore_signal(barrier, inc=1, device_id=peer, device_id_type=MESH)

    depth = gate.shape[0]
    chunk = gate.shape[1] // na
    whole = chunk // 128 * 128
    half = chunk - whole
    cols = down.shape[1]
    model = residual.shape[1]
    own_rows = residual.shape[0]
    rows = q_w.shape[0]
    kspan = nb * depth
    wide_heads, narrow_heads = gat_w.shape[1], gat_n.shape[1]
    heads = wide_heads + narrow_heads
    dv_w = v_w.shape[1] // wide_heads
    dv_n = v_n.shape[1] // narrow_heads

    def local(src, dst, i):
        pltpu.make_async_copy(src, dst, in_sem.at[i]).start()

    def landed(sem, ref):
        pltpu.make_async_copy(ref, ref, sem).wait()

    local(gat_w, gatw_v, 0)
    local(gat_n, gatn_v, 1)
    for src, dst in ((k_w, kw_v), (v_w, vw_v)):
        local(src, dst, 2)
    for src, dst in ((k_n, kn_v), (v_n, vn_v)):
        local(src, dst, 3)

    def slab_parts(c):
        odd = c % 2
        return c * chunk + odd * half, c * chunk + (1 - odd) * whole

    def d_slab(r, lo=0, size=chunk):
        return d_all.at[
            r // 2, pl.ds(lo, size), pl.ds(pl.multiple_of(lax.rem(r, 2) * cols, cols), cols)
        ]

    first, second = slab_parts(a)
    own_down = (
        pltpu.make_async_copy(
            down.at[pl.ds(pl.multiple_of(first, half), whole)],
            d_slab(me, 0, whole),
            in_sem.at[4],
        ),
        pltpu.make_async_copy(
            down.at[pl.ds(pl.multiple_of(second, half), half)],
            d_slab(me, whole, half),
            in_sem.at[5],
        ),
    )
    for c in own_down:
        c.start()
    for c in range(na):
        lo, hi = slab_parts(c)
        pltpu.make_async_copy(
            down.at[lo : lo + whole], d_own.at[c, 0:whole], in_sem.at[6]
        ).start()
        pltpu.make_async_copy(
            down.at[hi : hi + half], d_own.at[c, whole:chunk], in_sem.at[6]
        ).start()
    for i, w in enumerate((gate, up)):
        for c in range(na):
            lo, _ = slab_parts(c)
            pltpu.make_async_copy(
                w.at[:, lo : lo + whole],
                gu_own.at[c, :, i * whole : (i + 1) * whole],
                in_sem.at[7],
            ).start()
        for c in range(na // 2):
            lo = 2 * c * chunk + whole
            pltpu.make_async_copy(
                w.at[:, lo : lo + 128], edge_v.at[i, c], in_sem.at[8]
            ).start()
    local(q_w, qw_v, 9)
    local(q_n, qn_v, 10)
    local(og_w, ogw_v, 11)
    local(og_n, ogn_v, 12)
    local(gain_w, gainw_v, 13)
    local(gain_n, gainn_v, 14)
    local(read_w, read_v.at[: read_w.shape[0]], 15)
    local(read_n, read_v.at[read_w.shape[0] :], 15)
    local(residual, res_v, 16)
    local(norm_gain, ngain_v, 17)

    def remote(src, dst, s_sem, r_sem, peer):
        return pltpu.make_async_remote_copy(
            src_ref=src,
            dst_ref=dst,
            send_sem=s_sem,
            recv_sem=r_sem,
            device_id=peer,
            device_id_type=MESH,
        )

    def go(copy):
        copy.start()

    def slab(kind, r, lo, size):
        if kind == 0:
            return gu_all.at[r, pl.ds(lo, size)]
        return d_slab(r, lo, size)

    extent = (depth, chunk)

    def z_copy(kind, k, r):
        src = (gu_own, d_own)[kind].at[a ^ k]
        return remote(
            src, slab(kind, r, 0, extent[kind]), s_sem.at[2 * kind], z_r.at[kind, k], (a ^ k, b, t)
        )

    def z_start(kind, k):
        go(z_copy(kind, k, me))

    def z_wait(kind, k):
        z_copy(kind, k, (a ^ k) * nb + b).wait_recv()

    def full_copy(kind, s, d, h, who):
        size = extent[kind] // 2
        ref = slab(kind, (a ^ s) * nb + who, h * size, size)
        i = h if d == h else 2 + kind * d
        return remote(ref, ref, s_sem.at[kind], f_r.at[kind, s, i], (a, b ^ (1 << d), t))

    def full_start(kind, s):
        for d, h in ((0, 0), (1, 1), (0, 1), (1, 0)):
            go(full_copy(kind, s, d, h, b))

    def full_wait(kind, s, d, h):
        full_copy(kind, s, d, h, b ^ (1 << d)).wait_recv()

    def diag_copy(kind, s, h, who):
        size = extent[kind] // 2
        ref = slab(kind, (a ^ s) * nb + who, h * size, size)
        return remote(ref, ref, s_sem.at[kind], f_r.at[kind, s, 2 + kind], (a, b ^ (2 >> h), t))

    def relay(kind, s):
        for h in range(2):
            full_wait(kind, s, h, h)
            go(diag_copy(kind, s, h, b ^ (1 << h)))

    def arrived(s):
        landed(f_r.at[0, s, 2], gu_all.at[:2])

    landed(in_sem.at[0], gatw_v)
    landed(in_sem.at[1], gatn_v)
    gat_v[:, :wide_heads, :] = gatw_v[...]
    gat_v[:, wide_heads:, :] = gatn_v[...]
    it = lax.broadcasted_iota(jnp.int32, (rows, rows), 0)
    js = lax.broadcasted_iota(jnp.int32, (rows, rows), 1)
    upper = (it <= js).astype(f32)
    eye = (it == js).astype(f32)
    last_dims = (((1,), (1,)), ((), ()))
    first_dims = (((0,), (0,)), ((), ()))
    exact = dict(precision=lax.Precision.HIGHEST, preferred_element_type=f32)
    gate_in = gat_v[0]
    x = gat_v[1]
    forget = jnp.minimum(x, 0.0) - jnp.log1p(jnp.exp(-jnp.abs(x))) + gat_v[2]
    cum = jnp.dot(forget, upper, **exact)
    cum_t = lax.dot_general(eye, cum, last_dims, **exact)
    diff = gate_in - cum
    diff_t = lax.dot_general(eye, diff, last_dims, **exact)
    total = cum[:, rows - 1 : rows]
    level = jnp.max(total + diff, axis=1, keepdims=True)
    total_t = cum_t[rows - 1 : rows, :]
    level_t = jnp.max(total_t + diff_t, axis=0, keepdims=True)
    tail_t = jnp.exp(total_t + diff_t - level_t)
    lane = lax.broadcasted_iota(jnp.int32, (heads, 128), 1)
    mark[...] = jnp.where(
        lane < 64, jnp.broadcast_to(level, (heads, 128)), jnp.broadcast_to(total, (heads, 128))
    )

    groups = (
        (qw_v, kw_v, vw_v, ogw_v, gainw_v, raw_w, DK_A, dv_w, wide_heads, 0),
        (qn_v, kn_v, vn_v, ogn_v, gainn_v, raw_n, DK_B, dv_n, narrow_heads, wide_heads),
    )
    fold = DK_B // 2
    deep = DK_A + fold

    for c in own_down:
        c.wait()
    pltpu.make_async_copy(d_own, d_own, in_sem.at[6]).wait()
    pl.semaphore_wait(barrier, len(peers))
    z_start(1, 1)
    is_inner = (a + 1) // 2 % 2
    inner = is_inner == 1
    order = (0, 1 + 2 * is_inner, 3 - 2 * is_inner, 2)
    odd = a % 2
    group = (0, 1, 2 + is_inner, 3 - is_inner)
    late = group[2:]


    joint = kw_v.shape[1] + vw_v.shape[1]
    landed(in_sem.at[2], read_v.at[: rows * joint // model])
    joint = kn_v.shape[1] + vn_v.shape[1]
    landed(in_sem.at[3], read_v.at[: rows * joint // model])
    for _, k, v, _, _, _, dk, dv, count, base in groups:
        scale = dk ** (-0.5)
        for h in range(count):
            i = base + h
            scaled = k[:, h * dk : (h + 1) * dk].astype(f32) * (tail_t[:, i : i + 1] * scale)
            memory = lax.dot_general(
                scaled.astype(bf16),
                v[:, h * dv : (h + 1) * dv],
                first_dims,
                preferred_element_type=f32,
            ).astype(bf16)
            if base == 0:
                sent[h, :dk, :] = memory
            else:
                sent[h, DK_A:deep, :dv] = memory[:fold]
                sent[h, DK_A:deep, dv:] = memory[fold:]

    def p1(m, r):
        peer = (a, b ^ m, t)
        return (
            remote(mark, mark_got.at[r], s_sem.at[3], p1_r.at[0, m], peer),
            remote(sent.at[b ^ m], got.at[r], s_sem.at[4], p1_r.at[1, m], peer),
        )

    for m in range(1, nb):
        for c in p1(m, b):
            go(c)
    got[b] = sent[b]
    mark_got[b] = mark[...]

    pltpu.make_async_copy(
        gu_own.at[:, :, : 2 * whole], gu_own.at[:, :, : 2 * whole], in_sem.at[7]
    ).wait()
    pltpu.make_async_copy(edge_v, edge_v, in_sem.at[8]).wait()
    for c in range(na // 2):
        ge, ue = edge_v[0, c], edge_v[1, c]
        gu_own[2 * c, :, 2 * whole :] = jnp.concatenate([ge[:, :half], ue[:, :half]], axis=1)
        gu_own[2 * c + 1, :, 2 * whole :] = jnp.concatenate([ge[:, half:], ue[:, half:]], axis=1)
    gu_all[me] = gu_own[a]

    @pl.when(inner)
    def _():
        z_copy(0, 3, me).start()

    full_start(0, 0)
    full_start(1, 0)

    landed(in_sem.at[9], qw_v)
    landed(in_sem.at[10], qn_v)
    for q, k, v, _, _, raw, dk, dv, count, base in groups:
        scale = dk ** (-0.5)
        for h in range(count):
            i = base + h
            q_h = q[:, h * dk : (h + 1) * dk]
            k_h = k[:, h * dk : (h + 1) * dk]
            v_h = v[:, h * dv : (h + 1) * dv]
            scores = lax.dot_general(q_h, k_h, last_dims, preferred_element_type=f32)
            logits = cum_t[:, i : i + 1] + diff[i : i + 1, :]
            logits = jnp.where(js <= it, logits, LOW)
            stab = jnp.max(logits, axis=1, keepdims=True)
            weighted = scores * scale * jnp.exp(logits - stab)
            raw[:, h * dv : (h + 1) * dv] = jnp.dot(
                weighted.astype(bf16), v_h, preferred_element_type=f32
            )
            stabs[:, i : i + 1] = stab

    for m in range(1, nb):
        for c in p1(m, b ^ m):
            c.wait_recv()
    spans = ((0, DK_A), (DK_A, deep))

    def read_mark(ref, where, row):
        line = ref[where, pl.ds(row, 1), :]
        return line[:, :1], line[:, 127:128]

    run = []
    for g, (lo, hi) in enumerate(spans):
        lev, tot = read_mark(mark_got, 0, b + g * wide_heads)
        state = got[0, lo:hi, :].astype(f32)
        run.append([(lev, tot)])
        for j in range(1, nb):
            prefix[j - 1, lo:hi, :] = state
            lev2, tot2 = read_mark(mark_got, j, b + g * wide_heads)
            new = jnp.maximum(lev + tot2, lev2)
            state = (
                jnp.exp(lev + tot2 - new) * state
                + jnp.exp(lev2 - new) * got[j, lo:hi, :].astype(f32)
            )
            lev, tot = new, tot + tot2
            run[g].append((lev, tot))
        total_s[lo:hi, :] = state.astype(bf16)
    lane1 = lax.broadcasted_iota(jnp.int32, (1, 128), 1)
    for g in range(2):
        lev, tot = run[g][nb - 1]
        tmark[g : g + 1, :] = jnp.where(
            lane1 < 64, jnp.broadcast_to(lev, (1, 128)), jnp.broadcast_to(tot, (1, 128))
        )

    def p2(k, r):
        peer = (a ^ k, b, t)
        return (
            remote(tmark, tmark_got.at[r], p2_s.at[0, k], p2_r.at[0, k], peer),
            remote(total_s, total_got.at[r], p2_s.at[1, k], p2_r.at[1, k], peer),
        )

    for k in range(1, na):

        @pl.when((a ^ k) > a)
        def _():
            for c in p2(k, a):
                c.start()

    @pl.when(inner)
    def _():
        z_copy(0, 2, me).start()
        z_copy(0, 1, me).start()

    @pl.when(jnp.logical_not(inner))
    def _():
        for k in range(1, na):
            z_copy(0, k, me).start()


    enter[...] = jnp.zeros(enter.shape, f32)
    enter_mark[...] = jnp.full(enter_mark.shape, LOW, f32)
    for k in range(1, na):

        @pl.when((a ^ k) < a)
        def _():
            for c in p2(k, a ^ k):
                c.wait_recv()

    for z in range(na - 1):

        @pl.when(z < a)
        def _():
            for g, (lo, hi) in enumerate(spans):
                lev = enter_mark[g : g + 1, :1]
                lev2, tot2 = read_mark(tmark_got, z, g)
                new = jnp.maximum(lev + tot2, lev2)
                enter[lo:hi, :] = (
                    jnp.exp(lev + tot2 - new) * enter[lo:hi, :]
                    + jnp.exp(lev2 - new) * total_got[z, lo:hi, :].astype(f32)
                )
                enter_mark[g : g + 1, :] = jnp.broadcast_to(new, (1, 128))

    for g, (lo, hi) in enumerate(spans):
        lev = enter_mark[g : g + 1, :1]
        back[0, lo:hi, :] = enter[lo:hi, :].astype(bf16)
        bmark[0, g : g + 1, :] = jnp.broadcast_to(lev, (1, 128))
        for j in range(1, nb):
            lev2, tot2 = run[g][j - 1]
            new = jnp.maximum(lev + tot2, lev2)
            back[j, lo:hi, :] = (
                jnp.exp(lev + tot2 - new) * enter[lo:hi, :]
                + jnp.exp(lev2 - new) * prefix[j - 1, lo:hi, :]
            ).astype(bf16)
            bmark[j, g : g + 1, :] = jnp.broadcast_to(new, (1, 128))

    def p3(m, r):
        peer = (a, b ^ m, t)
        return (
            remote(bmark.at[b ^ m], bmark_got.at[r], s_sem.at[5], p3_r.at[0, m], peer),
            remote(back.at[b ^ m], carried.at[r], s_sem.at[6], p3_r.at[1, m], peer),
        )

    for m in range(1, nb):
        for c in p3(m, b):
            go(c)
    carried[b] = back[b]
    bmark_got[b] = bmark[b]
    relay(0, 0)
    relay(1, 0)

    for i, ref in enumerate((ogw_v, ogn_v, gainw_v, gainn_v)):
        landed(in_sem.at[11 + i], ref)
    for m in range(1, nb):
        for c in p3(m, b ^ m):
            c.wait_recv()

    for g, (q, _, _, og, gain, raw, dk, dv, count, base) in enumerate(groups):
        for h in range(count):
            i = base + h
            if g == 0:
                memory = carried[h, :dk, :]
            else:
                memory = jnp.concatenate(
                    [carried[h, DK_A:deep, :dv], carried[h, DK_A:deep, dv:]], axis=0
                )
            own = stabs[:, i : i + 1]
            shifted = cum_t[:, i : i + 1] + bmark_got[h, g : g + 1, :1]
            both = jnp.maximum(own, shifted)
            span_h = slice(h * dv, (h + 1) * dv)
            incoming = jnp.dot(
                q[:, h * dk : (h + 1) * dk], memory, preferred_element_type=f32
            )
            value = raw[:, span_h] * jnp.exp(own - both) + incoming * jnp.exp(shifted - both)
            value = value * lax.rsqrt(jnp.mean(value * value, axis=1, keepdims=True) + 1e-06)
            gate_h = 1.0 / (1.0 + jnp.exp(-og[:, span_h].astype(f32)))
            value = value * gain[span_h].astype(f32).reshape(1, dv) * gate_h
            lo = g * raw_w.shape[1] + h * dv
            gated[:, lo : lo + dv] = value.astype(bf16)

    z_wait(0, order[1])
    full_start(0, order[1])

    for i, ref in enumerate((read_v, res_v, ngain_v)):
        landed(in_sem.at[15 + i], ref)
    tile = model // 4
    for j in range(model // tile):
        sl = slice(j * tile, (j + 1) * tile)
        p = jnp.dot(gated[...], read_v[:, sl], preferred_element_type=f32).astype(bf16)
        part[:, :, sl] = p.reshape(2, own_rows, tile)
    partner = (a, b, 1 - t)
    swap = remote(part.at[1 - t], part_got, s_sem.at[7], t_r.at[0], partner)
    go(swap)
    swap.wait_recv()
    mixed = part[t].astype(f32) + part_got[...].astype(f32)
    mid = (res_v[...].astype(f32) + mixed).astype(bf16)
    middle[...] = mid
    mid = mid.astype(f32)
    normed = mid * lax.rsqrt(jnp.mean(mid * mid, axis=-1, keepdims=True) + 1e-06)
    block = 2 * own_rows

    piece = own_rows // 2

    def row_block(z, core, c, size=piece):
        lo = (z * 2 + core) * own_rows + c * piece
        return x_all.at[pl.ds(pl.multiple_of(lo, piece), size)]

    x_all[pl.ds(pl.multiple_of((a * 2 + t) * own_rows, own_rows), own_rows), :] = (
        normed * ngain_v[...].astype(f32).reshape(1, model)
    ).astype(bf16)

    def x_copy(i, k, z, c):
        ref = row_block(z, t, c)
        return remote(ref, ref, s_sem.at[9], x_r.at[i, c], (a ^ k, b, t))

    def y_copy(z, core, c):
        ref = row_block(z, core, c)
        return remote(ref, ref, s_sem.at[10], y_r.at[0], partner)

    for c in range(2):
        go(x_copy(0, 2, a, c))
    for c in range(2):
        go(x_copy(1, 1, a, c))
    for c in range(2):
        go(y_copy(a, t, c))

    @pl.when(inner)
    def _():
        z_copy(1, 3, me).start()
        z_copy(1, 2, me).start()

    width = gu_all.shape[2]
    tiles = [(lo, min(lo + 512, width)) for lo in range(0, width, 512)]

    def unit(lo, m, s, fresh):
        z = a ^ s
        xs = x_all[pl.ds(lo, m), pl.ds(pl.multiple_of(z * kspan, kspan), kspan)]
        for c0, c1 in tiles:
            w = gu_all[pl.ds(z * nb, nb), :, c0:c1].reshape(kspan, c1 - c0)
            p = jnp.dot(xs, w, preferred_element_type=f32)
            if fresh:
                acc[pl.ds(lo, m), c0:c1] = p
            else:
                acc[pl.ds(lo, m), c0:c1] += p

    def passed_on(i, k):
        z = a ^ k
        for c in range(2):
            x_copy(i, 1 if i else 2, z, c).wait_recv()
            if i == 0:
                go(x_copy(2, 1, z, c))
            go(y_copy(z, t, c))

    z_wait(0, order[2])
    full_start(0, order[2])
    relay(0, order[1])
    z_wait(0, order[3])
    full_start(0, order[3])
    relay(0, order[2])
    passed_on(0, 2)

    @pl.when(jnp.logical_not(inner))
    def _():
        z_copy(1, 2, me).start()
        z_copy(1, 3, me).start()


    passed_on(1, 1)
    relay(0, order[3])
    z_wait(1, 1)
    full_start(1, 1)
    passed_on(2, 3)
    total_rows = na * block
    landed(y_r.at[0], x_all.at[: total_rows // 2])
    for s in range(na):
        if s == 3:
            z_wait(1, late[0])
            full_start(1, late[0])
        arrived(order[s])
        unit(0, total_rows, order[s], s == 0)

    for j in range(2):
        sl = slice(j * total_rows // 2, (j + 1) * total_rows // 2)
        gt = acc[sl, :whole]
        hidden[sl, :whole] = (
            gt * (1.0 / (1.0 + jnp.exp(-gt))) * acc[sl, whole : 2 * whole]
        ).astype(bf16)
        mx = acc[sl, 2 * whole :]
        hx = mx * (1.0 / (1.0 + jnp.exp(-mx))) * pltpu.roll(mx, half, 1)
        hidden[sl, whole:] = hx[:, :half].astype(bf16)
    relay(1, 1)
    z_wait(1, late[1])
    full_start(1, late[1])

    side = b // 2
    high = a // 2
    unit_cols = 2 * cols

    def t_copy(u):
        return remote(
            terms.at[u, :, 1 - t], terms_got.at[u], s_sem.at[8], t_r.at[1 + u], partner
        )

    def other(u):
        g = (3 - is_inner, 2 + is_inner, is_inner, 1 - is_inner)[u // 2]
        return 2 * g + u % 2

    def place(u):
        return (a ^ group[u // 2]) * 2 + (side + u) % 2

    def down_unit(u):
        g = group[u // 2]
        if u % 2 == 0:
            full_wait(1, g, 0, 1)
        else:
            landed(f_r.at[1, g, 3], d_all.at[0, : 3 * chunk // 4])
        v = jnp.dot(hidden[...], d_all[place(u)], preferred_element_type=f32)
        terms[u] = v.astype(bf16).reshape(terms.shape[1:])
        go(t_copy(u))

    def a_copy(u, w):
        return remote(sums.at[u, :, 1 - odd], a_got.at[w], s_sem.at[11], a_r.at[w], (a ^ 1, b, t))

    def b_copy(u, w):
        return remote(joined.at[u], b_got.at[w], s_sem.at[12], b_r.at[w], (a ^ 2, b, t))

    def sum_unit(u):
        t_copy(u).wait_recv()
        sums[u] = (
            (terms[u, :, t].astype(f32) + terms_got[u].astype(f32))
            .astype(bf16)
            .reshape(sums.shape[1:])
        )
        go(a_copy(u, u ^ 2 if u < 4 else u))

    def join_unit(u):
        a_copy(u, u).wait_recv()
        joined[u] = (
            sums[u, 1 - high, odd].astype(f32) + a_got[u, 1 - high].astype(f32)
        ).astype(bf16)
        go(b_copy(u, other(u)))

    def finish_unit(u):
        b_copy(u, u).wait_recv()
        v = sums[u, high, odd].astype(f32) + a_got[u, high].astype(f32)
        v = v + b_got[u].astype(f32)
        c0 = pl.ds(pl.multiple_of(place(u) * unit_cols, unit_cols), unit_cols)
        out[:, c0] = (middle[:, c0].astype(f32) + v).astype(bf16)

    down_unit(0)
    down_unit(1)
    down_unit(2)
    sum_unit(0)
    sum_unit(1)
    relay(1, late[0])
    sum_unit(2)
    down_unit(4)
    down_unit(3)
    sum_unit(4)
    relay(1, late[1])
    join_unit(2)
    join_unit(0)
    sum_unit(3)
    down_unit(6)
    join_unit(3)
    join_unit(4)
    sum_unit(6)
    down_unit(5)
    join_unit(1)
    sum_unit(5)
    join_unit(6)
    down_unit(7)
    sum_unit(7)
    join_unit(5)
    join_unit(7)

    for u in (4, 5, 2, 3, 6, 7, 0, 1):
        finish_unit(u)

    sends = (
        gu_all.at[: n - 1],
        d_all.at[: 3 * n // 8],
        d_own.at[: na - 1],
        mark_got.at[: nb - 1],
        got.at[: nb - 1],
        bmark_got.at[: nb - 1],
        carried.at[: nb - 1],
        part_got,
        terms_got,
        x_all.at[: 3 * own_rows],
        x_all.at[: total_rows // 2],
        a_got,
        b_got,
    )
    for i, ref in enumerate(sends):
        landed(s_sem.at[i], ref)
    for k in range(1, na):

        @pl.when((a ^ k) > a)
        def _():
            for c in p2(k, a):
                c.wait_send()


def layer(na, nb, *args):
    (res, q_w, k_w, v_w, og_w, gat_w, gain_w, read_w) = args[:8]
    (q_n, k_n, v_n, og_n, gat_n, gain_n, read_n, norm_gain, gate, up, down) = args[8:]
    bf16, f32 = jnp.bfloat16, jnp.float32
    n = na * nb
    depth = gate.shape[0]
    chunk = gate.shape[1] // na
    whole = chunk // 128 * 128
    width = 2 * whole + 128
    cols = down.shape[1]
    own_rows, model = res.shape
    rows = q_w.shape[0]
    heads = gat_w.shape[1] + gat_n.shape[1]
    deep = DK_A + DK_B // 2
    dv = v_w.shape[1] // gat_w.shape[1]
    total_rows = na * 2 * own_rows
    units = n // 2

    def vm(shape, dtype=bf16):
        return pltpu.VMEM(shape, dtype)

    def like(x):
        return pltpu.VMEM(x.shape, x.dtype)

    dma = pltpu.SemaphoreType.DMA
    scratch = [
        like(res),
        like(q_w),
        like(k_w),
        like(v_w),
        like(og_w),
        like(gat_w),
        like(gain_w),
        like(q_n),
        like(k_n),
        like(v_n),
        like(og_n),
        like(gat_n),
        like(gain_n),
        vm((read_w.shape[0] + read_n.shape[0], model)),
        like(norm_gain),
        vm((2, na // 2, depth, 128)),
        vm((na, depth, width)),
        vm((na, chunk, cols)),
        vm((n, depth, width)),
        vm((n // 2, chunk, 2 * cols)),
        vm((3, heads, rows), f32),
        vm(v_w.shape, f32),
        vm(v_n.shape, f32),
        vm((rows, 128), f32),
        vm((nb, deep, dv)),
        vm((nb, deep, dv)),
        vm((heads, 128), f32),
        vm((nb, heads, 128), f32),
        vm((nb - 1, deep, dv), f32),
        vm((deep, dv)),
        vm((na, deep, dv)),
        vm((8, 128), f32),
        vm((na, 8, 128), f32),
        vm((deep, dv), f32),
        vm((8, 128), f32),
        vm((nb, deep, dv)),
        vm((nb, deep, dv)),
        vm((nb, 8, 128), f32),
        vm((nb, 8, 128), f32),
        vm((rows, v_w.shape[1] + v_n.shape[1])),
        vm((2, own_rows, model)),
        vm((own_rows, model)),
        vm((own_rows, model)),
        vm((total_rows, model)),
        vm((total_rows, width), f32),
        vm((total_rows, chunk)),
        vm((units, na, 2, own_rows, 2 * cols)),
        vm((units, na, own_rows, 2 * cols)),
        vm((units, na // 2, 2, own_rows, 2 * cols)),
        vm((units, na // 2, own_rows, 2 * cols)),
        vm((units, own_rows, 2 * cols)),
        vm((units, own_rows, 2 * cols)),
        vm(res.shape),
        dma((18,)),
        dma((13,)),
        dma((2, nb)),
        dma((2, na)),
        dma((2, na)),
        dma((2, nb)),
        dma((2, na)),
        dma((2, na, 4)),
        dma((1 + units,)),
        dma((3, 2)),
        dma((1,)),
        dma((units,)),
        dma((units,)),
    ]
    hbm = pl.BlockSpec(memory_space=pl.ANY)
    return pl.pallas_call(
        functools.partial(layer_kernel, na, nb),
        out_shape=pltpu.VMEM(res.shape, bf16),
        in_specs=[hbm] * 19,
        out_specs=pl.BlockSpec(memory_space=pltpu.VMEM),
        scratch_shapes=scratch,
        compiler_params=pltpu.CompilerParams(
            collective_id=0, has_side_effects=True, vmem_limit_bytes=60 * 2**20
        ),
    )(
        res,
        q_w,
        k_w,
        v_w,
        og_w,
        gat_w,
        gain_w,
        read_w,
        q_n,
        k_n,
        v_n,
        og_n,
        gat_n,
        gain_n,
        read_n,
        norm_gain,
        gate,
        up,
        down,
    )


def fits(mesh_shape, args):
    na, nb, ntp = mesh_shape
    gate, gat_w, gat_n = args[16], args[5], args[12]
    q_w, v_w, v_n = args[1], args[3], args[10]
    heads_w, heads_n = gat_w.shape[1], gat_n.shape[1]
    return (
        na == nb == 4
        and ntp == 2
        and gate.shape[1] % na == 0
        and gate.shape[1] // na % 128 == 64
        and heads_w == heads_n == nb
        and q_w.shape[0] == 128
        and v_w.shape[1] // heads_w == 2 * (v_n.shape[1] // heads_n)
    )


def passed(block, axis, step):
    size = lax.axis_size(axis)
    if step % size == 0:
        return block
    return lax.ppermute(block, axis, [(i, (i + step) % size) for i in range(size)])


def gathered(block, axis):
    return jnp.concatenate([passed(block, axis, r) for r in range(lax.axis_size(axis))], axis=0)


def returned(blocks, axis):
    size = lax.axis_size(axis)
    rows = blocks.shape[0] // size
    pieces = [passed(blocks[r * rows : (r + 1) * rows], axis, -r) for r in range(size)]
    return sum(p.astype(jnp.float32) for p in pieces)


def plain_body(
    residual,
    query_wide,
    key_wide,
    value_wide,
    outgate_wide,
    gating_wide,
    gain_wide,
    readout_wide,
    query_narrow,
    key_narrow,
    value_narrow,
    outgate_narrow,
    gating_narrow,
    gain_narrow,
    readout_narrow,
    norm_gain,
    gate_weight,
    up_weight,
    down_weight,
):
    na, nb = lax.axis_size("a"), lax.axis_size("b")
    depth, hidden_tp = gate_weight.shape
    chunk = hidden_tp // na
    out_cols = down_weight.shape[1]
    model = residual.shape[1]

    def spread(pieces):
        return lax.all_to_all(pieces, "a", split_axis=0, concat_axis=0, tiled=True)

    mine = (
        spread(jnp.moveaxis(gate_weight.reshape(depth, na, chunk), 1, 0)),
        spread(jnp.moveaxis(up_weight.reshape(depth, na, chunk), 1, 0)),
        spread(down_weight.reshape(na, chunk, out_cols)),
    )
    gate_all, up_all, down_all = (
        lax.all_gather(m, "b", axis=0, tiled=True) for m in mine
    )
    *_, gating_wide, gating_narrow = lax.optimization_barrier(
        (*mine, gating_wide, gating_narrow)
    )

    gated_w, gated_n = cell(
        query_wide,
        key_wide,
        value_wide,
        outgate_wide,
        gating_wide,
        gain_wide,
        query_narrow,
        key_narrow,
        value_narrow,
        outgate_narrow,
        gating_narrow,
        gain_narrow,
    )
    partial = (
        jnp.dot(gated_w, readout_wide, preferred_element_type=jnp.float32)
        + jnp.dot(gated_n, readout_narrow, preferred_element_type=jnp.float32)
    ).astype(jnp.bfloat16)
    own_rows = residual.shape[0]
    ntp, core = lax.axis_size("tp"), lax.axis_index("tp")
    mixed = 0.0
    for r in range(ntp):
        block = lax.dynamic_slice_in_dim(partial, lax.rem(core + r, ntp) * own_rows, own_rows)
        mixed = mixed + passed(block, "tp", r).astype(jnp.float32)
    middle_f = (residual.astype(jnp.float32) + mixed).astype(jnp.bfloat16).astype(jnp.float32)
    normed = middle_f * lax.rsqrt(jnp.mean(middle_f * middle_f, axis=-1, keepdims=True) + 1e-06)
    normed = (normed * norm_gain.astype(jnp.float32)).astype(jnp.bfloat16)
    own_rows = normed.shape[0]
    normed = normed.reshape(own_rows, na, nb, depth).swapaxes(1, 2).reshape(own_rows, model)
    all_rows = gathered(gathered(normed, "a"), "tp")
    gate = jnp.dot(all_rows, gate_all.reshape(model, chunk), preferred_element_type=jnp.float32)
    upper = jnp.dot(all_rows, up_all.reshape(model, chunk), preferred_element_type=jnp.float32)
    hidden = (jax.nn.silu(gate) * upper).astype(jnp.bfloat16)
    down = jnp.transpose(down_all, (1, 0, 2)).reshape(chunk, model)
    terms = jnp.dot(hidden, down, preferred_element_type=jnp.float32)
    back = returned(returned(terms.astype(jnp.bfloat16), "tp").astype(jnp.bfloat16), "a")
    back = back.reshape(own_rows, nb, na, out_cols).swapaxes(1, 2).reshape(own_rows, model)
    return (middle_f + back).astype(jnp.bfloat16)


def body(*args):
    sizes = tuple(lax.axis_size(x) for x in ("a", "b", "tp"))
    if fits(sizes, args):
        return layer(sizes[0], sizes[1], *args)
    return plain_body(*args)


def solution(mesh):
    sp, tp = mesh.shape["sp"], mesh.shape["tp"]
    a = 4 if sp % 4 == 0 else 1
    split = Mesh(mesh.devices.reshape(a, sp // a, tp), ("a", "b", "tp"))
    s = ("a", "b")
    in_specs = (
        P(("a", "b", "tp"), None),
        P(s, "tp"),
        P(s, "tp"),
        P(s, "tp"),
        P(s, "tp"),
        P(None, "tp", s),
        P("tp"),
        P("tp", None),
        P(s, "tp"),
        P(s, "tp"),
        P(s, "tp"),
        P(s, "tp"),
        P(None, "tp", s),
        P("tp"),
        P("tp", None),
        P(),
        P(s, "tp"),
        P(s, "tp"),
        P("tp", s),
    )
    out_specs = P(("a", "b", "tp"), None)
    return jax.shard_map(body, mesh=split, in_specs=in_specs, out_specs=out_specs, check_vma=False)
```

```python
import functools

import jax
import jax.numpy as jnp
from jax import lax
from jax.experimental import pallas as pl
from jax.experimental.pallas import tpu as pltpu
from jax.sharding import Mesh, PartitionSpec as P

DK_A = 128
DK_B = 64
LOW = -1e30
MESH = pl.DeviceIdType.MESH


def cell_kernel(
    n,
    q_w,
    k_w,
    v_w,
    og_w,
    gain_w,
    q_n,
    k_n,
    v_n,
    og_n,
    gain_n,
    gating,
    out_w,
    out_n,
    raw_w,
    raw_n,
    stabs,
    sent,
    got,
    back,
    carried,
    mem_w,
    mem_n,
    state,
    levels,
    send_sem,
    recv_sem,
    send_sem2,
    recv_sem2,
):
    na, nb = lax.axis_size("a"), lax.axis_size("b")
    tp = lax.axis_index("tp")
    me = lax.axis_index("a") * nb + lax.axis_index("b")

    def where_is(index):
        return (index // nb, lax.rem(index, nb), tp)

    barrier = pltpu.get_barrier_semaphore()

    def greet(r, _):
        peer = lax.rem(me + r, n)
        pl.semaphore_signal(barrier, inc=1, device_id=where_is(peer), device_id_type=MESH)
        return 0

    lax.fori_loop(1, n, greet, 0)

    rows = q_w.shape[0]
    heads_p = gating.shape[1]
    groups = (
        (q_w, k_w, v_w, og_w, gain_w, out_w, raw_w, mem_w, DK_A),
        (q_n, k_n, v_n, og_n, gain_n, out_n, raw_n, mem_n, DK_B),
    )
    heads = tuple(g[0].shape[1] // g[8] for g in groups)
    parts = tuple(h * g[8] // n for h, g in zip(heads, groups))
    starts = (0, parts[0])
    extra = parts[0] + parts[1]

    it = lax.broadcasted_iota(jnp.int32, (rows, rows), 0)
    js = lax.broadcasted_iota(jnp.int32, (rows, rows), 1)
    upper = (it <= js).astype(jnp.float32)
    eye = (it == js).astype(jnp.float32)
    last_dims = (((1,), (1,)), ((), ()))
    first_dims = (((0,), (0,)), ((), ()))
    gate_in = gating[0]
    x = gating[1]
    forget = jnp.minimum(x, 0.0) - jnp.log1p(jnp.exp(-jnp.abs(x))) + gating[2]
    cum = jnp.dot(
        forget, upper, precision=lax.Precision.HIGHEST, preferred_element_type=jnp.float32
    )
    cum_t = lax.dot_general(
        eye, cum, last_dims, precision=lax.Precision.HIGHEST, preferred_element_type=jnp.float32
    )
    diff = gate_in - cum
    diff_t = lax.dot_general(
        eye, diff, last_dims, precision=lax.Precision.HIGHEST, preferred_element_type=jnp.float32
    )
    total = cum[:, rows - 1 : rows]
    level = jnp.max(total + diff, axis=1, keepdims=True)
    total_t = cum_t[rows - 1 : rows, :]
    level_t = jnp.max(total_t + diff_t, axis=0, keepdims=True)
    tail_t = jnp.exp(total_t + diff_t - level_t)
    width = sent.shape[2]
    lane = lax.broadcasted_iota(jnp.int32, (heads_p, width), 1)
    marks = jnp.where(
        lane < width // 2,
        jnp.broadcast_to(level, (heads_p, width)),
        jnp.broadcast_to(total, (heads_p, width)),
    )

    index = 0
    for g, (q, k, v, _, _, _, raw, _, dk) in enumerate(groups):
        dv = v.shape[1] // heads[g]
        scale = dk ** (-0.5)
        for h in range(heads[g]):
            k_h = k[:, h * dk : (h + 1) * dk]
            v_h = v[:, h * dv : (h + 1) * dv]
            scaled = k_h.astype(jnp.float32) * (tail_t[:, index : index + 1] * scale)
            memory = lax.dot_general(
                scaled.astype(jnp.bfloat16), v_h, first_dims, preferred_element_type=jnp.float32
            )
            size = parts[g]
            per = dk // size
            for p in range(per):
                sent[h * per + p, starts[g] : starts[g] + size, :dv] = memory[
                    p * size : (p + 1) * size
                ]
            index += 1
    spare = v_n.shape[1] // heads[1]
    if spare < width:
        sent[:, starts[1] : extra, spare:] = jnp.zeros((n, parts[1], width - spare), jnp.float32)
    for p in range(n):
        sent[p, extra : extra + heads_p, :] = marks

    pl.semaphore_wait(barrier, n - 1)

    def out_copy(r):
        peer = lax.rem(me + r, n)
        return pltpu.make_async_remote_copy(
            src_ref=sent.at[peer],
            dst_ref=got.at[me],
            send_sem=send_sem.at[r],
            recv_sem=recv_sem.at[r],
            device_id=where_is(peer),
            device_id_type=MESH,
        )

    lax.fori_loop(1, n, lambda r, c: (out_copy(r).start(), c)[1], 0)
    got[me] = sent[me]

    index = 0
    for g, (q, k, v, _, _, _, raw, _, dk) in enumerate(groups):
        dv = v.shape[1] // heads[g]
        scale = dk ** (-0.5)
        for h in range(heads[g]):
            q_h = q[:, h * dk : (h + 1) * dk]
            k_h = k[:, h * dk : (h + 1) * dk]
            v_h = v[:, h * dv : (h + 1) * dv]
            scores = lax.dot_general(q_h, k_h, last_dims, preferred_element_type=jnp.float32)
            logits = cum_t[:, index : index + 1] + diff[index : index + 1, :]
            logits = jnp.where(js <= it, logits, LOW)
            stab = jnp.max(logits, axis=1, keepdims=True)
            weighted = scores * scale * jnp.exp(logits - stab)
            raw[:, h * dv : (h + 1) * dv] = jnp.dot(
                weighted.astype(jnp.bfloat16), v_h, preferred_element_type=jnp.float32
            )
            stabs[:, index : index + 1] = stab
            index += 1

    lax.fori_loop(1, n, lambda r, c: (out_copy(r).wait(), c)[1], 0)

    which = tuple(
        (me * parts[g]) // groups[g][8] + (heads[0] if g else 0) for g in range(2)
    )
    sub = lax.broadcasted_iota(jnp.int32, (heads_p, width), 0)
    picks = tuple(sub == w for w in which)

    def merge(t, _):
        level_c = levels[0]
        back[t] = state[...]
        levels[1] = jnp.where(t == me, level_c, levels[1])
        mark = got[t, extra : extra + heads_p, :]
        lev = jnp.broadcast_to(mark[:, :1], mark.shape)
        tot = jnp.broadcast_to(mark[:, width - 1 :], mark.shape)
        new = jnp.maximum(level_c + tot, lev)
        old_f = jnp.exp(level_c + tot - new)
        new_f = jnp.exp(lev - new)
        levels[0] = new
        for g in range(2):
            span = slice(starts[g], starts[g] + parts[g])

            def pick(f):
                return jnp.sum(jnp.where(picks[g], f, 0.0), axis=0, keepdims=True)

            state[span, :] = pick(old_f) * state[span, :] + pick(new_f) * got[t, span, :]
        return 0

    levels[...] = jnp.full(levels.shape, LOW, jnp.float32)
    state[...] = jnp.zeros(state.shape, jnp.float32)
    lax.fori_loop(0, n, merge, 0)
    entering = levels[1]

    def back_copy(r):
        peer = lax.rem(me + r, n)
        return pltpu.make_async_remote_copy(
            src_ref=back.at[peer],
            dst_ref=carried.at[me],
            send_sem=send_sem2.at[r],
            recv_sem=recv_sem2.at[r],
            device_id=where_is(peer),
            device_id_type=MESH,
        )

    lax.fori_loop(1, n, lambda r, c: (back_copy(r).start(), c)[1], 0)
    carried[me] = back[me]
    entering_t = lax.dot_general(
        jnp.where(
            lax.broadcasted_iota(jnp.int32, (rows, width), 1) == 0, 1.0, 0.0
        ),
        entering,
        last_dims,
        precision=lax.Precision.HIGHEST,
        preferred_element_type=jnp.float32,
    )
    shifted = cum_t + entering_t
    own = stabs[:, :heads_p]
    both = jnp.maximum(own, shifted)
    own_f = jnp.exp(own - both)
    in_f = jnp.exp(shifted - both)
    lax.fori_loop(1, n, lambda r, c: (back_copy(r).wait(), c)[1], 0)

    index = 0
    for g, (q, _, v, og, gain, out, raw, mem, dk) in enumerate(groups):
        dv = v.shape[1] // heads[g]
        size = parts[g]
        per = dk // size
        for h in range(heads[g]):
            for p in range(per):
                mem[p * size : (p + 1) * size, :] = carried[
                    h * per + p, starts[g] : starts[g] + size, :dv
                ]
            memory = mem[...]
            high = memory.astype(jnp.bfloat16)
            rest = (memory - high.astype(jnp.float32)).astype(jnp.bfloat16)
            q_h = q[:, h * dk : (h + 1) * dk]
            cols = slice(h * dv, (h + 1) * dv)
            incoming = jnp.dot(q_h, high, preferred_element_type=jnp.float32) + jnp.dot(
                q_h, rest, preferred_element_type=jnp.float32
            )
            value = (
                raw[:, cols] * own_f[:, index : index + 1]
                + incoming * in_f[:, index : index + 1]
            )
            value = value * lax.rsqrt(jnp.mean(value * value, axis=1, keepdims=True) + 1e-06)
            gate = 1.0 / (1.0 + jnp.exp(-og[:, cols].astype(jnp.float32)))
            value = value * gain[:, cols].astype(jnp.float32) * gate
            out[:, cols] = value.astype(jnp.bfloat16)
            index += 1


def cell(q_w, k_w, v_w, og_w, gat_w, gain_w, q_n, k_n, v_n, og_n, gat_n, gain_n):
    n = lax.axis_size("a") * lax.axis_size("b")
    rows = q_w.shape[0]
    heads = gat_w.shape[1] + gat_n.shape[1]
    heads_p = -(-heads // 8) * 8
    gating = jnp.concatenate([gat_w, gat_n], axis=1)
    gating = jnp.pad(gating, ((0, 0), (0, heads_p - heads), (0, 0)))
    parts = (q_w.shape[1] // n, q_n.shape[1] // n)
    width = v_w.shape[1] // gat_w.shape[1]
    width_n = v_n.shape[1] // gat_n.shape[1]
    vmem = pl.BlockSpec(memory_space=pltpu.VMEM)
    state = parts[0] + parts[1]
    return pl.pallas_call(
        functools.partial(cell_kernel, n),
        out_shape=(
            jax.ShapeDtypeStruct(v_w.shape, jnp.bfloat16),
            jax.ShapeDtypeStruct(v_n.shape, jnp.bfloat16),
        ),
        in_specs=[vmem] * 11,
        out_specs=(vmem, vmem),
        scratch_shapes=[
            pltpu.VMEM(v_w.shape, jnp.float32),
            pltpu.VMEM(v_n.shape, jnp.float32),
            pltpu.VMEM((rows, 128), jnp.float32),
            pltpu.VMEM((n, state + heads_p, width), jnp.float32),
            pltpu.VMEM((n, state + heads_p, width), jnp.float32),
            pltpu.VMEM((n, state, width), jnp.float32),
            pltpu.VMEM((n, state, width), jnp.float32),
            pltpu.VMEM((DK_A, width), jnp.float32),
            pltpu.VMEM((DK_B, width_n), jnp.float32),
            pltpu.VMEM((state, width), jnp.float32),
            pltpu.VMEM((2, heads_p, width), jnp.float32),
            pltpu.SemaphoreType.DMA((n,)),
            pltpu.SemaphoreType.DMA((n,)),
            pltpu.SemaphoreType.DMA((n,)),
            pltpu.SemaphoreType.DMA((n,)),
        ],
        compiler_params=pltpu.CompilerParams(
            collective_id=0, has_side_effects=True, vmem_limit_bytes=32 * 2**20
        ),
        cost_estimate=pl.CostEstimate(
            flops=2 * 10**9, bytes_accessed=120 * 10**6, transcendentals=0
        ),
    )(
        q_w,
        k_w,
        v_w,
        og_w,
        gain_w.reshape(1, -1),
        q_n,
        k_n,
        v_n,
        og_n,
        gain_n.reshape(1, -1),
        gating,
    )


def layer_kernel(na, nb, *refs):
    (
        residual,
        q_w,
        k_w,
        v_w,
        og_w,
        gat_w,
        gain_w,
        read_w,
        q_n,
        k_n,
        v_n,
        og_n,
        gat_n,
        gain_n,
        read_n,
        norm_gain,
        gate,
        up,
        down,
        out,
        res_v,
        qw_v,
        kw_v,
        vw_v,
        ogw_v,
        gatw_v,
        gainw_v,
        qn_v,
        kn_v,
        vn_v,
        ogn_v,
        gatn_v,
        gainn_v,
        read_v,
        ngain_v,
        edge_v,
        gu_own,
        d_own,
        gu_all,
        d_all,
        gat_v,
        raw_w,
        raw_n,
        stabs,
        sent,
        got,
        mark,
        mark_got,
        prefix,
        total_s,
        total_got,
        tmark,
        tmark_got,
        enter,
        enter_mark,
        back,
        carried,
        bmark,
        bmark_got,
        gated,
        part,
        part_got,
        middle,
        x_all,
        acc,
        hidden,
        terms,
        terms_got,
        sums,
        a_got,
        joined,
        b_got,
        out_v,
        in_sem,
        s_sem,
        p1_r,
        p2_s,
        p2_r,
        p3_r,
        z_r,
        f_r,
        t_r,
        x_r,
        y_r,
        a_r,
        b_r,
    ) = refs
    n = na * nb
    a, b, t = lax.axis_index("a"), lax.axis_index("b"), lax.axis_index("tp")
    me = a * nb + b
    f32, bf16 = jnp.float32, jnp.bfloat16

    barrier = pltpu.get_barrier_semaphore()
    peers = [(a ^ k, b, t) for k in range(1, na)]
    peers += [(a, b ^ m, t) for m in range(1, nb)]
    peers += [(a, b, 1 - t)]
    for peer in peers:
        pl.semaphore_signal(barrier, inc=1, device_id=peer, device_id_type=MESH)

    depth = gate.shape[0]
    chunk = gate.shape[1] // na
    whole = chunk // 128 * 128
    half = chunk - whole
    cols = down.shape[1]
    model = residual.shape[1]
    own_rows = residual.shape[0]
    rows = q_w.shape[0]
    kspan = nb * depth
    wide_heads, narrow_heads = gat_w.shape[1], gat_n.shape[1]
    heads = wide_heads + narrow_heads
    dv_w = v_w.shape[1] // wide_heads
    dv_n = v_n.shape[1] // narrow_heads

    def local(src, dst, i):
        pltpu.make_async_copy(src, dst, in_sem.at[i]).start()

    def landed(sem, ref):
        pltpu.make_async_copy(ref, ref, sem).wait()

    local(gat_w, gatw_v, 0)
    local(gat_n, gatn_v, 1)
    for src, dst in ((k_w, kw_v), (v_w, vw_v)):
        local(src, dst, 2)
    for src, dst in ((k_n, kn_v), (v_n, vn_v)):
        local(src, dst, 3)

    def slab_parts(c):
        odd = c % 2
        return c * chunk + odd * half, c * chunk + (1 - odd) * whole

    def d_slab(r, lo=0, size=chunk):
        return d_all.at[
            r // 2, pl.ds(lo, size), pl.ds(pl.multiple_of(lax.rem(r, 2) * cols, cols), cols)
        ]

    first, second = slab_parts(a)
    own_down = (
        pltpu.make_async_copy(
            down.at[pl.ds(pl.multiple_of(first, half), whole)],
            d_slab(me, 0, whole),
            in_sem.at[4],
        ),
        pltpu.make_async_copy(
            down.at[pl.ds(pl.multiple_of(second, half), half)],
            d_slab(me, whole, half),
            in_sem.at[5],
        ),
    )
    for c in own_down:
        c.start()
    for c in range(na):
        lo, hi = slab_parts(c)
        pltpu.make_async_copy(
            down.at[lo : lo + whole], d_own.at[c, 0:whole], in_sem.at[6]
        ).start()
        pltpu.make_async_copy(
            down.at[hi : hi + half], d_own.at[c, whole:chunk], in_sem.at[6]
        ).start()
    for i, w in enumerate((gate, up)):
        for c in range(na):
            lo, _ = slab_parts(c)
            pltpu.make_async_copy(
                w.at[:, lo : lo + whole],
                gu_own.at[c, :, i * whole : (i + 1) * whole],
                in_sem.at[7],
            ).start()
        for c in range(na // 2):
            lo = 2 * c * chunk + whole
            pltpu.make_async_copy(
                w.at[:, lo : lo + 128], edge_v.at[i, c], in_sem.at[8]
            ).start()
    local(q_w, qw_v, 9)
    local(q_n, qn_v, 10)
    local(og_w, ogw_v, 11)
    local(og_n, ogn_v, 12)
    local(gain_w, gainw_v, 13)
    local(gain_n, gainn_v, 14)
    local(read_w, read_v.at[: read_w.shape[0]], 15)
    local(read_n, read_v.at[read_w.shape[0] :], 15)
    local(residual, res_v, 16)
    local(norm_gain, ngain_v, 17)

    def remote(src, dst, s_sem, r_sem, peer):
        return pltpu.make_async_remote_copy(
            src_ref=src,
            dst_ref=dst,
            send_sem=s_sem,
            recv_sem=r_sem,
            device_id=peer,
            device_id_type=MESH,
        )

    def go(copy):
        copy.start()

    def slab(kind, r, lo, size):
        if kind == 0:
            return gu_all.at[r, pl.ds(lo, size)]
        return d_slab(r, lo, size)

    extent = (depth, chunk)

    def z_copy(kind, k, r):
        src = (gu_own, d_own)[kind].at[a ^ k]
        return remote(
            src, slab(kind, r, 0, extent[kind]), s_sem.at[2 * kind], z_r.at[kind, k], (a ^ k, b, t)
        )

    def z_start(kind, k):
        go(z_copy(kind, k, me))

    def z_wait(kind, k):
        z_copy(kind, k, (a ^ k) * nb + b).wait_recv()

    def full_copy(kind, s, d, h, who):
        size = extent[kind] // 2
        ref = slab(kind, (a ^ s) * nb + who, h * size, size)
        i = h if d == h else 2 + kind * d
        return remote(ref, ref, s_sem.at[kind], f_r.at[kind, s, i], (a, b ^ (1 << d), t))

    def full_start(kind, s):
        for d, h in ((0, 0), (1, 1), (0, 1), (1, 0)):
            go(full_copy(kind, s, d, h, b))

    def full_wait(kind, s, d, h):
        full_copy(kind, s, d, h, b ^ (1 << d)).wait_recv()

    def diag_copy(kind, s, h, who):
        size = extent[kind] // 2
        ref = slab(kind, (a ^ s) * nb + who, h * size, size)
        return remote(ref, ref, s_sem.at[kind], f_r.at[kind, s, 2 + kind], (a, b ^ (2 >> h), t))

    def relay(kind, s):
        for h in range(2):
            full_wait(kind, s, h, h)
            go(diag_copy(kind, s, h, b ^ (1 << h)))

    def arrived(s):
        landed(f_r.at[0, s, 2], gu_all.at[:2])

    landed(in_sem.at[0], gatw_v)
    landed(in_sem.at[1], gatn_v)
    gat_v[:, :wide_heads, :] = gatw_v[...]
    gat_v[:, wide_heads:, :] = gatn_v[...]
    it = lax.broadcasted_iota(jnp.int32, (rows, rows), 0)
    js = lax.broadcasted_iota(jnp.int32, (rows, rows), 1)
    upper = (it <= js).astype(f32)
    eye = (it == js).astype(f32)
    last_dims = (((1,), (1,)), ((), ()))
    first_dims = (((0,), (0,)), ((), ()))
    exact = dict(precision=lax.Precision.HIGHEST, preferred_element_type=f32)
    gate_in = gat_v[0]
    x = gat_v[1]
    forget = jnp.minimum(x, 0.0) - jnp.log1p(jnp.exp(-jnp.abs(x))) + gat_v[2]
    cum = jnp.dot(forget, upper, **exact)
    cum_t = lax.dot_general(eye, cum, last_dims, **exact)
    diff = gate_in - cum
    diff_t = lax.dot_general(eye, diff, last_dims, **exact)
    total = cum[:, rows - 1 : rows]
    level = jnp.max(total + diff, axis=1, keepdims=True)
    total_t = cum_t[rows - 1 : rows, :]
    level_t = jnp.max(total_t + diff_t, axis=0, keepdims=True)
    tail_t = jnp.exp(total_t + diff_t - level_t)
    lane = lax.broadcasted_iota(jnp.int32, (heads, 128), 1)
    mark[...] = jnp.where(
        lane < 64, jnp.broadcast_to(level, (heads, 128)), jnp.broadcast_to(total, (heads, 128))
    )

    groups = (
        (qw_v, kw_v, vw_v, ogw_v, gainw_v, raw_w, DK_A, dv_w, wide_heads, 0),
        (qn_v, kn_v, vn_v, ogn_v, gainn_v, raw_n, DK_B, dv_n, narrow_heads, wide_heads),
    )
    fold = DK_B // 2
    deep = DK_A + fold

    is_inner = (a + 1) // 2 % 2
    inner = is_inner == 1
    order = (0, 1 + 2 * is_inner, 3 - 2 * is_inner, 2)
    odd = a % 2
    group = (0, 1, 2 + is_inner, 3 - is_inner)
    late = group[2:]


    joint = kw_v.shape[1] + vw_v.shape[1]
    landed(in_sem.at[2], read_v.at[: rows * joint // model])
    joint = kn_v.shape[1] + vn_v.shape[1]
    landed(in_sem.at[3], read_v.at[: rows * joint // model])
    for _, k, v, _, _, _, dk, dv, count, base in groups:
        scale = dk ** (-0.5)
        for h in range(count):
            i = base + h
            scaled = k[:, h * dk : (h + 1) * dk].astype(f32) * (tail_t[:, i : i + 1] * scale)
            memory = lax.dot_general(
                scaled.astype(bf16),
                v[:, h * dv : (h + 1) * dv],
                first_dims,
                preferred_element_type=f32,
            ).astype(bf16)
            if base == 0:
                sent[h, :dk, :] = memory
            else:
                sent[h, DK_A:deep, :dv] = memory[:fold]
                sent[h, DK_A:deep, dv:] = memory[fold:]

    def p1(m, r):
        peer = (a, b ^ m, t)
        return (
            remote(mark, mark_got.at[r], s_sem.at[3], p1_r.at[0, m], peer),
            remote(sent.at[b ^ m], got.at[r], s_sem.at[4], p1_r.at[1, m], peer),
        )

    pl.semaphore_wait(barrier, len(peers))
    for m in range(1, nb):
        for c in p1(m, b):
            go(c)
    for c in own_down:
        c.wait()
    pltpu.make_async_copy(d_own, d_own, in_sem.at[6]).wait()
    z_start(1, 1)
    got[b] = sent[b]
    mark_got[b] = mark[...]

    pltpu.make_async_copy(
        gu_own.at[:, :, : 2 * whole], gu_own.at[:, :, : 2 * whole], in_sem.at[7]
    ).wait()
    pltpu.make_async_copy(edge_v, edge_v, in_sem.at[8]).wait()
    for c in range(na // 2):
        ge, ue = edge_v[0, c], edge_v[1, c]
        gu_own[2 * c, :, 2 * whole :] = jnp.concatenate([ge[:, :half], ue[:, :half]], axis=1)
        gu_own[2 * c + 1, :, 2 * whole :] = jnp.concatenate([ge[:, half:], ue[:, half:]], axis=1)
    gu_all[me] = gu_own[a]

    @pl.when(inner)
    def _():
        z_copy(0, 3, me).start()

    full_start(0, 0)
    full_start(1, 0)

    landed(in_sem.at[9], qw_v)
    landed(in_sem.at[10], qn_v)
    for q, k, v, _, _, raw, dk, dv, count, base in groups:
        scale = dk ** (-0.5)
        for h in range(count):
            i = base + h
            q_h = q[:, h * dk : (h + 1) * dk]
            k_h = k[:, h * dk : (h + 1) * dk]
            v_h = v[:, h * dv : (h + 1) * dv]
            scores = lax.dot_general(q_h, k_h, last_dims, preferred_element_type=f32)
            logits = cum_t[:, i : i + 1] + diff[i : i + 1, :]
            logits = jnp.where(js <= it, logits, LOW)
            stab = jnp.max(logits, axis=1, keepdims=True)
            weighted = scores * scale * jnp.exp(logits - stab)
            raw[:, h * dv : (h + 1) * dv] = jnp.dot(
                weighted.astype(bf16), v_h, preferred_element_type=f32
            )
            stabs[:, i : i + 1] = stab

    for m in range(1, nb):
        for c in p1(m, b ^ m):
            c.wait_recv()
    spans = ((0, DK_A), (DK_A, deep))

    def read_mark(ref, where, row):
        line = ref[where, pl.ds(row, 1), :]
        return line[:, :1], line[:, 127:128]

    run = []
    for g, (lo, hi) in enumerate(spans):
        lev, tot = read_mark(mark_got, 0, b + g * wide_heads)
        state = got[0, lo:hi, :].astype(f32)
        run.append([(lev, tot)])
        for j in range(1, nb):
            prefix[j - 1, lo:hi, :] = state
            lev2, tot2 = read_mark(mark_got, j, b + g * wide_heads)
            new = jnp.maximum(lev + tot2, lev2)
            state = (
                jnp.exp(lev + tot2 - new) * state
                + jnp.exp(lev2 - new) * got[j, lo:hi, :].astype(f32)
            )
            lev, tot = new, tot + tot2
            run[g].append((lev, tot))
        total_s[lo:hi, :] = state.astype(bf16)
    lane1 = lax.broadcasted_iota(jnp.int32, (1, 128), 1)
    for g in range(2):
        lev, tot = run[g][nb - 1]
        tmark[g : g + 1, :] = jnp.where(
            lane1 < 64, jnp.broadcast_to(lev, (1, 128)), jnp.broadcast_to(tot, (1, 128))
        )

    def p2(k, r):
        peer = (a ^ k, b, t)
        return (
            remote(tmark, tmark_got.at[r], p2_s.at[0, k], p2_r.at[0, k], peer),
            remote(total_s, total_got.at[r], p2_s.at[1, k], p2_r.at[1, k], peer),
        )

    for k in range(1, na):

        @pl.when((a ^ k) > a)
        def _():
            for c in p2(k, a):
                c.start()

    @pl.when(inner)
    def _():
        z_copy(0, 2, me).start()
        z_copy(0, 1, me).start()

    @pl.when(jnp.logical_not(inner))
    def _():
        for k in range(1, na):
            z_copy(0, k, me).start()


    enter[...] = jnp.zeros(enter.shape, f32)
    enter_mark[...] = jnp.full(enter_mark.shape, LOW, f32)
    for k in range(1, na):

        @pl.when((a ^ k) < a)
        def _():
            for c in p2(k, a ^ k):
                c.wait_recv()

    for z in range(na - 1):

        @pl.when(z < a)
        def _():
            for g, (lo, hi) in enumerate(spans):
                lev = enter_mark[g : g + 1, :1]
                lev2, tot2 = read_mark(tmark_got, z, g)
                new = jnp.maximum(lev + tot2, lev2)
                enter[lo:hi, :] = (
                    jnp.exp(lev + tot2 - new) * enter[lo:hi, :]
                    + jnp.exp(lev2 - new) * total_got[z, lo:hi, :].astype(f32)
                )
                enter_mark[g : g + 1, :] = jnp.broadcast_to(new, (1, 128))

    for g, (lo, hi) in enumerate(spans):
        lev = enter_mark[g : g + 1, :1]
        back[0, lo:hi, :] = enter[lo:hi, :].astype(bf16)
        bmark[0, g : g + 1, :] = jnp.broadcast_to(lev, (1, 128))
        for j in range(1, nb):
            lev2, tot2 = run[g][j - 1]
            new = jnp.maximum(lev + tot2, lev2)
            back[j, lo:hi, :] = (
                jnp.exp(lev + tot2 - new) * enter[lo:hi, :]
                + jnp.exp(lev2 - new) * prefix[j - 1, lo:hi, :]
            ).astype(bf16)
            bmark[j, g : g + 1, :] = jnp.broadcast_to(new, (1, 128))

    def p3(m, r):
        peer = (a, b ^ m, t)
        return (
            remote(bmark.at[b ^ m], bmark_got.at[r], s_sem.at[5], p3_r.at[0, m], peer),
            remote(back.at[b ^ m], carried.at[r], s_sem.at[6], p3_r.at[1, m], peer),
        )

    for m in range(1, nb):
        for c in p3(m, b):
            go(c)
    carried[b] = back[b]
    bmark_got[b] = bmark[b]
    relay(0, 0)
    relay(1, 0)

    for i, ref in enumerate((ogw_v, ogn_v, gainw_v, gainn_v)):
        landed(in_sem.at[11 + i], ref)
    for m in range(1, nb):
        for c in p3(m, b ^ m):
            c.wait_recv()

    for g, (q, _, _, og, gain, raw, dk, dv, count, base) in enumerate(groups):
        for h in range(count):
            i = base + h
            if g == 0:
                memory = carried[h, :dk, :]
            else:
                memory = jnp.concatenate(
                    [carried[h, DK_A:deep, :dv], carried[h, DK_A:deep, dv:]], axis=0
                )
            own = stabs[:, i : i + 1]
            shifted = cum_t[:, i : i + 1] + bmark_got[h, g : g + 1, :1]
            both = jnp.maximum(own, shifted)
            span_h = slice(h * dv, (h + 1) * dv)
            incoming = jnp.dot(
                q[:, h * dk : (h + 1) * dk], memory, preferred_element_type=f32
            )
            value = raw[:, span_h] * jnp.exp(own - both) + incoming * jnp.exp(shifted - both)
            value = value * lax.rsqrt(jnp.mean(value * value, axis=1, keepdims=True) + 1e-06)
            gate_h = 1.0 / (1.0 + jnp.exp(-og[:, span_h].astype(f32)))
            value = value * gain[span_h].astype(f32).reshape(1, dv) * gate_h
            lo = g * raw_w.shape[1] + h * dv
            gated[:, lo : lo + dv] = value.astype(bf16)

    z_wait(0, order[1])
    full_start(0, order[1])

    for i, ref in enumerate((read_v, res_v, ngain_v)):
        landed(in_sem.at[15 + i], ref)
    tile = model // 4
    for j in range(model // tile):
        sl = slice(j * tile, (j + 1) * tile)
        p = jnp.dot(gated[...], read_v[:, sl], preferred_element_type=f32).astype(bf16)
        part[:, :, sl] = p.reshape(2, own_rows, tile)
    partner = (a, b, 1 - t)
    swap = remote(part.at[1 - t], part_got, s_sem.at[7], t_r.at[0], partner)
    go(swap)
    swap.wait_recv()
    mixed = part[t].astype(f32) + part_got[...].astype(f32)
    mid = (res_v[...].astype(f32) + mixed).astype(bf16)
    middle[...] = mid
    mid = mid.astype(f32)
    normed = mid * lax.rsqrt(jnp.mean(mid * mid, axis=-1, keepdims=True) + 1e-06)
    block = 2 * own_rows

    piece = own_rows // 2

    def row_block(z, core, c, size=piece):
        lo = (z * 2 + core) * own_rows + c * piece
        return x_all.at[pl.ds(pl.multiple_of(lo, piece), size)]

    x_all[pl.ds(pl.multiple_of((a * 2 + t) * own_rows, own_rows), own_rows), :] = (
        normed * ngain_v[...].astype(f32).reshape(1, model)
    ).astype(bf16)

    def x_copy(i, k, z, c):
        ref = row_block(z, t, c)
        return remote(ref, ref, s_sem.at[9], x_r.at[i, c], (a ^ k, b, t))

    def y_copy(z, core, c, i=0):
        ref = row_block(z, core, c)
        return remote(ref, ref, s_sem.at[10], y_r.at[i // 2], partner)

    for c in range(2):
        go(x_copy(0, 2, a, c))
    for c in range(2):
        go(x_copy(1, 1, a, c))
    for c in range(2):
        go(y_copy(a, t, c))

    @pl.when(inner)
    def _():
        z_copy(1, 3, me).start()
        z_copy(1, 2, me).start()

    width = gu_all.shape[2]
    tiles = [(lo, min(lo + 512, width)) for lo in range(0, width, 512)]

    def unit(lo, m, s, fresh):
        z = a ^ s
        xs = x_all[pl.ds(lo, m), pl.ds(pl.multiple_of(z * kspan, kspan), kspan)]
        for c0, c1 in tiles:
            w = gu_all[pl.ds(z * nb, nb), :, c0:c1].reshape(kspan, c1 - c0)
            p = jnp.dot(xs, w, preferred_element_type=f32)
            if fresh:
                acc[pl.ds(lo, m), c0:c1] = p
            else:
                acc[pl.ds(lo, m), c0:c1] += p

    def passed_on(i, k):
        z = a ^ k
        for c in range(2):
            x_copy(i, 1 if i else 2, z, c).wait_recv()
            if i == 0:
                go(x_copy(2, 1, z, c))
            go(y_copy(z, t, c, i))

    z_wait(0, order[2])
    full_start(0, order[2])
    relay(0, order[1])
    z_wait(0, order[3])
    full_start(0, order[3])
    relay(0, order[2])
    passed_on(0, 2)

    @pl.when(jnp.logical_not(inner))
    def _():
        z_copy(1, 2, me).start()
        z_copy(1, 3, me).start()


    passed_on(1, 1)
    relay(0, order[3])
    z_wait(1, 1)
    full_start(1, 1)
    total_rows = na * block
    landed(y_r.at[0], x_all.at[: 3 * own_rows])

    def row_unit(k, s):
        unit(pl.multiple_of((a ^ k) * block, block), block, order[s], s == 0)

    for s in range(2):
        arrived(order[s])
        for k in range(na - 1):
            row_unit(k, s)
    passed_on(2, 3)
    landed(y_r.at[1], x_all.at[:own_rows])
    for s in range(2):
        row_unit(na - 1, s)
    for s in range(2, na):
        if s == 3:
            z_wait(1, late[0])
            full_start(1, late[0])
        arrived(order[s])
        unit(0, total_rows, order[s], False)

    for j in range(2):
        sl = slice(j * total_rows // 2, (j + 1) * total_rows // 2)
        gt = acc[sl, :whole]
        hidden[sl, :whole] = (
            gt * (1.0 / (1.0 + jnp.exp(-gt))) * acc[sl, whole : 2 * whole]
        ).astype(bf16)
        mx = acc[sl, 2 * whole :]
        hx = mx * (1.0 / (1.0 + jnp.exp(-mx))) * pltpu.roll(mx, half, 1)
        hidden[sl, whole:] = hx[:, :half].astype(bf16)
    relay(1, 1)
    z_wait(1, late[1])
    full_start(1, late[1])

    side = b // 2
    high = a // 2
    unit_cols = 2 * cols

    def t_copy(u):
        return remote(
            terms.at[u, :, 1 - t], terms_got.at[u], s_sem.at[8], t_r.at[1 + u], partner
        )

    def other(u):
        g = (3 - is_inner, 2 + is_inner, is_inner, 1 - is_inner)[u // 2]
        return 2 * g + u % 2

    def place(u):
        return (a ^ group[u // 2]) * 2 + (side + u) % 2

    def down_unit(u):
        g = group[u // 2]
        if u % 2 == 0:
            full_wait(1, g, 0, 1)
        else:
            landed(f_r.at[1, g, 3], d_all.at[0, : 3 * chunk // 4])
        v = jnp.dot(hidden[...], d_all[place(u)], preferred_element_type=f32)
        terms[u] = v.astype(bf16).reshape(terms.shape[1:])
        go(t_copy(u))

    def a_copy(u, w):
        return remote(sums.at[u, :, 1 - odd], a_got.at[w], s_sem.at[11], a_r.at[w], (a ^ 1, b, t))

    def b_copy(u, w):
        return remote(joined.at[u], b_got.at[w], s_sem.at[12], b_r.at[w], (a ^ 2, b, t))

    def sum_unit(u):
        t_copy(u).wait_recv()
        sums[u] = (
            (terms[u, :, t].astype(f32) + terms_got[u].astype(f32))
            .astype(bf16)
            .reshape(sums.shape[1:])
        )
        go(a_copy(u, u ^ 2 if u < 4 else u))

    def join_unit(u):
        a_copy(u, u).wait_recv()
        joined[u] = (
            sums[u, 1 - high, odd].astype(f32) + a_got[u, 1 - high].astype(f32)
        ).astype(bf16)
        go(b_copy(u, other(u)))

    def finish_unit(u):
        b_copy(u, u).wait_recv()
        v = sums[u, high, odd].astype(f32) + a_got[u, high].astype(f32)
        v = v + b_got[u].astype(f32)
        c0 = pl.ds(pl.multiple_of(place(u) * unit_cols, unit_cols), unit_cols)
        out[:, c0] = (middle[:, c0].astype(f32) + v).astype(bf16)

    down_unit(0)
    down_unit(1)
    down_unit(2)
    sum_unit(0)
    sum_unit(1)
    relay(1, late[0])
    sum_unit(2)
    down_unit(4)
    down_unit(3)
    sum_unit(4)
    relay(1, late[1])
    join_unit(2)
    join_unit(0)
    sum_unit(3)
    join_unit(3)
    down_unit(6)
    join_unit(4)
    sum_unit(6)
    join_unit(1)
    down_unit(5)
    sum_unit(5)
    join_unit(6)
    down_unit(7)
    sum_unit(7)
    join_unit(5)
    join_unit(7)

    for u in (4, 5, 2, 3, 6, 7, 0, 1):
        finish_unit(u)

    sends = (
        gu_all.at[: n - 1],
        d_all.at[: 3 * n // 8],
        d_own.at[: na - 1],
        mark_got.at[: nb - 1],
        got.at[: nb - 1],
        bmark_got.at[: nb - 1],
        carried.at[: nb - 1],
        part_got,
        terms_got,
        x_all.at[: 3 * own_rows],
        x_all.at[: total_rows // 2],
        a_got,
        b_got,
    )
    for i, ref in enumerate(sends):
        landed(s_sem.at[i], ref)
    for k in range(1, na):

        @pl.when((a ^ k) > a)
        def _():
            for c in p2(k, a):
                c.wait_send()


def layer(na, nb, *args):
    (res, q_w, k_w, v_w, og_w, gat_w, gain_w, read_w) = args[:8]
    (q_n, k_n, v_n, og_n, gat_n, gain_n, read_n, norm_gain, gate, up, down) = args[8:]
    bf16, f32 = jnp.bfloat16, jnp.float32
    n = na * nb
    depth = gate.shape[0]
    chunk = gate.shape[1] // na
    whole = chunk // 128 * 128
    width = 2 * whole + 128
    cols = down.shape[1]
    own_rows, model = res.shape
    rows = q_w.shape[0]
    heads = gat_w.shape[1] + gat_n.shape[1]
    deep = DK_A + DK_B // 2
    dv = v_w.shape[1] // gat_w.shape[1]
    total_rows = na * 2 * own_rows
    units = n // 2

    def vm(shape, dtype=bf16):
        return pltpu.VMEM(shape, dtype)

    def like(x):
        return pltpu.VMEM(x.shape, x.dtype)

    dma = pltpu.SemaphoreType.DMA
    scratch = [
        like(res),
        like(q_w),
        like(k_w),
        like(v_w),
        like(og_w),
        like(gat_w),
        like(gain_w),
        like(q_n),
        like(k_n),
        like(v_n),
        like(og_n),
        like(gat_n),
        like(gain_n),
        vm((read_w.shape[0] + read_n.shape[0], model)),
        like(norm_gain),
        vm((2, na // 2, depth, 128)),
        vm((na, depth, width)),
        vm((na, chunk, cols)),
        vm((n, depth, width)),
        vm((n // 2, chunk, 2 * cols)),
        vm((3, heads, rows), f32),
        vm(v_w.shape, f32),
        vm(v_n.shape, f32),
        vm((rows, 128), f32),
        vm((nb, deep, dv)),
        vm((nb, deep, dv)),
        vm((heads, 128), f32),
        vm((nb, heads, 128), f32),
        vm((nb - 1, deep, dv), f32),
        vm((deep, dv)),
        vm((na, deep, dv)),
        vm((8, 128), f32),
        vm((na, 8, 128), f32),
        vm((deep, dv), f32),
        vm((8, 128), f32),
        vm((nb, deep, dv)),
        vm((nb, deep, dv)),
        vm((nb, 8, 128), f32),
        vm((nb, 8, 128), f32),
        vm((rows, v_w.shape[1] + v_n.shape[1])),
        vm((2, own_rows, model)),
        vm((own_rows, model)),
        vm((own_rows, model)),
        vm((total_rows, model)),
        vm((total_rows, width), f32),
        vm((total_rows, chunk)),
        vm((units, na, 2, own_rows, 2 * cols)),
        vm((units, na, own_rows, 2 * cols)),
        vm((units, na // 2, 2, own_rows, 2 * cols)),
        vm((units, na // 2, own_rows, 2 * cols)),
        vm((units, own_rows, 2 * cols)),
        vm((units, own_rows, 2 * cols)),
        vm(res.shape),
        dma((18,)),
        dma((13,)),
        dma((2, nb)),
        dma((2, na)),
        dma((2, na)),
        dma((2, nb)),
        dma((2, na)),
        dma((2, na, 4)),
        dma((1 + units,)),
        dma((3, 2)),
        dma((2,)),
        dma((units,)),
        dma((units,)),
    ]
    hbm = pl.BlockSpec(memory_space=pl.ANY)
    return pl.pallas_call(
        functools.partial(layer_kernel, na, nb),
        out_shape=pltpu.VMEM(res.shape, bf16),
        in_specs=[hbm] * 19,
        out_specs=pl.BlockSpec(memory_space=pltpu.VMEM),
        scratch_shapes=scratch,
        compiler_params=pltpu.CompilerParams(
            collective_id=0, has_side_effects=True, vmem_limit_bytes=60 * 2**20
        ),
    )(
        res,
        q_w,
        k_w,
        v_w,
        og_w,
        gat_w,
        gain_w,
        read_w,
        q_n,
        k_n,
        v_n,
        og_n,
        gat_n,
        gain_n,
        read_n,
        norm_gain,
        gate,
        up,
        down,
    )


def fits(mesh_shape, args):
    na, nb, ntp = mesh_shape
    gate, gat_w, gat_n = args[16], args[5], args[12]
    q_w, v_w, v_n = args[1], args[3], args[10]
    heads_w, heads_n = gat_w.shape[1], gat_n.shape[1]
    return (
        na == nb == 4
        and ntp == 2
        and gate.shape[1] % na == 0
        and gate.shape[1] // na % 128 == 64
        and heads_w == heads_n == nb
        and q_w.shape[0] == 128
        and v_w.shape[1] // heads_w == 2 * (v_n.shape[1] // heads_n)
    )


def passed(block, axis, step):
    size = lax.axis_size(axis)
    if step % size == 0:
        return block
    return lax.ppermute(block, axis, [(i, (i + step) % size) for i in range(size)])


def gathered(block, axis):
    return jnp.concatenate([passed(block, axis, r) for r in range(lax.axis_size(axis))], axis=0)


def returned(blocks, axis):
    size = lax.axis_size(axis)
    rows = blocks.shape[0] // size
    pieces = [passed(blocks[r * rows : (r + 1) * rows], axis, -r) for r in range(size)]
    return sum(p.astype(jnp.float32) for p in pieces)


def plain_body(
    residual,
    query_wide,
    key_wide,
    value_wide,
    outgate_wide,
    gating_wide,
    gain_wide,
    readout_wide,
    query_narrow,
    key_narrow,
    value_narrow,
    outgate_narrow,
    gating_narrow,
    gain_narrow,
    readout_narrow,
    norm_gain,
    gate_weight,
    up_weight,
    down_weight,
):
    na, nb = lax.axis_size("a"), lax.axis_size("b")
    depth, hidden_tp = gate_weight.shape
    chunk = hidden_tp // na
    out_cols = down_weight.shape[1]
    model = residual.shape[1]

    def spread(pieces):
        return lax.all_to_all(pieces, "a", split_axis=0, concat_axis=0, tiled=True)

    mine = (
        spread(jnp.moveaxis(gate_weight.reshape(depth, na, chunk), 1, 0)),
        spread(jnp.moveaxis(up_weight.reshape(depth, na, chunk), 1, 0)),
        spread(down_weight.reshape(na, chunk, out_cols)),
    )
    gate_all, up_all, down_all = (
        lax.all_gather(m, "b", axis=0, tiled=True) for m in mine
    )
    *_, gating_wide, gating_narrow = lax.optimization_barrier(
        (*mine, gating_wide, gating_narrow)
    )

    gated_w, gated_n = cell(
        query_wide,
        key_wide,
        value_wide,
        outgate_wide,
        gating_wide,
        gain_wide,
        query_narrow,
        key_narrow,
        value_narrow,
        outgate_narrow,
        gating_narrow,
        gain_narrow,
    )
    partial = (
        jnp.dot(gated_w, readout_wide, preferred_element_type=jnp.float32)
        + jnp.dot(gated_n, readout_narrow, preferred_element_type=jnp.float32)
    ).astype(jnp.bfloat16)
    own_rows = residual.shape[0]
    ntp, core = lax.axis_size("tp"), lax.axis_index("tp")
    mixed = 0.0
    for r in range(ntp):
        block = lax.dynamic_slice_in_dim(partial, lax.rem(core + r, ntp) * own_rows, own_rows)
        mixed = mixed + passed(block, "tp", r).astype(jnp.float32)
    middle_f = (residual.astype(jnp.float32) + mixed).astype(jnp.bfloat16).astype(jnp.float32)
    normed = middle_f * lax.rsqrt(jnp.mean(middle_f * middle_f, axis=-1, keepdims=True) + 1e-06)
    normed = (normed * norm_gain.astype(jnp.float32)).astype(jnp.bfloat16)
    own_rows = normed.shape[0]
    normed = normed.reshape(own_rows, na, nb, depth).swapaxes(1, 2).reshape(own_rows, model)
    all_rows = gathered(gathered(normed, "a"), "tp")
    gate = jnp.dot(all_rows, gate_all.reshape(model, chunk), preferred_element_type=jnp.float32)
    upper = jnp.dot(all_rows, up_all.reshape(model, chunk), preferred_element_type=jnp.float32)
    hidden = (jax.nn.silu(gate) * upper).astype(jnp.bfloat16)
    down = jnp.transpose(down_all, (1, 0, 2)).reshape(chunk, model)
    terms = jnp.dot(hidden, down, preferred_element_type=jnp.float32)
    back = returned(returned(terms.astype(jnp.bfloat16), "tp").astype(jnp.bfloat16), "a")
    back = back.reshape(own_rows, nb, na, out_cols).swapaxes(1, 2).reshape(own_rows, model)
    return (middle_f + back).astype(jnp.bfloat16)


def body(*args):
    sizes = tuple(lax.axis_size(x) for x in ("a", "b", "tp"))
    if fits(sizes, args):
        return layer(sizes[0], sizes[1], *args)
    return plain_body(*args)


def solution(mesh):
    sp, tp = mesh.shape["sp"], mesh.shape["tp"]
    a = 4 if sp % 4 == 0 else 1
    split = Mesh(mesh.devices.reshape(a, sp // a, tp), ("a", "b", "tp"))
    s = ("a", "b")
    in_specs = (
        P(("a", "b", "tp"), None),
        P(s, "tp"),
        P(s, "tp"),
        P(s, "tp"),
        P(s, "tp"),
        P(None, "tp", s),
        P("tp"),
        P("tp", None),
        P(s, "tp"),
        P(s, "tp"),
        P(s, "tp"),
        P(s, "tp"),
        P(None, "tp", s),
        P("tp"),
        P("tp", None),
        P(),
        P(s, "tp"),
        P(s, "tp"),
        P("tp", s),
    )
    out_specs = P(("a", "b", "tp"), None)
    return jax.shard_map(body, mesh=split, in_specs=in_specs, out_specs=out_specs, check_vma=False)
```

```python
import functools

import jax
import jax.numpy as jnp
from jax import lax
from jax.experimental import pallas as pl
from jax.experimental.pallas import tpu as pltpu
from jax.sharding import Mesh, PartitionSpec as P

DK_A = 128
DK_B = 64
LOW = -1e30
MESH = pl.DeviceIdType.MESH


def cell_kernel(
    n,
    q_w,
    k_w,
    v_w,
    og_w,
    gain_w,
    q_n,
    k_n,
    v_n,
    og_n,
    gain_n,
    gating,
    out_w,
    out_n,
    raw_w,
    raw_n,
    stabs,
    sent,
    got,
    back,
    carried,
    mem_w,
    mem_n,
    state,
    levels,
    send_sem,
    recv_sem,
    send_sem2,
    recv_sem2,
):
    na, nb = lax.axis_size("a"), lax.axis_size("b")
    tp = lax.axis_index("tp")
    me = lax.axis_index("a") * nb + lax.axis_index("b")

    def where_is(index):
        return (index // nb, lax.rem(index, nb), tp)

    barrier = pltpu.get_barrier_semaphore()

    def greet(r, _):
        peer = lax.rem(me + r, n)
        pl.semaphore_signal(barrier, inc=1, device_id=where_is(peer), device_id_type=MESH)
        return 0

    lax.fori_loop(1, n, greet, 0)

    rows = q_w.shape[0]
    heads_p = gating.shape[1]
    groups = (
        (q_w, k_w, v_w, og_w, gain_w, out_w, raw_w, mem_w, DK_A),
        (q_n, k_n, v_n, og_n, gain_n, out_n, raw_n, mem_n, DK_B),
    )
    heads = tuple(g[0].shape[1] // g[8] for g in groups)
    parts = tuple(h * g[8] // n for h, g in zip(heads, groups))
    starts = (0, parts[0])
    extra = parts[0] + parts[1]

    it = lax.broadcasted_iota(jnp.int32, (rows, rows), 0)
    js = lax.broadcasted_iota(jnp.int32, (rows, rows), 1)
    upper = (it <= js).astype(jnp.float32)
    eye = (it == js).astype(jnp.float32)
    last_dims = (((1,), (1,)), ((), ()))
    first_dims = (((0,), (0,)), ((), ()))
    gate_in = gating[0]
    x = gating[1]
    forget = jnp.minimum(x, 0.0) - jnp.log1p(jnp.exp(-jnp.abs(x))) + gating[2]
    cum = jnp.dot(
        forget, upper, precision=lax.Precision.HIGHEST, preferred_element_type=jnp.float32
    )
    cum_t = lax.dot_general(
        eye, cum, last_dims, precision=lax.Precision.HIGHEST, preferred_element_type=jnp.float32
    )
    diff = gate_in - cum
    diff_t = lax.dot_general(
        eye, diff, last_dims, precision=lax.Precision.HIGHEST, preferred_element_type=jnp.float32
    )
    total = cum[:, rows - 1 : rows]
    level = jnp.max(total + diff, axis=1, keepdims=True)
    total_t = cum_t[rows - 1 : rows, :]
    level_t = jnp.max(total_t + diff_t, axis=0, keepdims=True)
    tail_t = jnp.exp(total_t + diff_t - level_t)
    width = sent.shape[2]
    lane = lax.broadcasted_iota(jnp.int32, (heads_p, width), 1)
    marks = jnp.where(
        lane < width // 2,
        jnp.broadcast_to(level, (heads_p, width)),
        jnp.broadcast_to(total, (heads_p, width)),
    )

    index = 0
    for g, (q, k, v, _, _, _, raw, _, dk) in enumerate(groups):
        dv = v.shape[1] // heads[g]
        scale = dk ** (-0.5)
        for h in range(heads[g]):
            k_h = k[:, h * dk : (h + 1) * dk]
            v_h = v[:, h * dv : (h + 1) * dv]
            scaled = k_h.astype(jnp.float32) * (tail_t[:, index : index + 1] * scale)
            memory = lax.dot_general(
                scaled.astype(jnp.bfloat16), v_h, first_dims, preferred_element_type=jnp.float32
            )
            size = parts[g]
            per = dk // size
            for p in range(per):
                sent[h * per + p, starts[g] : starts[g] + size, :dv] = memory[
                    p * size : (p + 1) * size
                ]
            index += 1
    spare = v_n.shape[1] // heads[1]
    if spare < width:
        sent[:, starts[1] : extra, spare:] = jnp.zeros((n, parts[1], width - spare), jnp.float32)
    for p in range(n):
        sent[p, extra : extra + heads_p, :] = marks

    pl.semaphore_wait(barrier, n - 1)

    def out_copy(r):
        peer = lax.rem(me + r, n)
        return pltpu.make_async_remote_copy(
            src_ref=sent.at[peer],
            dst_ref=got.at[me],
            send_sem=send_sem.at[r],
            recv_sem=recv_sem.at[r],
            device_id=where_is(peer),
            device_id_type=MESH,
        )

    lax.fori_loop(1, n, lambda r, c: (out_copy(r).start(), c)[1], 0)
    got[me] = sent[me]

    index = 0
    for g, (q, k, v, _, _, _, raw, _, dk) in enumerate(groups):
        dv = v.shape[1] // heads[g]
        scale = dk ** (-0.5)
        for h in range(heads[g]):
            q_h = q[:, h * dk : (h + 1) * dk]
            k_h = k[:, h * dk : (h + 1) * dk]
            v_h = v[:, h * dv : (h + 1) * dv]
            scores = lax.dot_general(q_h, k_h, last_dims, preferred_element_type=jnp.float32)
            logits = cum_t[:, index : index + 1] + diff[index : index + 1, :]
            logits = jnp.where(js <= it, logits, LOW)
            stab = jnp.max(logits, axis=1, keepdims=True)
            weighted = scores * scale * jnp.exp(logits - stab)
            raw[:, h * dv : (h + 1) * dv] = jnp.dot(
                weighted.astype(jnp.bfloat16), v_h, preferred_element_type=jnp.float32
            )
            stabs[:, index : index + 1] = stab
            index += 1

    lax.fori_loop(1, n, lambda r, c: (out_copy(r).wait(), c)[1], 0)

    which = tuple(
        (me * parts[g]) // groups[g][8] + (heads[0] if g else 0) for g in range(2)
    )
    sub = lax.broadcasted_iota(jnp.int32, (heads_p, width), 0)
    picks = tuple(sub == w for w in which)

    def merge(t, _):
        level_c = levels[0]
        back[t] = state[...]
        levels[1] = jnp.where(t == me, level_c, levels[1])
        mark = got[t, extra : extra + heads_p, :]
        lev = jnp.broadcast_to(mark[:, :1], mark.shape)
        tot = jnp.broadcast_to(mark[:, width - 1 :], mark.shape)
        new = jnp.maximum(level_c + tot, lev)
        old_f = jnp.exp(level_c + tot - new)
        new_f = jnp.exp(lev - new)
        levels[0] = new
        for g in range(2):
            span = slice(starts[g], starts[g] + parts[g])

            def pick(f):
                return jnp.sum(jnp.where(picks[g], f, 0.0), axis=0, keepdims=True)

            state[span, :] = pick(old_f) * state[span, :] + pick(new_f) * got[t, span, :]
        return 0

    levels[...] = jnp.full(levels.shape, LOW, jnp.float32)
    state[...] = jnp.zeros(state.shape, jnp.float32)
    lax.fori_loop(0, n, merge, 0)
    entering = levels[1]

    def back_copy(r):
        peer = lax.rem(me + r, n)
        return pltpu.make_async_remote_copy(
            src_ref=back.at[peer],
            dst_ref=carried.at[me],
            send_sem=send_sem2.at[r],
            recv_sem=recv_sem2.at[r],
            device_id=where_is(peer),
            device_id_type=MESH,
        )

    lax.fori_loop(1, n, lambda r, c: (back_copy(r).start(), c)[1], 0)
    carried[me] = back[me]
    entering_t = lax.dot_general(
        jnp.where(
            lax.broadcasted_iota(jnp.int32, (rows, width), 1) == 0, 1.0, 0.0
        ),
        entering,
        last_dims,
        precision=lax.Precision.HIGHEST,
        preferred_element_type=jnp.float32,
    )
    shifted = cum_t + entering_t
    own = stabs[:, :heads_p]
    both = jnp.maximum(own, shifted)
    own_f = jnp.exp(own - both)
    in_f = jnp.exp(shifted - both)
    lax.fori_loop(1, n, lambda r, c: (back_copy(r).wait(), c)[1], 0)

    index = 0
    for g, (q, _, v, og, gain, out, raw, mem, dk) in enumerate(groups):
        dv = v.shape[1] // heads[g]
        size = parts[g]
        per = dk // size
        for h in range(heads[g]):
            for p in range(per):
                mem[p * size : (p + 1) * size, :] = carried[
                    h * per + p, starts[g] : starts[g] + size, :dv
                ]
            memory = mem[...]
            high = memory.astype(jnp.bfloat16)
            rest = (memory - high.astype(jnp.float32)).astype(jnp.bfloat16)
            q_h = q[:, h * dk : (h + 1) * dk]
            cols = slice(h * dv, (h + 1) * dv)
            incoming = jnp.dot(q_h, high, preferred_element_type=jnp.float32) + jnp.dot(
                q_h, rest, preferred_element_type=jnp.float32
            )
            value = (
                raw[:, cols] * own_f[:, index : index + 1]
                + incoming * in_f[:, index : index + 1]
            )
            value = value * lax.rsqrt(jnp.mean(value * value, axis=1, keepdims=True) + 1e-06)
            gate = 1.0 / (1.0 + jnp.exp(-og[:, cols].astype(jnp.float32)))
            value = value * gain[:, cols].astype(jnp.float32) * gate
            out[:, cols] = value.astype(jnp.bfloat16)
            index += 1


def cell(q_w, k_w, v_w, og_w, gat_w, gain_w, q_n, k_n, v_n, og_n, gat_n, gain_n):
    n = lax.axis_size("a") * lax.axis_size("b")
    rows = q_w.shape[0]
    heads = gat_w.shape[1] + gat_n.shape[1]
    heads_p = -(-heads // 8) * 8
    gating = jnp.concatenate([gat_w, gat_n], axis=1)
    gating = jnp.pad(gating, ((0, 0), (0, heads_p - heads), (0, 0)))
    parts = (q_w.shape[1] // n, q_n.shape[1] // n)
    width = v_w.shape[1] // gat_w.shape[1]
    width_n = v_n.shape[1] // gat_n.shape[1]
    vmem = pl.BlockSpec(memory_space=pltpu.VMEM)
    state = parts[0] + parts[1]
    return pl.pallas_call(
        functools.partial(cell_kernel, n),
        out_shape=(
            jax.ShapeDtypeStruct(v_w.shape, jnp.bfloat16),
            jax.ShapeDtypeStruct(v_n.shape, jnp.bfloat16),
        ),
        in_specs=[vmem] * 11,
        out_specs=(vmem, vmem),
        scratch_shapes=[
            pltpu.VMEM(v_w.shape, jnp.float32),
            pltpu.VMEM(v_n.shape, jnp.float32),
            pltpu.VMEM((rows, 128), jnp.float32),
            pltpu.VMEM((n, state + heads_p, width), jnp.float32),
            pltpu.VMEM((n, state + heads_p, width), jnp.float32),
            pltpu.VMEM((n, state, width), jnp.float32),
            pltpu.VMEM((n, state, width), jnp.float32),
            pltpu.VMEM((DK_A, width), jnp.float32),
            pltpu.VMEM((DK_B, width_n), jnp.float32),
            pltpu.VMEM((state, width), jnp.float32),
            pltpu.VMEM((2, heads_p, width), jnp.float32),
            pltpu.SemaphoreType.DMA((n,)),
            pltpu.SemaphoreType.DMA((n,)),
            pltpu.SemaphoreType.DMA((n,)),
            pltpu.SemaphoreType.DMA((n,)),
        ],
        compiler_params=pltpu.CompilerParams(
            collective_id=0, has_side_effects=True, vmem_limit_bytes=32 * 2**20
        ),
        cost_estimate=pl.CostEstimate(
            flops=2 * 10**9, bytes_accessed=120 * 10**6, transcendentals=0
        ),
    )(
        q_w,
        k_w,
        v_w,
        og_w,
        gain_w.reshape(1, -1),
        q_n,
        k_n,
        v_n,
        og_n,
        gain_n.reshape(1, -1),
        gating,
    )


def layer_kernel(na, nb, *refs):
    (
        residual,
        q_w,
        k_w,
        v_w,
        og_w,
        gat_w,
        gain_w,
        read_w,
        q_n,
        k_n,
        v_n,
        og_n,
        gat_n,
        gain_n,
        read_n,
        norm_gain,
        gate,
        up,
        down,
        out,
        res_v,
        qw_v,
        kw_v,
        vw_v,
        ogw_v,
        gatw_v,
        gainw_v,
        qn_v,
        kn_v,
        vn_v,
        ogn_v,
        gatn_v,
        gainn_v,
        read_v,
        ngain_v,
        edge_v,
        gu_own,
        d_own,
        gu_all,
        d_all,
        gat_v,
        raw_w,
        raw_n,
        stabs,
        sent,
        got,
        mark,
        mark_got,
        prefix,
        total_s,
        total_got,
        tmark,
        tmark_got,
        enter,
        enter_mark,
        back,
        carried,
        bmark,
        bmark_got,
        gated,
        part,
        part_got,
        middle,
        x_all,
        acc,
        hidden,
        terms,
        terms_got,
        sums,
        a_got,
        joined,
        b_got,
        out_v,
        in_sem,
        s_sem,
        p1_r,
        p2_s,
        p2_r,
        p3_r,
        z_r,
        f_r,
        t_r,
        x_r,
        y_r,
        a_r,
        b_r,
    ) = refs
    n = na * nb
    a, b, t = lax.axis_index("a"), lax.axis_index("b"), lax.axis_index("tp")
    me = a * nb + b
    f32, bf16 = jnp.float32, jnp.bfloat16

    barrier = pltpu.get_barrier_semaphore()
    peers = [(a ^ k, b, t) for k in range(1, na)]
    peers += [(a, b ^ m, t) for m in range(1, nb)]
    peers += [(a, b, 1 - t)]
    for peer in peers:
        pl.semaphore_signal(barrier, inc=1, device_id=peer, device_id_type=MESH)

    depth = gate.shape[0]
    chunk = gate.shape[1] // na
    whole = chunk // 128 * 128
    half = chunk - whole
    cols = down.shape[1]
    model = residual.shape[1]
    own_rows = residual.shape[0]
    rows = q_w.shape[0]
    kspan = nb * depth
    wide_heads, narrow_heads = gat_w.shape[1], gat_n.shape[1]
    heads = wide_heads + narrow_heads
    dv_w = v_w.shape[1] // wide_heads
    dv_n = v_n.shape[1] // narrow_heads

    def local(src, dst, i):
        pltpu.make_async_copy(src, dst, in_sem.at[i]).start()

    def landed(sem, ref):
        pltpu.make_async_copy(ref, ref, sem).wait()

    local(gat_w, gatw_v, 0)
    local(gat_n, gatn_v, 1)
    for src, dst in ((k_w, kw_v), (v_w, vw_v)):
        local(src, dst, 2)
    for src, dst in ((k_n, kn_v), (v_n, vn_v)):
        local(src, dst, 3)

    def slab_parts(c):
        odd = c % 2
        return c * chunk + odd * half, c * chunk + (1 - odd) * whole

    def d_slab(r, lo=0, size=chunk):
        return d_all.at[
            r // 2, pl.ds(lo, size), pl.ds(pl.multiple_of(lax.rem(r, 2) * cols, cols), cols)
        ]

    first, second = slab_parts(a)
    own_down = (
        pltpu.make_async_copy(
            down.at[pl.ds(pl.multiple_of(first, half), whole)],
            d_slab(me, 0, whole),
            in_sem.at[4],
        ),
        pltpu.make_async_copy(
            down.at[pl.ds(pl.multiple_of(second, half), half)],
            d_slab(me, whole, half),
            in_sem.at[5],
        ),
    )
    for c in own_down:
        c.start()
    for c in range(na):
        lo, hi = slab_parts(c)
        pltpu.make_async_copy(
            down.at[lo : lo + whole], d_own.at[c, 0:whole], in_sem.at[6]
        ).start()
        pltpu.make_async_copy(
            down.at[hi : hi + half], d_own.at[c, whole:chunk], in_sem.at[6]
        ).start()
    for i, w in enumerate((gate, up)):
        for c in range(na):
            lo, _ = slab_parts(c)
            pltpu.make_async_copy(
                w.at[:, lo : lo + whole],
                gu_own.at[c, :, i * whole : (i + 1) * whole],
                in_sem.at[7],
            ).start()
        for c in range(na // 2):
            lo = 2 * c * chunk + whole
            pltpu.make_async_copy(
                w.at[:, lo : lo + 128], edge_v.at[i, c], in_sem.at[8]
            ).start()
    local(q_w, qw_v, 9)
    local(q_n, qn_v, 10)
    local(og_w, ogw_v, 11)
    local(og_n, ogn_v, 12)
    local(gain_w, gainw_v, 13)
    local(gain_n, gainn_v, 14)
    local(read_w, read_v.at[: read_w.shape[0]], 15)
    local(read_n, read_v.at[read_w.shape[0] :], 15)
    local(residual, res_v, 16)
    local(norm_gain, ngain_v, 17)

    def remote(src, dst, s_sem, r_sem, peer):
        return pltpu.make_async_remote_copy(
            src_ref=src,
            dst_ref=dst,
            send_sem=s_sem,
            recv_sem=r_sem,
            device_id=peer,
            device_id_type=MESH,
        )

    def go(copy):
        copy.start()

    def slab(kind, r, lo, size):
        if kind == 0:
            return gu_all.at[r, pl.ds(lo, size)]
        return d_slab(r, lo, size)

    extent = (depth, chunk)

    def z_copy(kind, k, r):
        src = (gu_own, d_own)[kind].at[a ^ k]
        return remote(
            src, slab(kind, r, 0, extent[kind]), s_sem.at[2 * kind], z_r.at[kind, k], (a ^ k, b, t)
        )

    def z_start(kind, k):
        go(z_copy(kind, k, me))

    def z_wait(kind, k):
        z_copy(kind, k, (a ^ k) * nb + b).wait_recv()

    def full_copy(kind, s, d, h, who):
        size = extent[kind] // 2
        ref = slab(kind, (a ^ s) * nb + who, h * size, size)
        i = h if d == h else 2 + kind * d
        return remote(ref, ref, s_sem.at[kind], f_r.at[kind, s, i], (a, b ^ (1 << d), t))

    def full_start(kind, s):
        for d, h in ((0, 0), (1, 1), (0, 1), (1, 0)):
            go(full_copy(kind, s, d, h, b))

    def full_wait(kind, s, d, h):
        full_copy(kind, s, d, h, b ^ (1 << d)).wait_recv()

    def diag_copy(kind, s, h, who):
        size = extent[kind] // 2
        ref = slab(kind, (a ^ s) * nb + who, h * size, size)
        return remote(ref, ref, s_sem.at[kind], f_r.at[kind, s, 2 + kind], (a, b ^ (2 >> h), t))

    def relay(kind, s):
        for h in range(2):
            full_wait(kind, s, h, h)
            go(diag_copy(kind, s, h, b ^ (1 << h)))

    def arrived(s):
        landed(f_r.at[0, s, 2], gu_all.at[:2])

    landed(in_sem.at[0], gatw_v)
    landed(in_sem.at[1], gatn_v)
    gat_v[:, :wide_heads, :] = gatw_v[...]
    gat_v[:, wide_heads:, :] = gatn_v[...]
    it = lax.broadcasted_iota(jnp.int32, (rows, rows), 0)
    js = lax.broadcasted_iota(jnp.int32, (rows, rows), 1)
    upper = (it <= js).astype(f32)
    eye = (it == js).astype(f32)
    last_dims = (((1,), (1,)), ((), ()))
    first_dims = (((0,), (0,)), ((), ()))
    exact = dict(precision=lax.Precision.HIGHEST, preferred_element_type=f32)
    gate_in = gat_v[0]
    x = gat_v[1]
    forget = jnp.minimum(x, 0.0) - jnp.log1p(jnp.exp(-jnp.abs(x))) + gat_v[2]
    cum = jnp.dot(forget, upper, **exact)
    cum_t = lax.dot_general(eye, cum, last_dims, **exact)
    diff = gate_in - cum
    diff_t = lax.dot_general(eye, diff, last_dims, **exact)
    total = cum[:, rows - 1 : rows]
    level = jnp.max(total + diff, axis=1, keepdims=True)
    total_t = cum_t[rows - 1 : rows, :]
    level_t = jnp.max(total_t + diff_t, axis=0, keepdims=True)
    tail_t = jnp.exp(total_t + diff_t - level_t)
    lane = lax.broadcasted_iota(jnp.int32, (heads, 128), 1)
    mark[...] = jnp.where(
        lane < 64, jnp.broadcast_to(level, (heads, 128)), jnp.broadcast_to(total, (heads, 128))
    )

    groups = (
        (qw_v, kw_v, vw_v, ogw_v, gainw_v, raw_w, DK_A, dv_w, wide_heads, 0),
        (qn_v, kn_v, vn_v, ogn_v, gainn_v, raw_n, DK_B, dv_n, narrow_heads, wide_heads),
    )
    fold = DK_B // 2
    deep = DK_A + fold

    is_inner = (a + 1) // 2 % 2
    inner = is_inner == 1
    order = (0, 1 + 2 * is_inner, 3 - 2 * is_inner, 2)
    odd = a % 2
    group = (0, 1, 2 + is_inner, 3 - is_inner)
    late = group[2:]


    joint = kw_v.shape[1] + vw_v.shape[1]
    landed(in_sem.at[2], read_v.at[: rows * joint // model])
    joint = kn_v.shape[1] + vn_v.shape[1]
    landed(in_sem.at[3], read_v.at[: rows * joint // model])
    for _, k, v, _, _, _, dk, dv, count, base in groups:
        scale = dk ** (-0.5)
        for h in range(count):
            i = base + h
            scaled = k[:, h * dk : (h + 1) * dk].astype(f32) * (tail_t[:, i : i + 1] * scale)
            memory = lax.dot_general(
                scaled.astype(bf16),
                v[:, h * dv : (h + 1) * dv],
                first_dims,
                preferred_element_type=f32,
            ).astype(bf16)
            if base == 0:
                sent[h, :dk, :] = memory
            else:
                sent[h, DK_A:deep, :dv] = memory[:fold]
                sent[h, DK_A:deep, dv:] = memory[fold:]

    note = heads + deep * dv_w // 256

    def p1(m, r):
        peer = (a, b ^ m, t)
        return (
            remote(mark, mark_got.at[r], s_sem.at[3], p1_r.at[m - 1], peer),
            remote(sent.at[b ^ m], got.at[r], s_sem.at[3], p1_r.at[m - 1], peer),
        )

    pl.semaphore_wait(barrier, len(peers))
    for m in range(1, nb):
        for c in p1(m, b):
            go(c)
    for c in own_down:
        c.wait()
    pltpu.make_async_copy(d_own, d_own, in_sem.at[6]).wait()
    z_start(1, 1)
    got[b] = sent[b]
    mark_got[b] = mark[...]

    pltpu.make_async_copy(
        gu_own.at[:, :, : 2 * whole], gu_own.at[:, :, : 2 * whole], in_sem.at[7]
    ).wait()
    pltpu.make_async_copy(edge_v, edge_v, in_sem.at[8]).wait()
    for c in range(na // 2):
        ge, ue = edge_v[0, c], edge_v[1, c]
        gu_own[2 * c, :, 2 * whole :] = jnp.concatenate([ge[:, :half], ue[:, :half]], axis=1)
        gu_own[2 * c + 1, :, 2 * whole :] = jnp.concatenate([ge[:, half:], ue[:, half:]], axis=1)
    gu_all[me] = gu_own[a]

    @pl.when(inner)
    def _():
        z_copy(0, 3, me).start()

    full_start(0, 0)
    full_start(1, 0)

    landed(in_sem.at[9], qw_v)
    landed(in_sem.at[10], qn_v)
    for q, k, v, _, _, raw, dk, dv, count, base in groups:
        scale = dk ** (-0.5)
        for h in range(count):
            i = base + h
            q_h = q[:, h * dk : (h + 1) * dk]
            k_h = k[:, h * dk : (h + 1) * dk]
            v_h = v[:, h * dv : (h + 1) * dv]
            scores = lax.dot_general(q_h, k_h, last_dims, preferred_element_type=f32)
            logits = cum_t[:, i : i + 1] + diff[i : i + 1, :]
            logits = jnp.where(js <= it, logits, LOW)
            stab = jnp.max(logits, axis=1, keepdims=True)
            weighted = scores * scale * jnp.exp(logits - stab)
            raw[:, h * dv : (h + 1) * dv] = jnp.dot(
                weighted.astype(bf16), v_h, preferred_element_type=f32
            )
            stabs[:, i : i + 1] = stab

    for m in range(1, nb):
        landed(p1_r.at[m - 1], acc.at[:note, :128])
    spans = ((0, DK_A), (DK_A, deep))

    def read_mark(ref, where, row):
        line = ref[where, pl.ds(row, 1), :]
        return line[:, :1], line[:, 127:128]

    run = []
    for g, (lo, hi) in enumerate(spans):
        lev, tot = read_mark(mark_got, 0, b + g * wide_heads)
        state = got[0, lo:hi, :].astype(f32)
        run.append([(lev, tot)])
        for j in range(1, nb):
            prefix[j - 1, lo:hi, :] = state
            lev2, tot2 = read_mark(mark_got, j, b + g * wide_heads)
            new = jnp.maximum(lev + tot2, lev2)
            state = (
                jnp.exp(lev + tot2 - new) * state
                + jnp.exp(lev2 - new) * got[j, lo:hi, :].astype(f32)
            )
            lev, tot = new, tot + tot2
            run[g].append((lev, tot))
        total_s[lo:hi, :] = state.astype(bf16)
    lane1 = lax.broadcasted_iota(jnp.int32, (1, 128), 1)
    for g in range(2):
        lev, tot = run[g][nb - 1]
        tmark[g : g + 1, :] = jnp.where(
            lane1 < 64, jnp.broadcast_to(lev, (1, 128)), jnp.broadcast_to(tot, (1, 128))
        )

    def p2(k, r):
        peer = (a ^ k, b, t)
        return (
            remote(tmark, tmark_got.at[r], p2_s.at[0, k], p2_r.at[0, k], peer),
            remote(total_s, total_got.at[r], p2_s.at[1, k], p2_r.at[1, k], peer),
        )

    for k in range(1, na):

        @pl.when((a ^ k) > a)
        def _():
            for c in p2(k, a):
                c.start()

    @pl.when(inner)
    def _():
        z_copy(0, 2, me).start()
        z_copy(0, 1, me).start()

    @pl.when(jnp.logical_not(inner))
    def _():
        for k in range(1, na):
            z_copy(0, k, me).start()


    enter[...] = jnp.zeros(enter.shape, f32)
    enter_mark[...] = jnp.full(enter_mark.shape, LOW, f32)
    for k in range(1, na):

        @pl.when((a ^ k) < a)
        def _():
            for c in p2(k, a ^ k):
                c.wait_recv()

    for z in range(na - 1):

        @pl.when(z < a)
        def _():
            for g, (lo, hi) in enumerate(spans):
                lev = enter_mark[g : g + 1, :1]
                lev2, tot2 = read_mark(tmark_got, z, g)
                new = jnp.maximum(lev + tot2, lev2)
                enter[lo:hi, :] = (
                    jnp.exp(lev + tot2 - new) * enter[lo:hi, :]
                    + jnp.exp(lev2 - new) * total_got[z, lo:hi, :].astype(f32)
                )
                enter_mark[g : g + 1, :] = jnp.broadcast_to(new, (1, 128))

    for g, (lo, hi) in enumerate(spans):
        lev = enter_mark[g : g + 1, :1]
        back[0, lo:hi, :] = enter[lo:hi, :].astype(bf16)
        bmark[0, g : g + 1, :] = jnp.broadcast_to(lev, (1, 128))
        for j in range(1, nb):
            lev2, tot2 = run[g][j - 1]
            new = jnp.maximum(lev + tot2, lev2)
            back[j, lo:hi, :] = (
                jnp.exp(lev + tot2 - new) * enter[lo:hi, :]
                + jnp.exp(lev2 - new) * prefix[j - 1, lo:hi, :]
            ).astype(bf16)
            bmark[j, g : g + 1, :] = jnp.broadcast_to(new, (1, 128))

    def p3(m, r):
        peer = (a, b ^ m, t)
        return (
            remote(bmark.at[b ^ m], bmark_got.at[r], s_sem.at[4], p3_r.at[m - 1], peer),
            remote(back.at[b ^ m], carried.at[r], s_sem.at[4], p3_r.at[m - 1], peer),
        )

    for m in range(1, nb):
        for c in p3(m, b):
            go(c)
    carried[b] = back[b]
    bmark_got[b] = bmark[b]
    relay(0, 0)
    relay(1, 0)

    for i, ref in enumerate((ogw_v, ogn_v, gainw_v, gainn_v)):
        landed(in_sem.at[11 + i], ref)
    for m in range(1, nb):
        landed(p3_r.at[m - 1], acc.at[:note, :128])

    for g, (q, _, _, og, gain, raw, dk, dv, count, base) in enumerate(groups):
        for h in range(count):
            i = base + h
            if g == 0:
                memory = carried[h, :dk, :]
            else:
                memory = jnp.concatenate(
                    [carried[h, DK_A:deep, :dv], carried[h, DK_A:deep, dv:]], axis=0
                )
            own = stabs[:, i : i + 1]
            shifted = cum_t[:, i : i + 1] + bmark_got[h, g : g + 1, :1]
            both = jnp.maximum(own, shifted)
            span_h = slice(h * dv, (h + 1) * dv)
            incoming = jnp.dot(
                q[:, h * dk : (h + 1) * dk], memory, preferred_element_type=f32
            )
            value = raw[:, span_h] * jnp.exp(own - both) + incoming * jnp.exp(shifted - both)
            value = value * lax.rsqrt(jnp.mean(value * value, axis=1, keepdims=True) + 1e-06)
            gate_h = 1.0 / (1.0 + jnp.exp(-og[:, span_h].astype(f32)))
            value = value * gain[span_h].astype(f32).reshape(1, dv) * gate_h
            lo = g * raw_w.shape[1] + h * dv
            gated[:, lo : lo + dv] = value.astype(bf16)

    z_wait(0, order[1])
    full_start(0, order[1])

    for i, ref in enumerate((read_v, res_v, ngain_v)):
        landed(in_sem.at[15 + i], ref)
    tile = model // 4
    for j in range(model // tile):
        sl = slice(j * tile, (j + 1) * tile)
        p = jnp.dot(gated[...], read_v[:, sl], preferred_element_type=f32).astype(bf16)
        part[:, :, sl] = p.reshape(2, own_rows, tile)
    partner = (a, b, 1 - t)
    swap = remote(part.at[1 - t], part_got, s_sem.at[5], t_r.at[0], partner)
    go(swap)
    swap.wait_recv()
    mixed = part[t].astype(f32) + part_got[...].astype(f32)
    mid = (res_v[...].astype(f32) + mixed).astype(bf16)
    middle[...] = mid
    mid = mid.astype(f32)
    normed = mid * lax.rsqrt(jnp.mean(mid * mid, axis=-1, keepdims=True) + 1e-06)
    block = 2 * own_rows

    piece = own_rows // 2

    def row_block(z, core, c, size=piece):
        lo = (z * 2 + core) * own_rows + c * piece
        return x_all.at[pl.ds(pl.multiple_of(lo, piece), size)]

    x_all[pl.ds(pl.multiple_of((a * 2 + t) * own_rows, own_rows), own_rows), :] = (
        normed * ngain_v[...].astype(f32).reshape(1, model)
    ).astype(bf16)

    def x_copy(i, k, z, c):
        ref = row_block(z, t, c)
        return remote(ref, ref, s_sem.at[7], x_r.at[i, c], (a ^ k, b, t))

    def y_copy(z, core, c, i=0):
        ref = row_block(z, core, c)
        return remote(ref, ref, s_sem.at[8], y_r.at[i // 2], partner)

    for c in range(2):
        go(x_copy(0, 2, a, c))
    for c in range(2):
        go(x_copy(1, 1, a, c))
    for c in range(2):
        go(y_copy(a, t, c))

    @pl.when(inner)
    def _():
        z_copy(1, 3, me).start()

    width = gu_all.shape[2]
    tiles = [(lo, min(lo + 512, width)) for lo in range(0, width, 512)]

    def unit(lo, m, s, fresh):
        z = a ^ s
        xs = x_all[pl.ds(lo, m), pl.ds(pl.multiple_of(z * kspan, kspan), kspan)]
        for c0, c1 in tiles:
            w = gu_all[pl.ds(z * nb, nb), :, c0:c1].reshape(kspan, c1 - c0)
            p = jnp.dot(xs, w, preferred_element_type=f32)
            if fresh:
                acc[pl.ds(lo, m), c0:c1] = p
            else:
                acc[pl.ds(lo, m), c0:c1] += p

    def passed_on(i, k):
        z = a ^ k
        for c in range(2):
            x_copy(i, 1 if i else 2, z, c).wait_recv()
            if i == 0:
                go(x_copy(2, 1, z, c))
            go(y_copy(z, t, c, i))

    z_wait(0, order[2])
    full_start(0, order[2])
    relay(0, order[1])
    z_wait(0, order[3])
    full_start(0, order[3])
    relay(0, order[2])
    passed_on(0, 2)

    @pl.when(inner)
    def _():
        z_copy(1, 2, me).start()


    @pl.when(jnp.logical_not(inner))
    def _():
        z_copy(1, 2, me).start()
        z_copy(1, 3, me).start()


    passed_on(1, 1)
    relay(0, order[3])
    z_wait(1, 1)
    full_start(1, 1)
    total_rows = na * block
    landed(y_r.at[0], x_all.at[: 3 * own_rows])

    def row_unit(k, s):
        unit(pl.multiple_of((a ^ k) * block, block), block, order[s], s == 0)

    for s in range(2):
        arrived(order[s])
        for k in range(na - 1):
            row_unit(k, s)
    passed_on(2, 3)
    landed(y_r.at[1], x_all.at[:own_rows])
    for s in range(2):
        row_unit(na - 1, s)
    for s in range(2, na):
        if s == 3:
            z_wait(1, late[0])
            full_start(1, late[0])
        arrived(order[s])
        unit(0, total_rows, order[s], False)

    for j in range(2):
        sl = slice(j * total_rows // 2, (j + 1) * total_rows // 2)
        gt = acc[sl, :whole]
        hidden[sl, :whole] = (
            gt * (1.0 / (1.0 + jnp.exp(-gt))) * acc[sl, whole : 2 * whole]
        ).astype(bf16)
        mx = acc[sl, 2 * whole :]
        hx = mx * (1.0 / (1.0 + jnp.exp(-mx))) * pltpu.roll(mx, half, 1)
        hidden[sl, whole:] = hx[:, :half].astype(bf16)
    relay(1, 1)
    z_wait(1, late[1])
    full_start(1, late[1])

    side = b // 2
    high = a // 2
    unit_cols = 2 * cols

    def t_copy(u):
        return remote(
            terms.at[u, :, 1 - t], terms_got.at[u], s_sem.at[6], t_r.at[1 + u], partner
        )

    def other(u):
        g = (3 - is_inner, 2 + is_inner, is_inner, 1 - is_inner)[u // 2]
        return 2 * g + u % 2

    def place(u):
        return (a ^ group[u // 2]) * 2 + (side + u) % 2

    def down_unit(u):
        g = group[u // 2]
        if u % 2 == 0:
            full_wait(1, g, 0, 1)
        else:
            landed(f_r.at[1, g, 3], d_all.at[0, : 3 * chunk // 4])
        v = jnp.dot(hidden[...], d_all[place(u)], preferred_element_type=f32)
        terms[u] = v.astype(bf16).reshape(terms.shape[1:])
        go(t_copy(u))

    def a_copy(u, w):
        return remote(sums.at[u, :, 1 - odd], a_got.at[w], s_sem.at[9], a_r.at[w], (a ^ 1, b, t))

    def b_copy(u, w):
        return remote(joined.at[u], b_got.at[w], s_sem.at[10], b_r.at[w], (a ^ 2, b, t))

    def sum_unit(u):
        t_copy(u).wait_recv()
        sums[u] = (
            (terms[u, :, t].astype(f32) + terms_got[u].astype(f32))
            .astype(bf16)
            .reshape(sums.shape[1:])
        )
        go(a_copy(u, u ^ 2 if u < 4 else u))

    def join_unit(u):
        a_copy(u, u).wait_recv()
        joined[u] = (
            sums[u, 1 - high, odd].astype(f32) + a_got[u, 1 - high].astype(f32)
        ).astype(bf16)
        go(b_copy(u, other(u)))

    def finish_unit(u):
        b_copy(u, u).wait_recv()
        v = sums[u, high, odd].astype(f32) + a_got[u, high].astype(f32)
        v = v + b_got[u].astype(f32)
        c0 = pl.ds(pl.multiple_of(place(u) * unit_cols, unit_cols), unit_cols)
        out[:, c0] = (middle[:, c0].astype(f32) + v).astype(bf16)

    down_unit(0)
    down_unit(1)
    down_unit(2)
    sum_unit(0)
    sum_unit(1)
    relay(1, late[0])
    sum_unit(2)
    down_unit(4)
    down_unit(3)
    sum_unit(4)
    relay(1, late[1])
    join_unit(2)
    join_unit(0)
    sum_unit(3)
    join_unit(3)
    down_unit(6)
    join_unit(4)
    sum_unit(6)
    join_unit(1)
    down_unit(5)
    sum_unit(5)
    join_unit(6)
    down_unit(7)
    sum_unit(7)
    join_unit(5)
    join_unit(7)

    for u in (4, 5, 2, 3, 6, 7, 0, 1):
        finish_unit(u)

    sends = (
        gu_all.at[: n - 1],
        d_all.at[: 3 * n // 8],
        d_own.at[: na - 1],
        acc.at[: (nb - 1) * note, :128],
        acc.at[: (nb - 1) * note, :128],
        part_got,
        terms_got,
        x_all.at[: 3 * own_rows],
        x_all.at[: total_rows // 2],
        a_got,
        b_got,
    )
    for i, ref in enumerate(sends):
        landed(s_sem.at[i], ref)
    for k in range(1, na):

        @pl.when((a ^ k) > a)
        def _():
            for c in p2(k, a):
                c.wait_send()


def layer(na, nb, *args):
    (res, q_w, k_w, v_w, og_w, gat_w, gain_w, read_w) = args[:8]
    (q_n, k_n, v_n, og_n, gat_n, gain_n, read_n, norm_gain, gate, up, down) = args[8:]
    bf16, f32 = jnp.bfloat16, jnp.float32
    n = na * nb
    depth = gate.shape[0]
    chunk = gate.shape[1] // na
    whole = chunk // 128 * 128
    width = 2 * whole + 128
    cols = down.shape[1]
    own_rows, model = res.shape
    rows = q_w.shape[0]
    heads = gat_w.shape[1] + gat_n.shape[1]
    deep = DK_A + DK_B // 2
    dv = v_w.shape[1] // gat_w.shape[1]
    total_rows = na * 2 * own_rows
    units = n // 2

    def vm(shape, dtype=bf16):
        return pltpu.VMEM(shape, dtype)

    def like(x):
        return pltpu.VMEM(x.shape, x.dtype)

    dma = pltpu.SemaphoreType.DMA
    scratch = [
        like(res),
        like(q_w),
        like(k_w),
        like(v_w),
        like(og_w),
        like(gat_w),
        like(gain_w),
        like(q_n),
        like(k_n),
        like(v_n),
        like(og_n),
        like(gat_n),
        like(gain_n),
        vm((read_w.shape[0] + read_n.shape[0], model)),
        like(norm_gain),
        vm((2, na // 2, depth, 128)),
        vm((na, depth, width)),
        vm((na, chunk, cols)),
        vm((n, depth, width)),
        vm((n // 2, chunk, 2 * cols)),
        vm((3, heads, rows), f32),
        vm(v_w.shape, f32),
        vm(v_n.shape, f32),
        vm((rows, 128), f32),
        vm((nb, deep, dv)),
        vm((nb, deep, dv)),
        vm((heads, 128), f32),
        vm((nb, heads, 128), f32),
        vm((nb - 1, deep, dv), f32),
        vm((deep, dv)),
        vm((na, deep, dv)),
        vm((8, 128), f32),
        vm((na, 8, 128), f32),
        vm((deep, dv), f32),
        vm((8, 128), f32),
        vm((nb, deep, dv)),
        vm((nb, deep, dv)),
        vm((nb, 8, 128), f32),
        vm((nb, 8, 128), f32),
        vm((rows, v_w.shape[1] + v_n.shape[1])),
        vm((2, own_rows, model)),
        vm((own_rows, model)),
        vm((own_rows, model)),
        vm((total_rows, model)),
        vm((total_rows, width), f32),
        vm((total_rows, chunk)),
        vm((units, na, 2, own_rows, 2 * cols)),
        vm((units, na, own_rows, 2 * cols)),
        vm((units, na // 2, 2, own_rows, 2 * cols)),
        vm((units, na // 2, own_rows, 2 * cols)),
        vm((units, own_rows, 2 * cols)),
        vm((units, own_rows, 2 * cols)),
        vm(res.shape),
        dma((18,)),
        dma((11,)),
        dma((nb - 1,)),
        dma((2, na)),
        dma((2, na)),
        dma((nb - 1,)),
        dma((2, na)),
        dma((2, na, 4)),
        dma((1 + units,)),
        dma((3, 2)),
        dma((2,)),
        dma((units,)),
        dma((units,)),
    ]
    hbm = pl.BlockSpec(memory_space=pl.ANY)
    return pl.pallas_call(
        functools.partial(layer_kernel, na, nb),
        out_shape=pltpu.VMEM(res.shape, bf16),
        in_specs=[hbm] * 19,
        out_specs=pl.BlockSpec(memory_space=pltpu.VMEM),
        scratch_shapes=scratch,
        compiler_params=pltpu.CompilerParams(
            collective_id=0, has_side_effects=True, vmem_limit_bytes=60 * 2**20
        ),
    )(
        res,
        q_w,
        k_w,
        v_w,
        og_w,
        gat_w,
        gain_w,
        read_w,
        q_n,
        k_n,
        v_n,
        og_n,
        gat_n,
        gain_n,
        read_n,
        norm_gain,
        gate,
        up,
        down,
    )


def fits(mesh_shape, args):
    na, nb, ntp = mesh_shape
    gate, gat_w, gat_n = args[16], args[5], args[12]
    q_w, v_w, v_n = args[1], args[3], args[10]
    heads_w, heads_n = gat_w.shape[1], gat_n.shape[1]
    return (
        na == nb == 4
        and ntp == 2
        and gate.shape[1] % na == 0
        and gate.shape[1] // na % 128 == 64
        and heads_w == heads_n == nb
        and q_w.shape[0] == 128
        and v_w.shape[1] // heads_w == 2 * (v_n.shape[1] // heads_n)
    )


def passed(block, axis, step):
    size = lax.axis_size(axis)
    if step % size == 0:
        return block
    return lax.ppermute(block, axis, [(i, (i + step) % size) for i in range(size)])


def gathered(block, axis):
    return jnp.concatenate([passed(block, axis, r) for r in range(lax.axis_size(axis))], axis=0)


def returned(blocks, axis):
    size = lax.axis_size(axis)
    rows = blocks.shape[0] // size
    pieces = [passed(blocks[r * rows : (r + 1) * rows], axis, -r) for r in range(size)]
    return sum(p.astype(jnp.float32) for p in pieces)


def plain_body(
    residual,
    query_wide,
    key_wide,
    value_wide,
    outgate_wide,
    gating_wide,
    gain_wide,
    readout_wide,
    query_narrow,
    key_narrow,
    value_narrow,
    outgate_narrow,
    gating_narrow,
    gain_narrow,
    readout_narrow,
    norm_gain,
    gate_weight,
    up_weight,
    down_weight,
):
    na, nb = lax.axis_size("a"), lax.axis_size("b")
    depth, hidden_tp = gate_weight.shape
    chunk = hidden_tp // na
    out_cols = down_weight.shape[1]
    model = residual.shape[1]

    def spread(pieces):
        return lax.all_to_all(pieces, "a", split_axis=0, concat_axis=0, tiled=True)

    mine = (
        spread(jnp.moveaxis(gate_weight.reshape(depth, na, chunk), 1, 0)),
        spread(jnp.moveaxis(up_weight.reshape(depth, na, chunk), 1, 0)),
        spread(down_weight.reshape(na, chunk, out_cols)),
    )
    gate_all, up_all, down_all = (
        lax.all_gather(m, "b", axis=0, tiled=True) for m in mine
    )
    *_, gating_wide, gating_narrow = lax.optimization_barrier(
        (*mine, gating_wide, gating_narrow)
    )

    gated_w, gated_n = cell(
        query_wide,
        key_wide,
        value_wide,
        outgate_wide,
        gating_wide,
        gain_wide,
        query_narrow,
        key_narrow,
        value_narrow,
        outgate_narrow,
        gating_narrow,
        gain_narrow,
    )
    partial = (
        jnp.dot(gated_w, readout_wide, preferred_element_type=jnp.float32)
        + jnp.dot(gated_n, readout_narrow, preferred_element_type=jnp.float32)
    ).astype(jnp.bfloat16)
    own_rows = residual.shape[0]
    ntp, core = lax.axis_size("tp"), lax.axis_index("tp")
    mixed = 0.0
    for r in range(ntp):
        block = lax.dynamic_slice_in_dim(partial, lax.rem(core + r, ntp) * own_rows, own_rows)
        mixed = mixed + passed(block, "tp", r).astype(jnp.float32)
    middle_f = (residual.astype(jnp.float32) + mixed).astype(jnp.bfloat16).astype(jnp.float32)
    normed = middle_f * lax.rsqrt(jnp.mean(middle_f * middle_f, axis=-1, keepdims=True) + 1e-06)
    normed = (normed * norm_gain.astype(jnp.float32)).astype(jnp.bfloat16)
    own_rows = normed.shape[0]
    normed = normed.reshape(own_rows, na, nb, depth).swapaxes(1, 2).reshape(own_rows, model)
    all_rows = gathered(gathered(normed, "a"), "tp")
    gate = jnp.dot(all_rows, gate_all.reshape(model, chunk), preferred_element_type=jnp.float32)
    upper = jnp.dot(all_rows, up_all.reshape(model, chunk), preferred_element_type=jnp.float32)
    hidden = (jax.nn.silu(gate) * upper).astype(jnp.bfloat16)
    down = jnp.transpose(down_all, (1, 0, 2)).reshape(chunk, model)
    terms = jnp.dot(hidden, down, preferred_element_type=jnp.float32)
    back = returned(returned(terms.astype(jnp.bfloat16), "tp").astype(jnp.bfloat16), "a")
    back = back.reshape(own_rows, nb, na, out_cols).swapaxes(1, 2).reshape(own_rows, model)
    return (middle_f + back).astype(jnp.bfloat16)


def body(*args):
    sizes = tuple(lax.axis_size(x) for x in ("a", "b", "tp"))
    if fits(sizes, args):
        return layer(sizes[0], sizes[1], *args)
    return plain_body(*args)


def solution(mesh):
    sp, tp = mesh.shape["sp"], mesh.shape["tp"]
    a = 4 if sp % 4 == 0 else 1
    split = Mesh(mesh.devices.reshape(a, sp // a, tp), ("a", "b", "tp"))
    s = ("a", "b")
    in_specs = (
        P(("a", "b", "tp"), None),
        P(s, "tp"),
        P(s, "tp"),
        P(s, "tp"),
        P(s, "tp"),
        P(None, "tp", s),
        P("tp"),
        P("tp", None),
        P(s, "tp"),
        P(s, "tp"),
        P(s, "tp"),
        P(s, "tp"),
        P(None, "tp", s),
        P("tp"),
        P("tp", None),
        P(),
        P(s, "tp"),
        P(s, "tp"),
        P("tp", s),
    )
    out_specs = P(("a", "b", "tp"), None)
    return jax.shard_map(body, mesh=split, in_specs=in_specs, out_specs=out_specs, check_vma=False)
```
